32 devices in a mesh: sp: 8 (over z, y), tp: 4 (over x, core).
Axes of the slice: x: 2, y: 2, z: 4, core: 2. Of those that a mesh axis runs over, the one named last changes fastest.
Arguments:
- query_a: bfloat16 [1024, 1536], P('sp', 'tp'), may hold values from -400 to 400
- query_b: bfloat16 [1024, 2048], P('sp', 'tp'), may hold values from -400 to 400
- latent: bfloat16 [1024, 512], P(('sp', 'tp')), may hold values from -6 to 6
- rope_key: bfloat16 [1024, 64], P(('sp', 'tp')), may hold values from -6 to 6
- latent_gain: float32 [512], replicated, may hold values from 0.1 to 1.9
- key_a_weight: bfloat16 [512, 1024], P(None, 'tp'), may hold values from -0.25 to 0.25
- value_a_weight: bfloat16 [512, 1024], P(None, 'tp'), may hold values from -0.25 to 0.25
- key_b_weight: bfloat16 [512, 1024], P(None, 'tp'), may hold values from -0.25 to 0.25
- value_b_weight: bfloat16 [512, 1024], P(None, 'tp'), may hold values from -0.25 to 0.25
- out_a_weight: bfloat16 [1024, 2048], P('tp'), may hold values from -0.25 to 0.25
- out_b_weight: bfloat16 [1024, 2048], P('tp'), may hold values from -0.25 to 0.25
- residual: bfloat16 [1024, 2048], P(('sp', 'tp')), may hold values from -6 to 6
- ffn_gain: float32 [2048], replicated, may hold values from 0.1 to 1.9
- routes: int32 [1024, 2], P(('sp', 'tp')), may hold values from 0 to 7, all different within a row; in each aligned block of 32 rows (0 to 31, 32 to 63, ...) at most 16 rows name the same one
- route_weight: float32 [1024, 2], P(('sp', 'tp')), may hold values from 0.2 to 1
- expert_gate: bfloat16 [8, 2048, 3072], P('sp', None, 'tp'), may hold values from -0.125 to 0.125
- expert_up: bfloat16 [8, 2048, 3072], P('sp', None, 'tp'), may hold values from -0.125 to 0.125
- expert_down: bfloat16 [8, 3072, 2048], P('sp', 'tp'), may hold values from -0.109375 to 0.109375
Outputs:
- layer_out: bfloat16 [1024, 2048], P(('sp', 'tp'))
The draws below stay inside these ranges and needn't reach their ends.
Inputs may be any that keep to these rules, and one draw needn't show every extreme that they name: `routes`: the 2 experts of a row differ. Among the 32 rows of one device no expert is named more than 16 times, a bound that some block reaches in some devices' rows.
All inputs are finite; a program needn't handle non-finite values.
Results may differ from the reference program's by a relative error of at most 0.019.
The reference program's roundings to bfloat16 on the way count: a program that leaves them out, or rounds other values in their place, can miss the bound.
Values may be sent and summed in bfloat16 or wider, within the bound.
A program may use at most 128 MiB of HBM per device.

```python
import math
import jax
import jax.numpy as jnp
import numpy as np
from jax import lax

D = 2048
RANK = 512
ROPE = 64
HEADS_A = 8
NOPE_A = 128
VAL_A = 128
HEADS_B = 16
NOPE_B = 64
VAL_B = 64
FF = 3072
TOP = 2
TOKENS = 1024
ROWS = 32
EXPERTS = 8
CAP = 16
N_TP = 4


def query_table(key, columns):
    normal_part = jax.random.normal(jax.random.fold_in(key, 13), (TOKENS, columns), jnp.float32)
    return (3.0 * jnp.clip(normal_part, -4.0, 4.0)).astype(jnp.bfloat16)


def draw_query_a(key, part):
    return query_table(jax.random.fold_in(key, 1), HEADS_A * (NOPE_A + ROPE))


def draw_query_b(key, part):
    return query_table(jax.random.fold_in(key, 2), HEADS_B * (NOPE_B + ROPE))


def levels(stream_key, dims, pieces, low, high):
    gain, own = 1.0, jax.random.fold_in(stream_key, 6)
    for axis_at, parts in pieces:
        steps = jnp.exp(jax.random.uniform(jax.random.fold_in(own, axis_at), (parts,), jnp.float32, low / len(pieces), high / len(pieces)))
        gain = gain * jnp.repeat(steps, dims[axis_at] // parts).reshape([-1 if axis == axis_at else 1 for axis in range(len(dims))])
    return gain


def routed_block(key, own, number, rows, amount, top, reach, lean):
    order = jax.random.permutation(key, amount)
    packed, common = portions_of(amount, rows * top, reach, lean, True), portions_of(amount, rows * top, reach, lean, False)
    places = jnp.arange(amount)

    def named(sizes, offset_by):
        used = int((sizes > 0).sum())
        fixed = max(1, used // 4)
        passed = fixed + (places - fixed + offset_by * (used - fixed)) % max(1, amount - fixed)
        return jnp.zeros((amount,), jnp.int32).at[order[jnp.where(places < fixed, places, passed)]].set(jnp.asarray(sizes, jnp.int32))

    sizes = jnp.where(number % 4 == 0, named(packed, number // 4), named(common, number - number // 4 - 1))
    mixed = jax.random.permutation(jax.random.fold_in(own, 3), amount)
    source_of, taker = mixed[0:amount // 2 * 2:2], mixed[1:amount // 2 * 2:2]
    margin = jnp.minimum(sizes[source_of] - 1, reach - sizes[taker]) // 2
    margin = jnp.where((source_of == order[0]) | (taker == order[0]) | (sizes[taker] == 0), 0, jnp.maximum(margin, 0))
    passed = jax.random.randint(jax.random.fold_in(own, 4), (amount // 2,), 0, 1 << 20) % (margin + 1)
    sizes = sizes.at[source_of].add(-passed).at[taker].add(passed)
    items = jnp.searchsorted(jnp.cumsum(sizes), jnp.arange(rows * top), side="right").astype(jnp.int32)
    table = items.reshape(top, rows).T
    table = table[jax.random.permutation(jax.random.fold_in(own, 1), rows)]
    offset_by = jax.random.randint(jax.random.fold_in(own, 2), (rows, 1), 0, top)
    return jnp.take_along_axis(table, (jnp.arange(top)[None, :] + offset_by) % top, axis=1)


def portions_of(count, total, most, slope, full):
    portions = [(1 << 20) // math.isqrt(grade ** slope) + 1 for grade in range(1, count + 1)]
    largest = most if full else min(most, max(-(-total // count), total * portions[0] // sum(portions)))
    least = 1 if total - largest >= count - 1 else 0
    given, surplus = [largest] + [least] * (count - 1), total - largest - least * (count - 1)
    while surplus > 0:
        free = [i for i in range(1, count) if given[i] < largest] or [i for i in range(1, count) if given[i] < most]
        pool, left = sum([portions[i] for i in free]), surplus
        for i in free:
            extra = min(most - given[i], max(1, left * portions[i] // pool), surplus)
            given[i] = given[i] + extra
            surplus = surplus - extra
    return np.array(given)


def noise(own_key, dims, spread, limit, cuts=(), kind=jnp.bfloat16):
    factor_of = levels(own_key, dims, cuts, -0.22, 0.18) if cuts else 1.0
    values = jax.random.normal(own_key, dims, jnp.float32) * spread * factor_of
    return jnp.minimum(jnp.maximum(values, -limit), limit).astype(kind)


def setup_inputs(seed: int = 0) -> dict:
    key_list = jax.random.split(jax.random.key(seed), 19)
    query_a = draw_query_a(jax.random.fold_in(key_list[18], 71), 0)
    query_b = draw_query_b(jax.random.fold_in(key_list[18], 71), 0)
    latent = noise(key_list[2], (TOKENS, RANK), 1.0, 6.0, ((0, 32),))
    rope_key = noise(key_list[3], (TOKENS, ROPE), 1.0, 6.0, ((0, 32),))
    latent_gain = jnp.clip(1.0 + 0.18 * jax.random.normal(key_list[4], (RANK,), jnp.float32), 0.1, 1.9)
    key_a_weight = noise(key_list[5], (RANK, HEADS_A * NOPE_A), RANK ** -0.5, 0.25, ((1, 4),))
    value_a_weight = noise(key_list[6], (RANK, HEADS_A * VAL_A), RANK ** -0.5, 0.25, ((1, 4),))
    key_b_weight = noise(key_list[7], (RANK, HEADS_B * NOPE_B), RANK ** -0.5, 0.25, ((1, 4),))
    value_b_weight = noise(key_list[8], (RANK, HEADS_B * VAL_B), RANK ** -0.5, 0.25, ((1, 4),))
    out_a_weight = noise(key_list[9], (HEADS_A * VAL_A, D), (D // 4) ** -0.5, 0.25, ((0, 4),))
    out_b_weight = noise(key_list[10], (HEADS_B * VAL_B, D), (D // 4) ** -0.5, 0.25, ((0, 4),))
    residual = noise(key_list[11], (TOKENS, D), 1.0, 6.0, ((0, 32),))
    ffn_gain = jnp.clip(1.0 + 0.18 * jax.random.normal(key_list[12], (D,), jnp.float32), 0.1, 1.9)
    routes_keys = jax.random.split(jax.random.fold_in(key_list[13], 1), TOKENS // ROWS)
    routes_turns = jax.random.permutation(jax.random.fold_in(key_list[13], 3), TOKENS // ROWS)
    routes = jax.vmap(lambda own, number: routed_block(jax.random.fold_in(key_list[13], 2), own, number, ROWS, EXPERTS, TOP, CAP, 1))(routes_keys, routes_turns).reshape((TOKENS, TOP))
    route_weight = jnp.clip(jnp.exp(math.log(1.0) - 1.609438 * jax.random.uniform(key_list[14], (TOKENS, TOP), jnp.float32) ** levels(key_list[14], (TOKENS, TOP), ((0, 32),), -0.2, 0.2)), 0.2, 1.0)
    expert_gate = noise(key_list[15], (EXPERTS, D, FF), D ** -0.5, 0.125, ((0, 8), (2, 4)))
    expert_up = noise(key_list[16], (EXPERTS, D, FF), D ** -0.5, 0.125, ((0, 8), (2, 4)))
    expert_down = noise(key_list[17], (EXPERTS, FF, D), FF ** -0.5, 0.109375, ((0, 8), (1, 4)))
    return {"query_a": query_a, "query_b": query_b, "latent": latent, "rope_key": rope_key, "latent_gain": latent_gain, "key_a_weight": key_a_weight, "value_a_weight": value_a_weight, "key_b_weight": key_b_weight, "value_b_weight": value_b_weight, "out_a_weight": out_a_weight, "out_b_weight": out_b_weight, "residual": residual, "ffn_gain": ffn_gain, "routes": routes, "route_weight": route_weight, "expert_gate": expert_gate, "expert_up": expert_up, "expert_down": expert_down}


epsilon = 1e-06
base_theta = 500000.0

def rms_scale(values, scales):
    floats = values.astype(jnp.float32)
    scaled = floats * lax.rsqrt(lax.optimization_barrier(jnp.mean(floats * floats, axis=-1, keepdims=True)) + epsilon)
    return (scaled * scales).astype(jnp.bfloat16)

def angle_tables(positions, rotary_width):
    inverse = jnp.power(jnp.float32(base_theta), -jnp.arange(0, rotary_width, 2, dtype=jnp.float32) / rotary_width)
    angles = positions.astype(jnp.float32)[:, None] * inverse[None, :]
    return (jnp.cos(angles), jnp.sin(angles))

def rotate(values, cosine, sine_table):
    middle = cosine.shape[-1]
    first_half = values[..., :middle].astype(jnp.float32)
    second_half = values[..., middle:].astype(jnp.float32)
    turned = jnp.concatenate([first_half * cosine - second_half * sine_table, second_half * cosine + first_half * sine_table], axis=-1)
    return turned.astype(jnp.bfloat16)

def prepare_queries(queries, head_count, nope_width, cosine, sine_table):
    shaped = queries.reshape(queries.shape[0], head_count, queries.shape[1] // head_count)
    turned = rotate(shaped[:, :, nope_width:], cosine[:, None, :], sine_table[:, None, :])
    return jnp.concatenate([shaped[:, :, :nope_width], turned], axis=-1)

def attend(queries, keys, values):
    total_rows = queries.shape[0]
    block_rows = math.gcd(total_rows, 512)
    scale = queries.shape[-1] ** (-0.5)
    key_places = jnp.arange(total_rows, dtype=jnp.int32)
    keys_wide = keys.astype(jnp.float32)
    values_wide = values.astype(jnp.float32)

    def one_block(block_index):
        first_row = block_index * block_rows
        chosen_rows = lax.dynamic_slice_in_dim(queries, first_row, block_rows, 0).astype(jnp.float32)
        scores = jnp.einsum('thd,shd->hts', chosen_rows, keys_wide) * scale
        query_places = first_row + jnp.arange(block_rows, dtype=jnp.int32)
        allowed = (key_places[None, :] <= query_places[:, None])[None]
        scores = jnp.where(allowed, scores, -jnp.inf)
        highest = lax.optimization_barrier(jnp.max(scores, axis=-1, keepdims=True))
        weights = jnp.where(allowed, jnp.exp(scores - highest), 0.0)
        weight_total = lax.optimization_barrier(jnp.sum(weights, axis=-1))
        rounded = lax.optimization_barrier(weights.astype(jnp.bfloat16)).astype(jnp.float32)
        summed = jnp.einsum('hts,shd->thd', rounded, values_wide)
        return (summed / jnp.transpose(weight_total)[:, :, None]).astype(jnp.bfloat16)
    outputs = lax.map(one_block, jnp.arange(total_rows // block_rows))
    return outputs.reshape(total_rows, -1)

def experts_apply(normed, routes, expert_gate, expert_up, expert_down):
    total_rows = normed.shape[0]
    depth = total_rows // ROWS * CAP
    chosen = routes.reshape(-1).astype(jnp.int32)
    matches = (chosen[:, None] == jnp.arange(EXPERTS, dtype=jnp.int32)[None, :]).astype(jnp.int32)
    running = (jnp.cumsum(matches, axis=0).astype(jnp.int32) - 1) * matches
    order_rank = lax.optimization_barrier(jnp.sum(running, axis=1)).astype(jnp.int32)
    source_rows = jnp.repeat(jnp.arange(total_rows, dtype=jnp.int32), TOP)
    buffer = jnp.zeros((EXPERTS, depth, normed.shape[1]), jnp.bfloat16).at[chosen, order_rank].set(normed[source_rows])

    def one_expert(operands):
        arrived, gate_weight, up_weight, down_weight = operands
        gate_values = jnp.dot(arrived, gate_weight, preferred_element_type=jnp.float32)
        up_values = jnp.dot(arrived, up_weight, preferred_element_type=jnp.float32)
        hidden = (jax.nn.silu(gate_values) * up_values).astype(jnp.bfloat16)
        block_width = hidden.shape[1] // N_TP
        accumulated = jnp.zeros((arrived.shape[0], down_weight.shape[1]), jnp.float32)
        for block_index in range(N_TP):
            partial_value = jnp.dot(hidden[:, block_index * block_width:(block_index + 1) * block_width], down_weight[block_index * block_width:(block_index + 1) * block_width], preferred_element_type=jnp.float32).astype(jnp.bfloat16)
            accumulated = accumulated + lax.optimization_barrier(partial_value).astype(jnp.float32)
        return accumulated.astype(jnp.bfloat16)
    results = lax.map(one_expert, (buffer, expert_gate, expert_up, expert_down))
    return results[chosen, order_rank].reshape(total_rows, TOP, -1)

def reference(query_a, query_b, latent, rope_key, latent_gain, key_a_weight, value_a_weight, key_b_weight, value_b_weight, out_a_weight, out_b_weight, residual, ffn_gain, routes, route_weight, expert_gate, expert_up, expert_down):
    total_rows = residual.shape[0]
    positions = jnp.arange(total_rows, dtype=jnp.int32)
    cosine, sine_table = angle_tables(positions, ROPE)
    normed_latent = rms_scale(latent, latent_gain)
    turned_key = rotate(rope_key, cosine, sine_table)

    def expand(weight, head_count):
        product = jnp.dot(normed_latent, weight, preferred_element_type=jnp.float32).astype(jnp.bfloat16)
        return product.reshape(total_rows, head_count, weight.shape[1] // head_count)
    key_a = expand(key_a_weight, HEADS_A)
    value_a = expand(value_a_weight, HEADS_A)
    key_b = expand(key_b_weight, HEADS_B)
    value_b = expand(value_b_weight, HEADS_B)
    keys_a = jnp.concatenate([key_a, jnp.broadcast_to(turned_key[:, None, :], (total_rows, HEADS_A, ROPE))], axis=-1)
    keys_b = jnp.concatenate([key_b, jnp.broadcast_to(turned_key[:, None, :], (total_rows, HEADS_B, ROPE))], axis=-1)
    out_a = attend(prepare_queries(query_a, HEADS_A, NOPE_A, cosine, sine_table), keys_a, value_a)
    out_b = attend(prepare_queries(query_b, HEADS_B, NOPE_B, cosine, sine_table), keys_b, value_b)
    projected = jnp.dot(out_a, out_a_weight, preferred_element_type=jnp.float32) + jnp.dot(out_b, out_b_weight, preferred_element_type=jnp.float32)
    hidden_state = (residual.astype(jnp.float32) + projected).astype(jnp.bfloat16)
    normed = rms_scale(hidden_state, ffn_gain)
    picked = experts_apply(normed, routes, expert_gate, expert_up, expert_down).astype(jnp.float32)
    expert_mix = lax.optimization_barrier(jnp.sum(picked * route_weight[:, :, None], axis=1))
    return (hidden_state.astype(jnp.float32) + expert_mix).astype(jnp.bfloat16)
```

```python
import functools

import jax
import jax.numpy as jnp
import numpy as np
from jax import lax
from jax.experimental import pallas as pl
from jax.experimental.pallas import tpu as pltpu
from jax.sharding import PartitionSpec as P

NOPE_A = 128
VAL_A = 128
NOPE_B = 64
VAL_B = 64
TOP = 2


epsilon = 1e-06
base_theta = 500000.0
masked_score = -1e30


def rms_scale(values, scales):
    floats = values.astype(jnp.float32)
    scaled = floats * lax.rsqrt(jnp.mean(floats * floats, axis=-1, keepdims=True) + epsilon)
    return (scaled * scales).astype(jnp.bfloat16)


def angle_tables(positions, rotary_width):
    inverse = jnp.power(
        jnp.float32(base_theta), -jnp.arange(0, rotary_width, 2, dtype=jnp.float32) / rotary_width
    )
    angles = positions.astype(jnp.float32)[:, None] * inverse[None, :]
    return (jnp.cos(angles), jnp.sin(angles))


def rotate(values, cosine, sine_table):
    middle = cosine.shape[-1]
    first_half = values[..., :middle].astype(jnp.float32)
    second_half = values[..., middle:].astype(jnp.float32)
    turned = jnp.concatenate(
        [
            first_half * cosine - second_half * sine_table,
            second_half * cosine + first_half * sine_table,
        ],
        axis=-1,
    )
    return turned.astype(jnp.bfloat16)


def prepare_queries(queries, head_count, nope_width, cosine, sine_table):
    shaped = queries.reshape(queries.shape[0], head_count, queries.shape[1] // head_count)
    turned = rotate(shaped[:, :, nope_width:], cosine[:, None, :], sine_table[:, None, :])
    return jnp.concatenate([shaped[:, :, :nope_width], turned], axis=-1)


def fold_group(carried, queries, key_nope, key_turned, values, query_first):
    top_score, weight_total, weighted = carried
    nope_width = key_nope.shape[2]
    scale = (nope_width + key_turned.shape[1]) ** (-0.5)
    scores = jnp.einsum(
        "thd,shd->hts", queries[:, :, :nope_width], key_nope, preferred_element_type=jnp.float32
    )
    scores = scores + jnp.einsum(
        "thd,sd->hts", queries[:, :, nope_width:], key_turned, preferred_element_type=jnp.float32
    )
    scores = scores * scale
    query_places = query_first + jnp.arange(queries.shape[0], dtype=jnp.int32)
    key_places = jnp.arange(key_nope.shape[0], dtype=jnp.int32)
    allowed = (key_places[None, :] <= query_places[:, None])[None]
    scores = jnp.where(allowed, scores, masked_score)
    new_top = jnp.maximum(top_score, jnp.max(scores, axis=-1))
    weights = jnp.where(allowed, jnp.exp(scores - new_top[:, :, None]), 0.0)
    new_total = jnp.sum(weights, axis=-1)
    product = jnp.einsum(
        "hts,shd->thd", weights.astype(jnp.bfloat16), values, preferred_element_type=jnp.float32
    )
    return (new_top, new_total, product)


def expand(source, weight, head_count):
    product = jnp.dot(source, weight, preferred_element_type=jnp.float32).astype(jnp.bfloat16)
    return product.reshape(source.shape[0], head_count, weight.shape[1] // head_count)


MESH = pl.DeviceIdType.MESH


def places():
    me, column = lax.axis_index("sp"), lax.axis_index("tp")
    half = lax.axis_size("tp") // 2
    across = lax.rem(column + half, 2 * half)
    partner = column + 1 - 2 * lax.rem(column, 2)
    return me, column, across, partner


def send(source, target, send_sem, recv_sem, place):
    return pltpu.make_async_remote_copy(
        src_ref=source,
        dst_ref=target,
        send_sem=send_sem,
        recv_sem=recv_sem,
        device_id={"sp": place[0], "tp": place[1]},
        device_id_type=MESH,
    )


def greet(count, me, column, others):
    barrier = pltpu.get_barrier_semaphore()

    def step(k, carry):
        pl.semaphore_signal(
            barrier,
            inc=1,
            device_id={"sp": lax.rem(me + k, count), "tp": column},
            device_id_type=MESH,
        )
        return carry

    lax.fori_loop(1, count, step, 0)
    for other in others:
        pl.semaphore_signal(
            barrier, inc=1, device_id={"sp": me, "tp": other}, device_id_type=MESH
        )
    pl.semaphore_wait(barrier, max(count, 1) - 1 + len(others))


def loop(low, high, step):
    lax.fori_loop(low, high, lambda k, carry: (step(k), carry)[1], 0)


def gather_kernel(count, causal, in_ref, out_ref, send_sem, recv_sem):
    me, column, across, partner = places()
    diagonal = lax.rem(partner + lax.axis_size("tp") // 2, lax.axis_size("tp"))
    greet(count, me, column, (across, partner))

    def own(p):
        return in_ref.at[0] if causal else in_ref.at[p]

    def over_sp(k):
        p = lax.rem(me + k, count)
        return send(
            own(p), out_ref.at[me, column], send_sem.at[0, k], recv_sem.at[0, me], (p, column)
        )

    def arrival(kind, s, t):
        block = out_ref.at[s, t]
        return send(block, block, send_sem.at[kind, s], recv_sem.at[kind, s], (me, partner))

    def pass_on(s, source):
        target = out_ref.at[s, column]
        return (
            send(source, target, send_sem.at[1, s], recv_sem.at[1, s], (me, across)),
            send(source, target, send_sem.at[2, s], recv_sem.at[2, s], (me, partner)),
        )

    def to_partner(s):
        block = out_ref.at[s, across]
        return send(block, block, send_sem.at[3, s], recv_sem.at[3, s], (me, partner))

    last = count - me if causal else count
    arrivals = me + 1 if causal else count

    loop(1, last, lambda k: over_sp(last - k).start())
    for copy in pass_on(me, own(me)):
        copy.start()
    out_ref[me, column] = in_ref[0] if causal else in_ref[me]
    if causal:

        def clear(s):
            out_ref[s] = jnp.zeros(out_ref.shape[1:], out_ref.dtype)

        loop(me + 1, count, clear)

    def origin(k):
        return lax.rem(me + count - k, count)

    def arrived(k):
        s = origin(k)
        arrival(0, s, column).wait_recv()
        for copy in pass_on(s, out_ref.at[s, column]):
            copy.start()

    loop(1, arrivals, arrived)

    def crossed(k):
        s = origin(k)
        arrival(1, s, across).wait_recv()
        to_partner(s).start()

    loop(0, arrivals, crossed)

    def settle(k):
        s = origin(k)
        arrival(2, s, partner).wait_recv()
        arrival(3, s, diagonal).wait_recv()
        for copy in pass_on(s, out_ref.at[s, column]):
            copy.wait_send()
        to_partner(s).wait_send()

    loop(0, arrivals, settle)
    loop(1, last, lambda k: over_sp(k).wait_send())


def gather(blocks, count, columns, causal, collective_id):
    return pl.pallas_call(
        functools.partial(gather_kernel, count, causal),
        out_shape=jax.ShapeDtypeStruct((count, columns) + blocks.shape[1:], blocks.dtype),
        in_specs=[pl.BlockSpec(memory_space=pltpu.VMEM)],
        out_specs=pl.BlockSpec(memory_space=pltpu.VMEM),
        scratch_shapes=[
            pltpu.SemaphoreType.DMA((4, count)),
            pltpu.SemaphoreType.DMA((4, count)),
        ],
        compiler_params=pltpu.CompilerParams(
            collective_id=collective_id, has_side_effects=True, vmem_limit_bytes=60000 * 1024
        ),
    )(blocks)


def hidden_kernel(
    columns, part_ref, residual_ref, gain_ref, pick_ref, hidden_ref, outgoing_ref, held, send_sem, recv_sem
):
    me, column, _, _ = places()
    others = [lax.rem(column + k, columns) for k in range(1, columns)]
    greet(1, me, column, others)
    copies = []
    for k, other in enumerate(others):
        copies.append(
            send(part_ref.at[other], held.at[k], send_sem.at[k], recv_sem.at[k], (me, other))
        )
    for copy in copies:
        copy.start()
    total = residual_ref[...].astype(jnp.float32) + part_ref[column].astype(jnp.float32)
    for k, copy in enumerate(copies):
        copy.wait_recv()
        total = total + held[k].astype(jnp.float32)
    hidden = total.astype(jnp.bfloat16)
    hidden_ref[...] = hidden
    normed = rms_scale(hidden, gain_ref[...])
    outgoing = jnp.dot(pick_ref[...], normed, preferred_element_type=jnp.float32)
    outgoing_ref[...] = outgoing.astype(jnp.bfloat16)
    for copy in copies:
        copy.wait_send()


def hidden_sum(parts, residual, gain, selection, collective_id):
    columns, rows, width = parts.shape
    return pl.pallas_call(
        functools.partial(hidden_kernel, columns),
        out_shape=[
            jax.ShapeDtypeStruct((rows, width), jnp.bfloat16),
            jax.ShapeDtypeStruct((selection.shape[0], width), jnp.bfloat16),
        ],
        in_specs=[pl.BlockSpec(memory_space=pltpu.VMEM)] * 4,
        out_specs=[pl.BlockSpec(memory_space=pltpu.VMEM)] * 2,
        scratch_shapes=[
            pltpu.VMEM((columns - 1, rows, width), jnp.bfloat16),
            pltpu.SemaphoreType.DMA((columns - 1,)),
            pltpu.SemaphoreType.DMA((columns - 1,)),
        ],
        compiler_params=pltpu.CompilerParams(
            collective_id=collective_id, has_side_effects=True, vmem_limit_bytes=60000 * 1024
        ),
    )(parts, residual, gain.reshape(1, width), selection)


def return_kernel(
    count, in_ref, out_ref, from_partner, pair, mine, from_across, done, send_sem, recv_sem
):
    me, column, across, partner = places()
    diagonal = lax.rem(partner + lax.axis_size("tp") // 2, lax.axis_size("tp"))
    greet(count, me, column, (across, partner))

    def place(k):
        return lax.rem(me + 1 + k, count)

    def to_partner(s, slot):
        wanted = (partner, diagonal)[slot]
        return send(
            in_ref.at[s, wanted],
            from_partner.at[slot, s],
            send_sem.at[slot, s],
            recv_sem.at[slot, s],
            (me, partner),
        )

    def over_x(s):
        return send(
            pair.at[s], from_across.at[s], send_sem.at[2, s], recv_sem.at[2, s], (me, across)
        )

    def back(s):
        return send(
            done.at[s], out_ref.at[me], send_sem.at[3, s], recv_sem.at[3, me], (s, column)
        )

    def start(k):
        s = place(k)
        to_partner(s, 1).start()
        to_partner(s, 0).start()

    loop(0, count, start)

    def both(s, slot):
        kept = in_ref[s, (column, across)[slot]].astype(jnp.float32)
        return kept + from_partner[slot, s].astype(jnp.float32)

    def paired(k):
        s = place(k)
        to_partner(s, 1).wait_recv()
        pair[s] = both(s, 1).astype(jnp.bfloat16)
        over_x(s).start()

    loop(0, count, paired)

    def total(s):
        to_partner(s, 0).wait_recv()
        mine[...] = both(s, 0)
        over_x(s).wait_recv()
        return (mine[...] + from_across[s].astype(jnp.float32)).astype(jnp.bfloat16)

    def summed(k):
        s = place(k)
        done[s] = total(s)
        back(s).start()

    loop(0, count - 1, summed)
    out_ref[me] = total(me)

    def arrived(k):
        s = place(k)
        send(
            done.at[s], out_ref.at[s], send_sem.at[3, s], recv_sem.at[3, s], (s, column)
        ).wait_recv()
        back(s).wait_send()

    loop(0, count - 1, arrived)

    def settle(s):
        to_partner(s, 0).wait_send()
        to_partner(s, 1).wait_send()
        over_x(s).wait_send()

    loop(0, count, settle)


def give_back(partials, collective_id):
    count, _, rows, width = partials.shape
    block = (count, rows, width)
    return pl.pallas_call(
        functools.partial(return_kernel, count),
        out_shape=jax.ShapeDtypeStruct(block, jnp.bfloat16),
        in_specs=[pl.BlockSpec(memory_space=pltpu.VMEM)],
        out_specs=pl.BlockSpec(memory_space=pltpu.VMEM),
        scratch_shapes=[
            pltpu.VMEM((2,) + block, jnp.bfloat16),
            pltpu.VMEM(block, jnp.bfloat16),
            pltpu.VMEM(block[1:], jnp.float32),
            pltpu.VMEM(block, jnp.bfloat16),
            pltpu.VMEM(block, jnp.bfloat16),
            pltpu.SemaphoreType.DMA((4, count)),
            pltpu.SemaphoreType.DMA((4, count)),
        ],
        compiler_params=pltpu.CompilerParams(
            collective_id=collective_id, has_side_effects=True, vmem_limit_bytes=60000 * 1024
        ),
    )(partials)


def experts_kernel(
    count,
    group,
    in_ref,
    selector_ref,
    share_ref,
    hidden_ref,
    gate_hbm,
    up_hbm,
    down_hbm,
    out_ref,
    rows,
    part,
    from_partner,
    pair,
    from_across,
    done,
    returned,
    gate,
    up,
    down,
    weight_sem,
    send_sem,
    recv_sem,
):
    me, column, across, partner = places()
    diagonal = lax.rem(partner + lax.axis_size("tp") // 2, lax.axis_size("tp"))
    loads = [
        pltpu.make_async_copy(source.at[0], target, weight_sem.at[index])
        for index, (source, target) in enumerate(((gate_hbm, gate), (up_hbm, up), (down_hbm, down)))
    ]
    for load in loads:
        load.start()
    greet(count, me, column, (across, partner))

    def origin(k):
        return lax.rem(me + count - k, count)

    def over_sp(k):
        p = lax.rem(me + k, count)
        return send(
            in_ref.at[p], rows.at[me, column], send_sem.at[0, k], recv_sem.at[0, me], (p, column)
        )

    def arrival(kind, s, t):
        block = rows.at[s, t]
        return send(block, block, send_sem.at[kind, s], recv_sem.at[kind, s], (me, partner))

    def pass_on(s, source):
        target = rows.at[s, column]
        return (
            send(source, target, send_sem.at[1, s], recv_sem.at[1, s], (me, across)),
            send(source, target, send_sem.at[2, s], recv_sem.at[2, s], (me, partner)),
        )

    def cross_on(s):
        block = rows.at[s, across]
        return send(block, block, send_sem.at[3, s], recv_sem.at[3, s], (me, partner))

    def to_partner(s, slot):
        wanted = (partner, diagonal)[slot]
        return send(
            part.at[s, wanted],
            from_partner.at[slot, s],
            send_sem.at[4 + slot, s],
            recv_sem.at[4 + slot, s],
            (me, partner),
        )

    def over_x(s):
        return send(
            pair.at[s], from_across.at[s], send_sem.at[6, s], recv_sem.at[6, s], (me, across)
        )

    def back(s):
        return send(
            done.at[s], returned.at[me], send_sem.at[7, s], recv_sem.at[7, me], (s, column)
        )

    loop(1, count, lambda k: over_sp(k).start())
    for copy in pass_on(me, in_ref.at[me]):
        copy.start()
    rows[me, column] = in_ref[me]

    def arrived(k):
        s = origin(k)
        arrival(0, s, column).wait_recv()
        for copy in pass_on(s, rows.at[s, column]):
            copy.start()

    def both(s, slot):
        kept = part[s, (column, across)[slot]].astype(jnp.float32)
        return kept + from_partner[slot, s].astype(jnp.float32)

    def paired(k):
        s = origin(k)
        to_partner(s, 1).wait_recv()
        pair[s] = both(s, 1).astype(jnp.bfloat16)
        over_x(s).start()

    def summed(k):
        s = origin(k)
        to_partner(s, 0).wait_recv()
        over_x(s).wait_recv()
        total = (both(s, 0) + from_across[s].astype(jnp.float32)).astype(jnp.bfloat16)

        @pl.when(k == 0)
        def _():
            returned[me] = total

        @pl.when(k > 0)
        def _():
            done[s] = total
            back(s).start()

    loop(1, group, arrived)
    block_rows = rows.shape[1] * rows.shape[2]
    width = rows.shape[3]

    def turn(j):
        first = j * group

        @pl.when(first + group < count)
        def _():
            loop(first + group, first + 2 * group, arrived)

        def crossed(k):
            s = origin(k)
            arrival(1, s, across).wait_recv()
            cross_on(s).start()

        loop(first, first + group, crossed)

        def whole(k):
            s = origin(k)
            arrival(2, s, partner).wait_recv()
            arrival(3, s, diagonal).wait_recv()

        loop(first, first + group, whole)

        @pl.when(j == 0)
        def _():
            for load in loads:
                load.wait()

        sources = [origin(first + i) for i in range(group)]
        flat = jnp.concatenate([rows[s].reshape(block_rows, width) for s in sources], axis=0)
        gate_values = jnp.dot(flat, gate[...], preferred_element_type=jnp.float32)
        up_values = jnp.dot(flat, up[...], preferred_element_type=jnp.float32)
        hidden = (jax.nn.silu(gate_values) * up_values).astype(jnp.bfloat16)
        product = jnp.dot(hidden, down[...], preferred_element_type=jnp.float32)
        product = product.astype(jnp.bfloat16)
        for i, s in enumerate(sources):
            part[s] = product[i * block_rows : (i + 1) * block_rows].reshape(rows.shape[1:])

        def leave(k):
            s = origin(k)
            to_partner(s, 1).start()
            to_partner(s, 0).start()

        loop(first, first + group, leave)

        @pl.when(j > 0)
        def _():
            loop(first - group, first, paired)

        @pl.when(j > 1)
        def _():
            loop(first - 2 * group, first - group, summed)

    turns = count // group
    loop(0, turns, turn)
    loop(count - group, count, paired)
    loop(max(turns - 2, 0) * group, count, summed)

    def home(k):
        s = origin(k)
        send(
            done.at[s], returned.at[s], send_sem.at[7, s], recv_sem.at[7, s], (s, column)
        ).wait_recv()
        back(s).wait_send()

    loop(1, count, home)
    picked = jnp.dot(
        selector_ref[...], returned[...].reshape(-1, width), preferred_element_type=jnp.float32
    )
    own_rows = hidden_ref.shape[0]
    mixed = jnp.zeros(hidden_ref.shape, jnp.float32)
    for route_index in range(TOP):
        mixed = mixed + (
            share_ref[:, route_index : route_index + 1]
            * picked[route_index * own_rows : (route_index + 1) * own_rows]
        )
    out_ref[...] = (hidden_ref[...].astype(jnp.float32) + mixed).astype(jnp.bfloat16)

    def settle(s):
        for copy in pass_on(s, rows.at[s, column]):
            copy.wait_send()
        cross_on(s).wait_send()
        to_partner(s, 0).wait_send()
        to_partner(s, 1).wait_send()
        over_x(s).wait_send()

    loop(0, count, settle)
    loop(1, count, lambda k: over_sp(k).wait_send())


def through_experts(outgoing, selector, share, hidden, gate, up, down, columns, collective_id):
    count, rows, width = outgoing.shape
    group = 2 if count % 2 == 0 else 1
    block = (count, rows, width)
    every = (count, columns, rows, width)
    return pl.pallas_call(
        functools.partial(experts_kernel, count, group),
        out_shape=jax.ShapeDtypeStruct(hidden.shape, jnp.bfloat16),
        in_specs=[pl.BlockSpec(memory_space=pltpu.VMEM)] * 4
        + [pl.BlockSpec(memory_space=pl.ANY)] * 3,
        out_specs=pl.BlockSpec(memory_space=pltpu.VMEM),
        scratch_shapes=[
            pltpu.VMEM(every, jnp.bfloat16),
            pltpu.VMEM(every, jnp.bfloat16),
            pltpu.VMEM((2,) + block, jnp.bfloat16),
            pltpu.VMEM(block, jnp.bfloat16),
            pltpu.VMEM(block, jnp.bfloat16),
            pltpu.VMEM(block, jnp.bfloat16),
            pltpu.VMEM(block, jnp.bfloat16),
            pltpu.VMEM(gate.shape[1:], jnp.bfloat16),
            pltpu.VMEM(up.shape[1:], jnp.bfloat16),
            pltpu.VMEM(down.shape[1:], jnp.bfloat16),
            pltpu.SemaphoreType.DMA((3,)),
            pltpu.SemaphoreType.DMA((8, count)),
            pltpu.SemaphoreType.DMA((8, count)),
        ],
        compiler_params=pltpu.CompilerParams(
            collective_id=collective_id, has_side_effects=True, vmem_limit_bytes=60000 * 1024
        ),
    )(outgoing, selector, share, hidden, gate, up, down)


def turn_tables(positions, rotary_width):
    inverse = np.power(
        np.float32(base_theta), -np.arange(0, rotary_width, 2, dtype=np.float32) / rotary_width
    ).astype(np.float32)
    angles = positions.astype(np.float32)[:, None] * inverse[None, :]
    cosine, sine = np.cos(angles), np.sin(angles)
    return np.concatenate([cosine, cosine, -sine, sine], axis=1).astype(np.float32)


def iotas(shape):
    return (
        lax.broadcasted_iota(jnp.int32, shape, 0),
        lax.broadcasted_iota(jnp.int32, shape, 1),
    )


def dot(left, right):
    return jnp.dot(left, right, preferred_element_type=jnp.float32)


def dot_over(left, right, left_dim, right_dim):
    return lax.dot_general(
        left, right, (((left_dim,), (right_dim,)), ((), ())), preferred_element_type=jnp.float32
    )


def layer_kernel(
    count,
    columns,
    heads_a,
    heads_b,
    query_a_hbm,
    query_b_hbm,
    latent_hbm,
    rope_hbm,
    latent_gain_hbm,
    key_a_hbm,
    value_a_hbm,
    key_b_hbm,
    value_b_hbm,
    out_a_hbm,
    out_b_hbm,
    residual_hbm,
    ffn_gain_hbm,
    routes_hbm,
    share_hbm,
    table_hbm,
    gate_hbm,
    up_hbm,
    down_hbm,
    out_ref,
    query_a,
    query_b,
    latent,
    rope,
    latent_gain,
    key_a,
    value_a,
    key_b,
    value_b,
    out_a,
    out_b,
    residual,
    ffn_gain,
    routes,
    share,
    own_table,
    query_table,
    gate,
    up,
    down,
    own,
    gathered,
    key_weight,
    keys,
    values,
    head_part,
    head_pair,
    head_from_partner,
    head_from_across,
    hidden,
    outgoing,
    rows,
    part,
    from_partner,
    pair,
    from_across,
    done,
    returned,
    load_sem,
    gather_send,
    gather_recv,
    sum_send,
    sum_recv,
    send_sem,
    recv_sem,
):
    me, column, across, partner = places()
    diagonal = lax.rem(partner + columns // 2, columns)
    row_count = latent.shape[0]
    span = query_a.shape[0]
    rank = latent.shape[1]
    rotary = rope.shape[1]
    width = residual.shape[1]
    total = count * span

    own_first = pl.multiple_of((me * columns + column) * row_count, row_count)
    query_first = pl.multiple_of(me * span, span)
    plan = [
        (latent_hbm, latent),
        (rope_hbm, rope),
        (latent_gain_hbm, latent_gain),
        (table_hbm.at[pl.ds(own_first, row_count)], own_table),
        (key_a_hbm, key_a),
        (key_b_hbm, key_b),
        (query_a_hbm, query_a),
        (query_b_hbm, query_b),
        (table_hbm.at[pl.ds(query_first, span)], query_table),
        (value_a_hbm, value_a),
        (value_b_hbm, value_b),
        (routes_hbm, routes),
        (share_hbm, share),
        (out_a_hbm, out_a),
        (out_b_hbm, out_b),
        (residual_hbm, residual),
        (ffn_gain_hbm, ffn_gain),
        (gate_hbm.at[0], gate),
        (up_hbm.at[0], up),
        (down_hbm.at[0], down),
    ]
    loads = [
        pltpu.make_async_copy(source, target, load_sem.at[index])
        for index, (source, target) in enumerate(plan)
    ]
    for load in loads:
        load.start()

    barrier = pltpu.get_barrier_semaphore()

    def hello(k, carry):
        pl.semaphore_signal(
            barrier,
            inc=1,
            device_id={"sp": lax.rem(me + k, count), "tp": column},
            device_id_type=MESH,
        )
        return carry

    lax.fori_loop(1, count, hello, 0)
    for other in (across, partner):
        pl.semaphore_signal(
            barrier, inc=1, device_id={"sp": me, "tp": other}, device_id_type=MESH
        )

    for load in loads[:4]:
        load.wait()
    row, col = iotas((128, 128))
    swap = (row == jnp.where(jnp.bitwise_and(col, rotary - 1) < rotary // 2, col + rotary // 2, col - rotary // 2))
    swap = swap.astype(jnp.bfloat16)
    own[:, :rank] = rms_scale(latent[...], latent_gain[...])
    key = rope[...]
    turned = key.astype(jnp.float32) * own_table[:, :rotary] + (
        dot(key, swap[:rotary, :rotary]) * own_table[:, rotary:]
    )
    own[:, rank : rank + rotary] = turned.astype(jnp.bfloat16)
    own[:, rank + rotary :] = jnp.zeros(
        (row_count, own.shape[1] - rank - rotary), jnp.bfloat16
    )
    pl.semaphore_wait(barrier, count + 1)

    def g_over_sp(k):
        p = lax.rem(me + k, count)
        return send(
            own, gathered.at[me, column], gather_send.at[0, k], gather_recv.at[0, me], (p, column)
        )

    def g_arrival(kind, s, t):
        block = gathered.at[s, t]
        return send(
            block, block, gather_send.at[kind, s], gather_recv.at[kind, s], (me, partner)
        )

    def g_pass_on(s, source):
        target = gathered.at[s, column]
        return (
            send(source, target, gather_send.at[1, s], gather_recv.at[1, s], (me, across)),
            send(source, target, gather_send.at[2, s], gather_recv.at[2, s], (me, partner)),
        )

    def g_to_partner(s):
        block = gathered.at[s, across]
        return send(
            block, block, gather_send.at[3, s], gather_recv.at[3, s], (me, partner)
        )

    last = count - me
    for copy in g_pass_on(me, own):
        copy.start()
    loop(1, last, lambda k: g_over_sp(last - k).start())
    gathered[me, column] = own[...]

    def clear(s):
        values[s] = jnp.zeros(values.shape[1:], values.dtype)
        keys[s] = jnp.zeros(keys.shape[1:], keys.dtype)

    loop(me + 1, count, clear)

    for load in loads[4:11]:
        load.wait()
    nope_a = key_a.shape[1] // heads_a
    nope_b = key_b.shape[1] // heads_b
    wide_a = 256
    wide_b = nope_b + rotary
    starts_a = []
    for h in range(heads_a):
        at = h * (nope_a + rotary)
        starts_a.append(at // 128 * 128)
        pad = at - starts_a[h]
        r, c = iotas((key_a.shape[1], wide_a))
        inside = (c >= pad) & (c < pad + nope_a)
        piece = ((r - c == h * nope_a - pad) & inside).astype(jnp.bfloat16)
        lanes = slice(h * wide_a, (h + 1) * wide_a)
        key_weight[:rank, lanes] = dot(key_a[...], piece).astype(jnp.bfloat16)
        r, c = iotas((own.shape[1] - rank, wide_a))
        key_weight[rank:, lanes] = ((c - r == pad + nope_a) & (r < rotary)).astype(jnp.bfloat16)
    base_b = heads_a * wide_a
    for h in range(heads_b):
        r, c = iotas((key_b.shape[1], wide_b))
        piece = ((r - c == h * nope_b) & (c < nope_b)).astype(jnp.bfloat16)
        lanes = slice(base_b + h * wide_b, base_b + (h + 1) * wide_b)
        key_weight[:rank, lanes] = dot(key_b[...], piece).astype(jnp.bfloat16)
        r, c = iotas((own.shape[1] - rank, wide_b))
        key_weight[rank:, lanes] = ((c - r == nope_b) & (r < rotary)).astype(jnp.bfloat16)

    lane = lax.broadcasted_iota(jnp.int32, (span, 128), 1)
    table = query_table[...]
    rolled = jnp.concatenate([table[:, rotary:], table[:, :rotary]], axis=1)
    low = lane < rotary
    one = jnp.ones((span, 128), jnp.float32)
    zero = jnp.zeros((span, 128), jnp.float32)
    turn_low = (jnp.where(low, table, one), jnp.where(low, rolled, zero))
    turn_high = (jnp.where(low, one, rolled), jnp.where(low, zero, table))

    def turn_tile(ref, at, factors):
        tile = ref[:, at : at + 128]
        turned_tile = tile.astype(jnp.float32) * factors[0] + dot(tile, swap) * factors[1]
        ref[:, at : at + 128] = turned_tile.astype(jnp.bfloat16)

    for h in range(heads_a):
        at = h * (nope_a + rotary) + nope_a
        turn_tile(query_a, at // 128 * 128, turn_low if at % 128 == 0 else turn_high)
    for h in range(heads_b):
        turn_tile(query_b, h * wide_b, turn_high)

    def origin(k):
        return me - k

    def g_step(k):
        @pl.when((k > 0) & (k <= me))
        def _():
            s = origin(k)
            g_arrival(0, s, column).wait_recv()
            for copy in g_pass_on(s, gathered.at[s, column]):
                copy.start()

        @pl.when((k >= 1) & (k <= me + 1))
        def _():
            s = origin(k - 1)
            g_arrival(1, s, across).wait_recv()
            g_to_partner(s).start()

        @pl.when(k >= 2)
        def _():
            s = origin(k - 2)
            g_arrival(2, s, partner).wait_recv()
            g_arrival(3, s, diagonal).wait_recv()
            packed = gathered[s].reshape(span, own.shape[1])
            keys[s] = dot(packed, key_weight[...]).astype(jnp.bfloat16)
            values[s, :, : value_a.shape[1]] = dot(packed[:, :rank], value_a[...]).astype(
                jnp.bfloat16
            )
            values[s, :, value_a.shape[1] :] = dot(packed[:, :rank], value_b[...]).astype(
                jnp.bfloat16
            )

    loop(0, me + 3, g_step)

    query_at, key_at = iotas((span, total))
    allowed = key_at <= query_at + query_first

    def weigh(queries, lanes, size):
        scores = dot_over(queries, keys[:, :, lanes].reshape(total, -1), 1, 1)
        scores = jnp.where(allowed, scores, masked_score)
        top = jnp.max(scores, axis=1, keepdims=True)
        weights = jnp.exp((scores - top) * size ** (-0.5))
        return weights.astype(jnp.bfloat16), jnp.sum(weights, axis=1, keepdims=True)

    def attend(parts, lanes, each):
        group = values[:, :, lanes].reshape(total, -1)
        results = [dot(weights, group) / sums for weights, sums in parts]
        result = results[0]
        at = lax.broadcasted_iota(jnp.int32, result.shape, 1)
        for h in range(1, len(parts)):
            result = jnp.where(at < h * each, result, results[h])
        return result.astype(jnp.bfloat16)

    for load in loads[11:17]:
        load.wait()
    mixed_a = attend(
        [
            weigh(
                query_a[:, starts_a[h] : starts_a[h] + wide_a],
                slice(h * wide_a, (h + 1) * wide_a),
                nope_a + rotary,
            )
            for h in range(heads_a)
        ],
        slice(0, value_a.shape[1]),
        value_a.shape[1] // heads_a,
    )
    mixed_b = attend(
        [
            weigh(
                query_b[:, h * wide_b : (h + 1) * wide_b],
                slice(base_b + h * wide_b, base_b + (h + 1) * wide_b),
                wide_b,
            )
            for h in range(heads_b)
        ],
        slice(value_a.shape[1], value_a.shape[1] + value_b.shape[1]),
        value_b.shape[1] // heads_b,
    )

    chunks = head_part.shape[0]
    chunk_width = head_part.shape[3]

    def s_partner(c, slot):
        return send(
            head_part.at[c, (partner, diagonal)[slot]],
            head_from_partner.at[c, slot],
            sum_send.at[slot, c],
            sum_recv.at[slot, c],
            (me, partner),
        )

    def s_across(c):
        return send(
            head_pair.at[c], head_from_across.at[c], sum_send.at[2, c], sum_recv.at[2, c], (me, across)
        )

    for c in range(chunks):
        lanes = slice(c * chunk_width, (c + 1) * chunk_width)
        product = dot(mixed_a, out_a[:, lanes]) + dot(mixed_b, out_b[:, lanes])
        head_part[c] = product.astype(jnp.bfloat16).reshape(head_part.shape[1:])
        s_partner(c, 1).start()
        s_partner(c, 0).start()
    for c in range(chunks):
        s_partner(c, 1).wait_recv()
        both = head_part[c, across].astype(jnp.float32) + head_from_partner[c, 1].astype(jnp.float32)
        head_pair[c] = both.astype(jnp.bfloat16)
        s_across(c).start()

    capacity = outgoing.shape[1]
    slots = count * capacity
    expert_at = lax.broadcasted_iota(jnp.int32, (count, row_count), 0)
    before = iotas((row_count, row_count))
    before = (before[0] < before[1]).astype(jnp.bfloat16)
    slot_at = lax.broadcasted_iota(jnp.int32, (slots, row_count), 0)
    earlier = jnp.zeros((count, 1), jnp.float32)
    picks = []
    for k in range(TOP):
        expert = routes[k : k + 1, :]
        named = (expert_at == expert).astype(jnp.float32)
        place = dot(named.astype(jnp.bfloat16), before) + earlier
        place = jnp.sum(place * named, axis=0, keepdims=True).astype(jnp.int32)
        picks.append((slot_at == expert * capacity + place).astype(jnp.float32))
        earlier = earlier + jnp.sum(named, axis=1, keepdims=True)
    selection = functools.reduce(lambda a, b: a + b, picks).astype(jnp.bfloat16)
    mixing = functools.reduce(
        lambda a, b: a + b, [pick * share[k : k + 1, :] for k, pick in enumerate(picks)]
    )

    squares = jnp.zeros((row_count, 1), jnp.float32)
    for c in range(chunks):
        lanes = slice(c * chunk_width, (c + 1) * chunk_width)
        s_partner(c, 0).wait_recv()
        summed_rows = (
            residual[:, lanes].astype(jnp.float32)
            + head_part[c, column].astype(jnp.float32)
            + head_from_partner[c, 0].astype(jnp.float32)
        )
        s_across(c).wait_recv()
        summed_rows = summed_rows + head_from_across[c].astype(jnp.float32)
        hidden[:, lanes] = summed_rows.astype(jnp.bfloat16)
    normed = rms_scale(hidden[...], ffn_gain[...])
    outgoing[...] = dot(selection, normed).astype(jnp.bfloat16).reshape(outgoing.shape)

    def peer(k):
        result = 0
        bit = 1
        while bit < count:
            mine = lax.rem(me // bit, 2)
            other = lax.rem(k // bit, 2)
            result = result + bit * lax.rem(mine + other, 2)
            bit *= 2
        return result

    def over_sp(k):
        p = peer(k)
        return send(
            outgoing.at[p], rows.at[k, column], send_sem.at[0, k], recv_sem.at[0, k], (p, column)
        )

    def pass_on(k, source):
        target = rows.at[k, column]
        return (
            send(source, target, send_sem.at[1, k], recv_sem.at[1, k], (me, across)),
            send(source, target, send_sem.at[2, k], recv_sem.at[2, k], (me, partner)),
        )

    def arrival(kind, k, t):
        block = rows.at[k, t]
        return send(block, block, send_sem.at[kind, k], recv_sem.at[kind, k], (me, partner))

    def cross_on(k):
        block = rows.at[k, across]
        return send(block, block, send_sem.at[3, k], recv_sem.at[3, k], (me, partner))

    def to_partner(k, slot):
        wanted = (partner, diagonal)[slot]
        return send(
            part.at[k, wanted],
            from_partner.at[slot, k],
            send_sem.at[4 + slot, k],
            recv_sem.at[4 + slot, k],
            (me, partner),
        )

    def over_x(k):
        return send(
            pair.at[k], from_across.at[k], send_sem.at[6, k], recv_sem.at[6, k], (me, across)
        )

    def back(k):
        p = peer(k)
        return send(
            done.at[k], returned.at[me], send_sem.at[7, k], recv_sem.at[7, k], (p, column)
        )

    for copy in pass_on(0, outgoing.at[me]):
        copy.start()
    loop(1, count, lambda k: over_sp(k).start())
    rows[0, column] = outgoing[me]

    def arrived(k):
        arrival(0, k, column).wait_recv()
        for copy in pass_on(k, rows.at[k, column]):
            copy.start()

    def crossed(k):
        arrival(1, k, across).wait_recv()
        cross_on(k).start()

    def whole(k):
        arrival(2, k, partner).wait_recv()
        arrival(3, k, diagonal).wait_recv()

    def both_of(k, slot):
        kept = part[k, (column, across)[slot]].astype(jnp.float32)
        return kept + from_partner[slot, k].astype(jnp.float32)

    def paired(k):
        to_partner(k, 1).wait_recv()
        pair[k] = both_of(k, 1).astype(jnp.bfloat16)
        over_x(k).start()

    def summed(k):
        to_partner(k, 0).wait_recv()
        over_x(k).wait_recv()
        result = (both_of(k, 0) + from_across[k].astype(jnp.float32)).astype(jnp.bfloat16)

        @pl.when(k == 0)
        def _():
            returned[me] = result

        @pl.when(k > 0)
        def _():
            done[k] = result
            back(k).start()

    group = 2
    block_rows = rows.shape[1] * rows.shape[2]
    loop(1, group, arrived)
    for load in loads[17:]:
        load.wait()

    def turn(j):
        first = j * group

        @pl.when(first + group < count)
        def _():
            loop(first + group, first + 2 * group, arrived)

        loop(first, first + group, crossed)

        @pl.when(j > 0)
        def _():
            loop(first - group, first, paired)

        @pl.when(j > 1)
        def _():
            loop(first - 2 * group, first - group, summed)

        loop(first, first + group, whole)
        flat = rows[pl.ds(first, group)].reshape(group * block_rows, width)
        gate_values = dot(flat, gate[...])
        up_values = dot(flat, up[...])
        act = (jax.nn.silu(gate_values) * up_values).astype(jnp.bfloat16)
        product = dot(act, down[...]).astype(jnp.bfloat16)
        part[pl.ds(first, group)] = product.reshape((group,) + part.shape[1:])

        def leave(k):
            to_partner(k, 1).start()
            to_partner(k, 0).start()

        loop(first, first + group, leave)

    turns = count // group
    loop(0, turns, turn)
    loop(count - group, count, paired)
    loop(max(turns - 2, 0) * group, count, summed)

    def home(k):
        p = peer(k)
        send(
            done.at[k], returned.at[p], send_sem.at[7, k], recv_sem.at[7, k], (p, column)
        ).wait_recv()

    loop(1, count, home)
    flat_returned = returned[...].reshape(slots, width)
    mixing_high = mixing.astype(jnp.bfloat16)
    mixing_low = (mixing - mixing_high.astype(jnp.float32)).astype(jnp.bfloat16)
    mixed = dot_over(mixing_high, flat_returned, 0, 0) + dot_over(mixing_low, flat_returned, 0, 0)
    out_ref[...] = (hidden[...].astype(jnp.float32) + mixed).astype(jnp.bfloat16)

    def g_settle(k):
        s = origin(k)
        for copy in g_pass_on(s, gathered.at[s, column]):
            copy.wait_send()
        g_to_partner(s).wait_send()

    loop(0, me + 1, g_settle)
    loop(1, last, lambda k: g_over_sp(k).wait_send())
    for c in range(chunks):
        s_partner(c, 0).wait_send()
        s_partner(c, 1).wait_send()
        s_across(c).wait_send()

    def settle(k):
        for copy in pass_on(k, rows.at[k, column]):
            copy.wait_send()
        cross_on(k).wait_send()
        to_partner(k, 0).wait_send()
        to_partner(k, 1).wait_send()
        over_x(k).wait_send()

    loop(0, count, settle)

    def settle_far(k):
        over_sp(k).wait_send()
        back(k).wait_send()

    loop(1, count, settle_far)


def whole_layer(
    query_a,
    query_b,
    latent,
    rope_key,
    latent_gain,
    key_a_weight,
    value_a_weight,
    key_b_weight,
    value_b_weight,
    out_a_weight,
    out_b_weight,
    residual,
    ffn_gain,
    routes,
    route_weight,
    expert_gate,
    expert_up,
    expert_down,
    capacity,
):
    count, columns = lax.axis_size("sp"), lax.axis_size("tp")
    row_count, rank = latent.shape
    rotary = rope_key.shape[1]
    span = query_a.shape[0]
    width = residual.shape[1]
    heads_a = key_a_weight.shape[1] // NOPE_A
    heads_b = key_b_weight.shape[1] // NOPE_B
    table = jnp.asarray(turn_tables(np.arange(count * span), rotary))
    packed = rank + rotary + (-(rank + rotary) % 128)
    key_width = heads_a * 256 + heads_b * (NOPE_B + rotary)
    value_width = value_a_weight.shape[1] + value_b_weight.shape[1]
    chunks = 4
    chunk_width = width // chunks
    block = (count, capacity, width)
    every = (count, columns, capacity, width)
    operands = (
        query_a,
        query_b,
        latent,
        rope_key,
        latent_gain.reshape(1, rank),
        key_a_weight,
        value_a_weight,
        key_b_weight,
        value_b_weight,
        out_a_weight,
        out_b_weight,
        residual,
        ffn_gain.reshape(1, width),
        routes.T,
        route_weight.T,
        table,
        expert_gate,
        expert_up,
        expert_down,
    )
    bf16 = jnp.bfloat16

    def room(shape, dtype=bf16):
        return pltpu.VMEM(shape, dtype)

    loaded = [room(operand.shape, operand.dtype) for operand in operands[:15]]
    loaded += [room((row_count, 2 * rotary), jnp.float32), room((span, 2 * rotary), jnp.float32)]
    loaded += [room(operand.shape[1:], operand.dtype) for operand in operands[16:]]
    dma = pltpu.SemaphoreType.DMA
    return pl.pallas_call(
        functools.partial(layer_kernel, count, columns, heads_a, heads_b),
        out_shape=jax.ShapeDtypeStruct(residual.shape, bf16),
        in_specs=[pl.BlockSpec(memory_space=pl.ANY)] * len(operands),
        out_specs=pl.BlockSpec(memory_space=pltpu.VMEM),
        scratch_shapes=loaded
        + [
            room((row_count, packed)),
            room((count, columns, row_count, packed)),
            room((packed, key_width)),
            room((count, span, key_width)),
            room((count, span, value_width)),
            room((chunks, columns, row_count, chunk_width)),
            room((chunks, row_count, chunk_width)),
            room((chunks, 2, row_count, chunk_width)),
            room((chunks, row_count, chunk_width)),
            room(residual.shape),
            room(block),
            room(every),
            room(every),
            room((2,) + block),
            room(block),
            room(block),
            room(block),
            room(block),
            dma((len(operands) + 1,)),
            dma((4, count)),
            dma((4, count)),
            dma((3, chunks)),
            dma((3, chunks)),
            dma((8, count)),
            dma((8, count)),
        ],
        compiler_params=pltpu.CompilerParams(
            collective_id=5, has_side_effects=True, vmem_limit_bytes=60000 * 1024
        ),
    )(*operands)


def body(
    query_a,
    query_b,
    latent,
    rope_key,
    latent_gain,
    key_a_weight,
    value_a_weight,
    key_b_weight,
    value_b_weight,
    out_a_weight,
    out_b_weight,
    residual,
    ffn_gain,
    routes,
    route_weight,
    expert_gate,
    expert_up,
    expert_down,
):
    column_count = lax.axis_size("tp")
    row_count = latent.shape[0]
    experts = lax.axis_size("sp")
    capacity = max(2, 2 * TOP * row_count // experts)
    paired_up = experts & (experts - 1) == 0 and experts > 1 and column_count == 4
    if capacity % 16 == 0 and paired_up:
        return whole_layer(
            query_a,
            query_b,
            latent,
            rope_key,
            latent_gain,
            key_a_weight,
            value_a_weight,
            key_b_weight,
            value_b_weight,
            out_a_weight,
            out_b_weight,
            residual,
            ffn_gain,
            routes,
            route_weight,
            expert_gate,
            expert_up,
            expert_down,
            capacity,
        )
    span_size = query_a.shape[0]
    rotary_width = rope_key.shape[1]
    own_first = (lax.axis_index("sp") * column_count + lax.axis_index("tp")) * row_count
    query_first = lax.axis_index("sp") * span_size
    own_cosine, own_sine = angle_tables(
        own_first + jnp.arange(row_count, dtype=jnp.int32), rotary_width
    )
    normed_latent = rms_scale(latent, latent_gain)
    turned_key = rotate(rope_key, own_cosine, own_sine)
    query_cosine, query_sine = angle_tables(
        query_first + jnp.arange(span_size, dtype=jnp.int32), rotary_width
    )
    heads_a = key_a_weight.shape[1] // NOPE_A
    heads_b = key_b_weight.shape[1] // NOPE_B
    ready_a = prepare_queries(query_a, heads_a, NOPE_A, query_cosine, query_sine)
    ready_b = prepare_queries(query_b, heads_b, NOPE_B, query_cosine, query_sine)

    def start_state(head_count, value_width):
        return (
            jnp.full((head_count, span_size), masked_score, jnp.float32),
            jnp.zeros((head_count, span_size), jnp.float32),
            jnp.zeros((span_size, head_count, value_width), jnp.float32),
        )

    initial = (start_state(heads_a, VAL_A), start_state(heads_b, VAL_B))

    def attend_block(carried, keys_a, values_a, keys_b, values_b, key_turned):
        return (
            fold_group(carried[0], ready_a, keys_a, key_turned, values_a, query_first),
            fold_group(carried[1], ready_b, keys_b, key_turned, values_b, query_first),
        )

    rank = normed_latent.shape[1]
    filler = jnp.zeros((row_count, -(rank + rotary_width) % 128), jnp.bfloat16)
    packed = jnp.concatenate([normed_latent, turned_key, filler], axis=1)
    gathered = gather(packed[None], lax.axis_size("sp"), column_count, True, 0)
    gathered = gathered.reshape(-1, packed.shape[1])
    portion_latent = gathered[:, :rank]
    portion_turned = gathered[:, rank : rank + rotary_width]

    def compute(current):
        return attend_block(
            current,
            expand(portion_latent, key_a_weight, heads_a),
            expand(portion_latent, value_a_weight, heads_a),
            expand(portion_latent, key_b_weight, heads_b),
            expand(portion_latent, value_b_weight, heads_b),
            portion_turned,
        )

    folded = compute(initial)

    def finish(carried):
        top_score, weight_total, weighted = carried
        scaled = weighted / jnp.transpose(weight_total)[:, :, None]
        return scaled.astype(jnp.bfloat16).reshape(span_size, -1)

    out_a = finish(folded[0])
    out_b = finish(folded[1])
    projected = (
        jnp.dot(out_a, out_a_weight, preferred_element_type=jnp.float32)
        + jnp.dot(out_b, out_b_weight, preferred_element_type=jnp.float32)
    ).astype(jnp.bfloat16)
    model_width = residual.shape[1]
    chosen = routes.reshape(-1)
    expert_ids = jnp.arange(experts, dtype=jnp.int32)
    matches = (chosen[:, None] == expert_ids[None, :]).astype(jnp.int32)
    order_rank = jnp.sum((jnp.cumsum(matches, axis=0) - 1) * matches, axis=1)
    slot_index = (chosen * capacity + order_rank).reshape(row_count, TOP)
    slot_ids = jnp.arange(experts * capacity, dtype=jnp.int32)
    selection = jnp.sum(
        (slot_ids[:, None, None] == slot_index[None, :, :]).astype(jnp.bfloat16), axis=2
    )
    hidden_state, outgoing = hidden_sum(
        projected.reshape(column_count, row_count, -1), residual, ffn_gain, selection, 1
    )
    outgoing = outgoing.reshape(experts, capacity, model_width)
    if capacity % 16 == 0:
        places_of = slot_index.T.reshape(-1)
        selector = (places_of[:, None] == slot_ids[None, :]).astype(jnp.bfloat16)
        return through_experts(
            outgoing,
            selector,
            route_weight,
            hidden_state,
            expert_gate,
            expert_up,
            expert_down,
            column_count,
            4,
        )
    portion = gather(outgoing, experts, column_count, False, 2)
    portion_shape = portion.shape
    flat_rows = portion.reshape(-1, model_width)
    gate_values = jnp.dot(flat_rows, expert_gate[0], preferred_element_type=jnp.float32)
    up_values = jnp.dot(flat_rows, expert_up[0], preferred_element_type=jnp.float32)
    hidden = (jax.nn.silu(gate_values) * up_values).astype(jnp.bfloat16)
    partial_value = jnp.dot(hidden, expert_down[0], preferred_element_type=jnp.float32).astype(
        jnp.bfloat16
    )
    returned = give_back(partial_value.reshape(portion_shape), 3)
    flat_returned = returned.reshape(experts * capacity, model_width)
    expert_mix = jnp.zeros((row_count, model_width), jnp.float32)
    for route_index in range(TOP):
        selector = (slot_index[:, route_index][:, None] == slot_ids[None, :]).astype(jnp.bfloat16)
        picked = jnp.dot(selector, flat_returned, preferred_element_type=jnp.float32)
        expert_mix = expert_mix + route_weight[:, route_index][:, None] * picked
    return (hidden_state.astype(jnp.float32) + expert_mix).astype(jnp.bfloat16)


def solution(mesh):
    placed = (
        P("sp", "tp"),
        P("sp", "tp"),
        P(("sp", "tp"), None),
        P(("sp", "tp"), None),
        P(),
        P(None, "tp"),
        P(None, "tp"),
        P(None, "tp"),
        P(None, "tp"),
        P("tp", None),
        P("tp", None),
        P(("sp", "tp"), None),
        P(),
        P(("sp", "tp"), None),
        P(("sp", "tp"), None),
        P("sp", None, "tp"),
        P("sp", None, "tp"),
        P("sp", "tp", None),
    )
    return jax.shard_map(
        body, mesh=mesh, in_specs=placed, out_specs=P(("sp", "tp"), None), check_vma=False
    )
```

```python
import functools

import jax
import jax.numpy as jnp
import numpy as np
from jax import lax
from jax.experimental import pallas as pl
from jax.experimental.pallas import tpu as pltpu
from jax.sharding import PartitionSpec as P

NOPE_A = 128
VAL_A = 128
NOPE_B = 64
VAL_B = 64
TOP = 2


epsilon = 1e-06
base_theta = 500000.0
masked_score = -1e30


def rms_scale(values, scales):
    floats = values.astype(jnp.float32)
    scaled = floats * lax.rsqrt(jnp.mean(floats * floats, axis=-1, keepdims=True) + epsilon)
    return (scaled * scales).astype(jnp.bfloat16)


def angle_tables(positions, rotary_width):
    inverse = jnp.power(
        jnp.float32(base_theta), -jnp.arange(0, rotary_width, 2, dtype=jnp.float32) / rotary_width
    )
    angles = positions.astype(jnp.float32)[:, None] * inverse[None, :]
    return (jnp.cos(angles), jnp.sin(angles))


def rotate(values, cosine, sine_table):
    middle = cosine.shape[-1]
    first_half = values[..., :middle].astype(jnp.float32)
    second_half = values[..., middle:].astype(jnp.float32)
    turned = jnp.concatenate(
        [
            first_half * cosine - second_half * sine_table,
            second_half * cosine + first_half * sine_table,
        ],
        axis=-1,
    )
    return turned.astype(jnp.bfloat16)


def prepare_queries(queries, head_count, nope_width, cosine, sine_table):
    shaped = queries.reshape(queries.shape[0], head_count, queries.shape[1] // head_count)
    turned = rotate(shaped[:, :, nope_width:], cosine[:, None, :], sine_table[:, None, :])
    return jnp.concatenate([shaped[:, :, :nope_width], turned], axis=-1)


def fold_group(carried, queries, key_nope, key_turned, values, query_first):
    top_score, weight_total, weighted = carried
    nope_width = key_nope.shape[2]
    scale = (nope_width + key_turned.shape[1]) ** (-0.5)
    scores = jnp.einsum(
        "thd,shd->hts", queries[:, :, :nope_width], key_nope, preferred_element_type=jnp.float32
    )
    scores = scores + jnp.einsum(
        "thd,sd->hts", queries[:, :, nope_width:], key_turned, preferred_element_type=jnp.float32
    )
    scores = scores * scale
    query_places = query_first + jnp.arange(queries.shape[0], dtype=jnp.int32)
    key_places = jnp.arange(key_nope.shape[0], dtype=jnp.int32)
    allowed = (key_places[None, :] <= query_places[:, None])[None]
    scores = jnp.where(allowed, scores, masked_score)
    new_top = jnp.maximum(top_score, jnp.max(scores, axis=-1))
    weights = jnp.where(allowed, jnp.exp(scores - new_top[:, :, None]), 0.0)
    new_total = jnp.sum(weights, axis=-1)
    product = jnp.einsum(
        "hts,shd->thd", weights.astype(jnp.bfloat16), values, preferred_element_type=jnp.float32
    )
    return (new_top, new_total, product)


def expand(source, weight, head_count):
    product = jnp.dot(source, weight, preferred_element_type=jnp.float32).astype(jnp.bfloat16)
    return product.reshape(source.shape[0], head_count, weight.shape[1] // head_count)


MESH = pl.DeviceIdType.MESH


def places():
    me, column = lax.axis_index("sp"), lax.axis_index("tp")
    half = lax.axis_size("tp") // 2
    across = lax.rem(column + half, 2 * half)
    partner = column + 1 - 2 * lax.rem(column, 2)
    return me, column, across, partner


def send(source, target, send_sem, recv_sem, place):
    return pltpu.make_async_remote_copy(
        src_ref=source,
        dst_ref=target,
        send_sem=send_sem,
        recv_sem=recv_sem,
        device_id={"sp": place[0], "tp": place[1]},
        device_id_type=MESH,
    )


def greet(count, me, column, others):
    barrier = pltpu.get_barrier_semaphore()

    def step(k, carry):
        pl.semaphore_signal(
            barrier,
            inc=1,
            device_id={"sp": lax.rem(me + k, count), "tp": column},
            device_id_type=MESH,
        )
        return carry

    lax.fori_loop(1, count, step, 0)
    for other in others:
        pl.semaphore_signal(
            barrier, inc=1, device_id={"sp": me, "tp": other}, device_id_type=MESH
        )
    pl.semaphore_wait(barrier, max(count, 1) - 1 + len(others))


def loop(low, high, step):
    lax.fori_loop(low, high, lambda k, carry: (step(k), carry)[1], 0)


def gather_kernel(count, causal, in_ref, out_ref, send_sem, recv_sem):
    me, column, across, partner = places()
    diagonal = lax.rem(partner + lax.axis_size("tp") // 2, lax.axis_size("tp"))
    greet(count, me, column, (across, partner))

    def own(p):
        return in_ref.at[0] if causal else in_ref.at[p]

    def over_sp(k):
        p = lax.rem(me + k, count)
        return send(
            own(p), out_ref.at[me, column], send_sem.at[0, k], recv_sem.at[0, me], (p, column)
        )

    def arrival(kind, s, t):
        block = out_ref.at[s, t]
        return send(block, block, send_sem.at[kind, s], recv_sem.at[kind, s], (me, partner))

    def pass_on(s, source):
        target = out_ref.at[s, column]
        return (
            send(source, target, send_sem.at[1, s], recv_sem.at[1, s], (me, across)),
            send(source, target, send_sem.at[2, s], recv_sem.at[2, s], (me, partner)),
        )

    def to_partner(s):
        block = out_ref.at[s, across]
        return send(block, block, send_sem.at[3, s], recv_sem.at[3, s], (me, partner))

    last = count - me if causal else count
    arrivals = me + 1 if causal else count

    loop(1, last, lambda k: over_sp(last - k).start())
    for copy in pass_on(me, own(me)):
        copy.start()
    out_ref[me, column] = in_ref[0] if causal else in_ref[me]
    if causal:

        def clear(s):
            out_ref[s] = jnp.zeros(out_ref.shape[1:], out_ref.dtype)

        loop(me + 1, count, clear)

    def origin(k):
        return lax.rem(me + count - k, count)

    def arrived(k):
        s = origin(k)
        arrival(0, s, column).wait_recv()
        for copy in pass_on(s, out_ref.at[s, column]):
            copy.start()

    loop(1, arrivals, arrived)

    def crossed(k):
        s = origin(k)
        arrival(1, s, across).wait_recv()
        to_partner(s).start()

    loop(0, arrivals, crossed)

    def settle(k):
        s = origin(k)
        arrival(2, s, partner).wait_recv()
        arrival(3, s, diagonal).wait_recv()
        for copy in pass_on(s, out_ref.at[s, column]):
            copy.wait_send()
        to_partner(s).wait_send()

    loop(0, arrivals, settle)
    loop(1, last, lambda k: over_sp(k).wait_send())


def gather(blocks, count, columns, causal, collective_id):
    return pl.pallas_call(
        functools.partial(gather_kernel, count, causal),
        out_shape=jax.ShapeDtypeStruct((count, columns) + blocks.shape[1:], blocks.dtype),
        in_specs=[pl.BlockSpec(memory_space=pltpu.VMEM)],
        out_specs=pl.BlockSpec(memory_space=pltpu.VMEM),
        scratch_shapes=[
            pltpu.SemaphoreType.DMA((4, count)),
            pltpu.SemaphoreType.DMA((4, count)),
        ],
        compiler_params=pltpu.CompilerParams(
            collective_id=collective_id, has_side_effects=True, vmem_limit_bytes=60000 * 1024
        ),
    )(blocks)


def hidden_kernel(
    columns, part_ref, residual_ref, gain_ref, pick_ref, hidden_ref, outgoing_ref, held, send_sem, recv_sem
):
    me, column, _, _ = places()
    others = [lax.rem(column + k, columns) for k in range(1, columns)]
    greet(1, me, column, others)
    copies = []
    for k, other in enumerate(others):
        copies.append(
            send(part_ref.at[other], held.at[k], send_sem.at[k], recv_sem.at[k], (me, other))
        )
    for copy in copies:
        copy.start()
    total = residual_ref[...].astype(jnp.float32) + part_ref[column].astype(jnp.float32)
    for k, copy in enumerate(copies):
        copy.wait_recv()
        total = total + held[k].astype(jnp.float32)
    hidden = total.astype(jnp.bfloat16)
    hidden_ref[...] = hidden
    normed = rms_scale(hidden, gain_ref[...])
    outgoing = jnp.dot(pick_ref[...], normed, preferred_element_type=jnp.float32)
    outgoing_ref[...] = outgoing.astype(jnp.bfloat16)
    for copy in copies:
        copy.wait_send()


def hidden_sum(parts, residual, gain, selection, collective_id):
    columns, rows, width = parts.shape
    return pl.pallas_call(
        functools.partial(hidden_kernel, columns),
        out_shape=[
            jax.ShapeDtypeStruct((rows, width), jnp.bfloat16),
            jax.ShapeDtypeStruct((selection.shape[0], width), jnp.bfloat16),
        ],
        in_specs=[pl.BlockSpec(memory_space=pltpu.VMEM)] * 4,
        out_specs=[pl.BlockSpec(memory_space=pltpu.VMEM)] * 2,
        scratch_shapes=[
            pltpu.VMEM((columns - 1, rows, width), jnp.bfloat16),
            pltpu.SemaphoreType.DMA((columns - 1,)),
            pltpu.SemaphoreType.DMA((columns - 1,)),
        ],
        compiler_params=pltpu.CompilerParams(
            collective_id=collective_id, has_side_effects=True, vmem_limit_bytes=60000 * 1024
        ),
    )(parts, residual, gain.reshape(1, width), selection)


def return_kernel(
    count, in_ref, out_ref, from_partner, pair, mine, from_across, done, send_sem, recv_sem
):
    me, column, across, partner = places()
    diagonal = lax.rem(partner + lax.axis_size("tp") // 2, lax.axis_size("tp"))
    greet(count, me, column, (across, partner))

    def place(k):
        return lax.rem(me + 1 + k, count)

    def to_partner(s, slot):
        wanted = (partner, diagonal)[slot]
        return send(
            in_ref.at[s, wanted],
            from_partner.at[slot, s],
            send_sem.at[slot, s],
            recv_sem.at[slot, s],
            (me, partner),
        )

    def over_x(s):
        return send(
            pair.at[s], from_across.at[s], send_sem.at[2, s], recv_sem.at[2, s], (me, across)
        )

    def back(s):
        return send(
            done.at[s], out_ref.at[me], send_sem.at[3, s], recv_sem.at[3, me], (s, column)
        )

    def start(k):
        s = place(k)
        to_partner(s, 1).start()
        to_partner(s, 0).start()

    loop(0, count, start)

    def both(s, slot):
        kept = in_ref[s, (column, across)[slot]].astype(jnp.float32)
        return kept + from_partner[slot, s].astype(jnp.float32)

    def paired(k):
        s = place(k)
        to_partner(s, 1).wait_recv()
        pair[s] = both(s, 1).astype(jnp.bfloat16)
        over_x(s).start()

    loop(0, count, paired)

    def total(s):
        to_partner(s, 0).wait_recv()
        mine[...] = both(s, 0)
        over_x(s).wait_recv()
        return (mine[...] + from_across[s].astype(jnp.float32)).astype(jnp.bfloat16)

    def summed(k):
        s = place(k)
        done[s] = total(s)
        back(s).start()

    loop(0, count - 1, summed)
    out_ref[me] = total(me)

    def arrived(k):
        s = place(k)
        send(
            done.at[s], out_ref.at[s], send_sem.at[3, s], recv_sem.at[3, s], (s, column)
        ).wait_recv()
        back(s).wait_send()

    loop(0, count - 1, arrived)

    def settle(s):
        to_partner(s, 0).wait_send()
        to_partner(s, 1).wait_send()
        over_x(s).wait_send()

    loop(0, count, settle)


def give_back(partials, collective_id):
    count, _, rows, width = partials.shape
    block = (count, rows, width)
    return pl.pallas_call(
        functools.partial(return_kernel, count),
        out_shape=jax.ShapeDtypeStruct(block, jnp.bfloat16),
        in_specs=[pl.BlockSpec(memory_space=pltpu.VMEM)],
        out_specs=pl.BlockSpec(memory_space=pltpu.VMEM),
        scratch_shapes=[
            pltpu.VMEM((2,) + block, jnp.bfloat16),
            pltpu.VMEM(block, jnp.bfloat16),
            pltpu.VMEM(block[1:], jnp.float32),
            pltpu.VMEM(block, jnp.bfloat16),
            pltpu.VMEM(block, jnp.bfloat16),
            pltpu.SemaphoreType.DMA((4, count)),
            pltpu.SemaphoreType.DMA((4, count)),
        ],
        compiler_params=pltpu.CompilerParams(
            collective_id=collective_id, has_side_effects=True, vmem_limit_bytes=60000 * 1024
        ),
    )(partials)


def experts_kernel(
    count,
    group,
    in_ref,
    selector_ref,
    share_ref,
    hidden_ref,
    gate_hbm,
    up_hbm,
    down_hbm,
    out_ref,
    rows,
    part,
    from_partner,
    pair,
    from_across,
    done,
    returned,
    gate,
    up,
    down,
    weight_sem,
    send_sem,
    recv_sem,
):
    me, column, across, partner = places()
    diagonal = lax.rem(partner + lax.axis_size("tp") // 2, lax.axis_size("tp"))
    loads = [
        pltpu.make_async_copy(source.at[0], target, weight_sem.at[index])
        for index, (source, target) in enumerate(((gate_hbm, gate), (up_hbm, up), (down_hbm, down)))
    ]
    for load in loads:
        load.start()
    greet(count, me, column, (across, partner))

    def origin(k):
        return lax.rem(me + count - k, count)

    def over_sp(k):
        p = lax.rem(me + k, count)
        return send(
            in_ref.at[p], rows.at[me, column], send_sem.at[0, k], recv_sem.at[0, me], (p, column)
        )

    def arrival(kind, s, t):
        block = rows.at[s, t]
        return send(block, block, send_sem.at[kind, s], recv_sem.at[kind, s], (me, partner))

    def pass_on(s, source):
        target = rows.at[s, column]
        return (
            send(source, target, send_sem.at[1, s], recv_sem.at[1, s], (me, across)),
            send(source, target, send_sem.at[2, s], recv_sem.at[2, s], (me, partner)),
        )

    def cross_on(s):
        block = rows.at[s, across]
        return send(block, block, send_sem.at[3, s], recv_sem.at[3, s], (me, partner))

    def to_partner(s, slot):
        wanted = (partner, diagonal)[slot]
        return send(
            part.at[s, wanted],
            from_partner.at[slot, s],
            send_sem.at[4 + slot, s],
            recv_sem.at[4 + slot, s],
            (me, partner),
        )

    def over_x(s):
        return send(
            pair.at[s], from_across.at[s], send_sem.at[6, s], recv_sem.at[6, s], (me, across)
        )

    def back(s):
        return send(
            done.at[s], returned.at[me], send_sem.at[7, s], recv_sem.at[7, me], (s, column)
        )

    loop(1, count, lambda k: over_sp(k).start())
    for copy in pass_on(me, in_ref.at[me]):
        copy.start()
    rows[me, column] = in_ref[me]

    def arrived(k):
        s = origin(k)
        arrival(0, s, column).wait_recv()
        for copy in pass_on(s, rows.at[s, column]):
            copy.start()

    def both(s, slot):
        kept = part[s, (column, across)[slot]].astype(jnp.float32)
        return kept + from_partner[slot, s].astype(jnp.float32)

    def paired(k):
        s = origin(k)
        to_partner(s, 1).wait_recv()
        pair[s] = both(s, 1).astype(jnp.bfloat16)
        over_x(s).start()

    def summed(k):
        s = origin(k)
        to_partner(s, 0).wait_recv()
        over_x(s).wait_recv()
        total = (both(s, 0) + from_across[s].astype(jnp.float32)).astype(jnp.bfloat16)

        @pl.when(k == 0)
        def _():
            returned[me] = total

        @pl.when(k > 0)
        def _():
            done[s] = total
            back(s).start()

    loop(1, group, arrived)
    block_rows = rows.shape[1] * rows.shape[2]
    width = rows.shape[3]

    def turn(j):
        first = j * group

        @pl.when(first + group < count)
        def _():
            loop(first + group, first + 2 * group, arrived)

        def crossed(k):
            s = origin(k)
            arrival(1, s, across).wait_recv()
            cross_on(s).start()

        loop(first, first + group, crossed)

        def whole(k):
            s = origin(k)
            arrival(2, s, partner).wait_recv()
            arrival(3, s, diagonal).wait_recv()

        loop(first, first + group, whole)

        @pl.when(j == 0)
        def _():
            for load in loads:
                load.wait()

        sources = [origin(first + i) for i in range(group)]
        flat = jnp.concatenate([rows[s].reshape(block_rows, width) for s in sources], axis=0)
        gate_values = jnp.dot(flat, gate[...], preferred_element_type=jnp.float32)
        up_values = jnp.dot(flat, up[...], preferred_element_type=jnp.float32)
        hidden = (jax.nn.silu(gate_values) * up_values).astype(jnp.bfloat16)
        product = jnp.dot(hidden, down[...], preferred_element_type=jnp.float32)
        product = product.astype(jnp.bfloat16)
        for i, s in enumerate(sources):
            part[s] = product[i * block_rows : (i + 1) * block_rows].reshape(rows.shape[1:])

        def leave(k):
            s = origin(k)
            to_partner(s, 1).start()
            to_partner(s, 0).start()

        loop(first, first + group, leave)

        @pl.when(j > 0)
        def _():
            loop(first - group, first, paired)

        @pl.when(j > 1)
        def _():
            loop(first - 2 * group, first - group, summed)

    turns = count // group
    loop(0, turns, turn)
    loop(count - group, count, paired)
    loop(max(turns - 2, 0) * group, count, summed)

    def home(k):
        s = origin(k)
        send(
            done.at[s], returned.at[s], send_sem.at[7, s], recv_sem.at[7, s], (s, column)
        ).wait_recv()
        back(s).wait_send()

    loop(1, count, home)
    picked = jnp.dot(
        selector_ref[...], returned[...].reshape(-1, width), preferred_element_type=jnp.float32
    )
    own_rows = hidden_ref.shape[0]
    mixed = jnp.zeros(hidden_ref.shape, jnp.float32)
    for route_index in range(TOP):
        mixed = mixed + (
            share_ref[:, route_index : route_index + 1]
            * picked[route_index * own_rows : (route_index + 1) * own_rows]
        )
    out_ref[...] = (hidden_ref[...].astype(jnp.float32) + mixed).astype(jnp.bfloat16)

    def settle(s):
        for copy in pass_on(s, rows.at[s, column]):
            copy.wait_send()
        cross_on(s).wait_send()
        to_partner(s, 0).wait_send()
        to_partner(s, 1).wait_send()
        over_x(s).wait_send()

    loop(0, count, settle)
    loop(1, count, lambda k: over_sp(k).wait_send())


def through_experts(outgoing, selector, share, hidden, gate, up, down, columns, collective_id):
    count, rows, width = outgoing.shape
    group = 2 if count % 2 == 0 else 1
    block = (count, rows, width)
    every = (count, columns, rows, width)
    return pl.pallas_call(
        functools.partial(experts_kernel, count, group),
        out_shape=jax.ShapeDtypeStruct(hidden.shape, jnp.bfloat16),
        in_specs=[pl.BlockSpec(memory_space=pltpu.VMEM)] * 4
        + [pl.BlockSpec(memory_space=pl.ANY)] * 3,
        out_specs=pl.BlockSpec(memory_space=pltpu.VMEM),
        scratch_shapes=[
            pltpu.VMEM(every, jnp.bfloat16),
            pltpu.VMEM(every, jnp.bfloat16),
            pltpu.VMEM((2,) + block, jnp.bfloat16),
            pltpu.VMEM(block, jnp.bfloat16),
            pltpu.VMEM(block, jnp.bfloat16),
            pltpu.VMEM(block, jnp.bfloat16),
            pltpu.VMEM(block, jnp.bfloat16),
            pltpu.VMEM(gate.shape[1:], jnp.bfloat16),
            pltpu.VMEM(up.shape[1:], jnp.bfloat16),
            pltpu.VMEM(down.shape[1:], jnp.bfloat16),
            pltpu.SemaphoreType.DMA((3,)),
            pltpu.SemaphoreType.DMA((8, count)),
            pltpu.SemaphoreType.DMA((8, count)),
        ],
        compiler_params=pltpu.CompilerParams(
            collective_id=collective_id, has_side_effects=True, vmem_limit_bytes=60000 * 1024
        ),
    )(outgoing, selector, share, hidden, gate, up, down)


def turn_tables(positions, rotary_width):
    inverse = np.power(
        np.float32(base_theta), -np.arange(0, rotary_width, 2, dtype=np.float32) / rotary_width
    ).astype(np.float32)
    angles = positions.astype(np.float32)[:, None] * inverse[None, :]
    cosine, sine = np.cos(angles), np.sin(angles)
    return np.concatenate([cosine, cosine, -sine, sine], axis=1).astype(np.float32)


def iotas(shape):
    return (
        lax.broadcasted_iota(jnp.int32, shape, 0),
        lax.broadcasted_iota(jnp.int32, shape, 1),
    )


def dot(left, right):
    return jnp.dot(left, right, preferred_element_type=jnp.float32)


def dot_over(left, right, left_dim, right_dim):
    return lax.dot_general(
        left, right, (((left_dim,), (right_dim,)), ((), ())), preferred_element_type=jnp.float32
    )


def layer_kernel(
    count,
    columns,
    heads_a,
    heads_b,
    query_a_hbm,
    query_b_hbm,
    latent_hbm,
    rope_hbm,
    latent_gain_hbm,
    key_a_hbm,
    value_a_hbm,
    key_b_hbm,
    value_b_hbm,
    out_a_hbm,
    out_b_hbm,
    residual_hbm,
    ffn_gain_hbm,
    routes_hbm,
    share_hbm,
    table_hbm,
    gate_hbm,
    up_hbm,
    down_hbm,
    out_ref,
    query_a,
    query_b,
    latent,
    rope,
    latent_gain,
    key_a,
    value_a,
    key_b,
    value_b,
    out_a,
    out_b,
    residual,
    ffn_gain,
    routes,
    share,
    own_table,
    query_table,
    gate,
    up,
    down,
    own,
    gathered,
    key_weight,
    keys,
    values,
    head_part,
    head_pair,
    head_from_partner,
    head_from_across,
    hidden,
    selection,
    mixing,
    outgoing,
    rows,
    part,
    from_partner,
    pair,
    from_across,
    done,
    returned,
    load_sem,
    gather_send,
    gather_recv,
    sum_send,
    sum_recv,
    send_sem,
    recv_sem,
):
    me, column, across, partner = places()
    diagonal = lax.rem(partner + columns // 2, columns)
    row_count = latent.shape[0]
    span = query_a.shape[0]
    rank = latent.shape[1]
    rotary = rope.shape[1]
    width = residual.shape[1]
    total = count * span

    own_first = pl.multiple_of((me * columns + column) * row_count, row_count)
    query_first = pl.multiple_of(me * span, span)
    plan = [
        (latent_hbm, latent),
        (rope_hbm, rope),
        (latent_gain_hbm, latent_gain),
        (table_hbm.at[pl.ds(own_first, row_count)], own_table),
        (key_a_hbm, key_a),
        (key_b_hbm, key_b),
        (query_a_hbm, query_a),
        (query_b_hbm, query_b),
        (table_hbm.at[pl.ds(query_first, span)], query_table),
        (value_a_hbm, value_a),
        (value_b_hbm, value_b),
        (routes_hbm, routes),
        (share_hbm, share),
        (out_a_hbm, out_a),
        (out_b_hbm, out_b),
        (residual_hbm, residual),
        (ffn_gain_hbm, ffn_gain),
        (gate_hbm.at[0], gate),
        (up_hbm.at[0], up),
        (down_hbm.at[0], down),
    ]
    loads = [
        pltpu.make_async_copy(source, target, load_sem.at[index])
        for index, (source, target) in enumerate(plan)
    ]
    for load in loads:
        load.start()

    barrier = pltpu.get_barrier_semaphore()

    def hello(k, carry):
        pl.semaphore_signal(
            barrier,
            inc=1,
            device_id={"sp": lax.rem(me + k, count), "tp": column},
            device_id_type=MESH,
        )
        return carry

    lax.fori_loop(1, count, hello, 0)
    for other in (across, partner):
        pl.semaphore_signal(
            barrier, inc=1, device_id={"sp": me, "tp": other}, device_id_type=MESH
        )

    for load in loads[:4]:
        load.wait()
    row, col = iotas((128, 128))
    swap = (row == jnp.where(jnp.bitwise_and(col, rotary - 1) < rotary // 2, col + rotary // 2, col - rotary // 2))
    swap = swap.astype(jnp.bfloat16)
    own[:, :rank] = rms_scale(latent[...], latent_gain[...])
    key = rope[...]
    turned = key.astype(jnp.float32) * own_table[:, :rotary] + (
        dot(key, swap[:rotary, :rotary]) * own_table[:, rotary:]
    )
    own[:, rank : rank + rotary] = turned.astype(jnp.bfloat16)
    own[:, rank + rotary :] = jnp.zeros(
        (row_count, own.shape[1] - rank - rotary), jnp.bfloat16
    )
    for load in loads[4:13]:
        load.wait()
    nope_a = key_a.shape[1] // heads_a
    nope_b = key_b.shape[1] // heads_b
    wide_a = 256
    wide_b = nope_b + rotary
    starts_a = []
    for h in range(heads_a):
        start = h * (nope_a + rotary)
        starts_a.append(start // 128 * 128)
        pad = start - starts_a[h]
        r, c = iotas((key_a.shape[1], wide_a))
        inside = (c >= pad) & (c < pad + nope_a)
        piece = ((r - c == h * nope_a - pad) & inside).astype(jnp.bfloat16)
        lanes = slice(h * wide_a, (h + 1) * wide_a)
        key_weight[:rank, lanes] = dot(key_a[...], piece).astype(jnp.bfloat16)
        r, c = iotas((own.shape[1] - rank, wide_a))
        key_weight[rank:, lanes] = ((c - r == pad + nope_a) & (r < rotary)).astype(jnp.bfloat16)
    base_b = heads_a * wide_a
    for h in range(heads_b):
        r, c = iotas((key_b.shape[1], wide_b))
        piece = ((r - c == h * nope_b) & (c < nope_b)).astype(jnp.bfloat16)
        lanes = slice(base_b + h * wide_b, base_b + (h + 1) * wide_b)
        key_weight[:rank, lanes] = dot(key_b[...], piece).astype(jnp.bfloat16)
        r, c = iotas((own.shape[1] - rank, wide_b))
        key_weight[rank:, lanes] = ((c - r == nope_b) & (r < rotary)).astype(jnp.bfloat16)

    lane = lax.broadcasted_iota(jnp.int32, (span, 128), 1)
    table = query_table[...]
    rolled = jnp.concatenate([table[:, rotary:], table[:, :rotary]], axis=1)
    low = lane < rotary
    one = jnp.ones((span, 128), jnp.float32)
    zero = jnp.zeros((span, 128), jnp.float32)
    turn_low = (jnp.where(low, table, one), jnp.where(low, rolled, zero))
    turn_high = (jnp.where(low, one, rolled), jnp.where(low, zero, table))

    def turn_tile(ref, start, factors):
        tile = ref[:, start : start + 128]
        turned_tile = tile.astype(jnp.float32) * factors[0] + dot(tile, swap) * factors[1]
        ref[:, start : start + 128] = turned_tile.astype(jnp.bfloat16)

    for h in range(heads_a):
        start = h * (nope_a + rotary) + nope_a
        turn_tile(query_a, start // 128 * 128, turn_low if start % 128 == 0 else turn_high)
    for h in range(heads_b):
        turn_tile(query_b, h * wide_b, turn_high)

    capacity = outgoing.shape[1]
    slots = count * capacity
    expert_at = lax.broadcasted_iota(jnp.int32, (count, row_count), 0)
    before = iotas((row_count, row_count))
    before = (before[0] < before[1]).astype(jnp.bfloat16)
    slot_at = lax.broadcasted_iota(jnp.int32, (slots, row_count), 0)
    earlier = jnp.zeros((count, 1), jnp.float32)
    picks = []
    for k in range(TOP):
        expert = routes[k : k + 1, :]
        named = (expert_at == expert).astype(jnp.float32)
        place = dot(named.astype(jnp.bfloat16), before) + earlier
        place = jnp.sum(place * named, axis=0, keepdims=True).astype(jnp.int32)
        picks.append((slot_at == expert * capacity + place).astype(jnp.float32))
        earlier = earlier + jnp.sum(named, axis=1, keepdims=True)
    selection[...] = functools.reduce(lambda a, b: a + b, picks).astype(jnp.bfloat16)
    mix = functools.reduce(
        lambda a, b: a + b, [pick * share[k : k + 1, :] for k, pick in enumerate(picks)]
    )
    mix_high = mix.astype(jnp.bfloat16)
    mixing[0] = mix_high
    mixing[1] = (mix - mix_high.astype(jnp.float32)).astype(jnp.bfloat16)

    pl.semaphore_wait(barrier, count + 1)

    half = count // 2
    upper = me // half
    at = lax.rem(me, half)

    def g_over_sp(k):
        p = lax.rem(me + k, count)
        return send(
            own, gathered.at[me, column], gather_send.at[0, k], gather_recv.at[0, me], (p, column)
        )

    def g_hand_on(k):
        p = upper * half + lax.rem(at + k, half)
        block = gathered.at[at, column]
        return send(block, block, gather_send.at[4, k], gather_recv.at[0, at], (p, column))

    def g_arrival(kind, s, t):
        block = gathered.at[s, t]
        return send(
            block, block, gather_send.at[kind, s], gather_recv.at[kind, s], (me, partner)
        )

    def g_pass_on(s, source):
        target = gathered.at[s, column]
        return (
            send(source, target, gather_send.at[1, s], gather_recv.at[1, s], (me, across)),
            send(source, target, gather_send.at[2, s], gather_recv.at[2, s], (me, partner)),
        )

    def g_to_partner(s):
        block = gathered.at[s, across]
        return send(
            block, block, gather_send.at[3, s], gather_recv.at[3, s], (me, partner)
        )

    last = half - at

    @pl.when(upper == 0)
    def _():
        g_over_sp(half).start()

    for copy in g_pass_on(me, own):
        copy.start()
    loop(1, last, lambda k: g_over_sp(last - k).start())
    gathered[me, column] = own[...]

    def clear(s):
        values[s] = jnp.zeros(values.shape[1:], values.dtype)
        keys[s] = jnp.zeros(keys.shape[1:], keys.dtype)

    loop(me + 1, count, clear)

    def origin(k):
        later = (k + count - at - 1) // count
        return (1 - later) * (me - k) + later * lax.rem(k - 1 + half, half)

    def g_arrived(k):
        s = origin(k)
        g_arrival(0, s, column).wait_recv()

        @pl.when(k == at + 1)
        def _():
            loop(1, half, lambda i: g_hand_on(i).start())

        for copy in g_pass_on(s, gathered.at[s, column]):
            copy.start()


    def g_step(k):
        @pl.when(k <= me)
        def _():
            s = origin(k)
            g_arrival(1, s, across).wait_recv()
            g_to_partner(s).start()

        @pl.when(k >= 1)
        def _():
            s = origin(k - 1)
            g_arrival(2, s, partner).wait_recv()
            g_arrival(3, s, diagonal).wait_recv()
            packed = gathered[s].reshape(span, own.shape[1])
            keys[s] = dot(packed, key_weight[...]).astype(jnp.bfloat16)
            values[s, :, : value_a.shape[1]] = dot(packed[:, :rank], value_a[...]).astype(
                jnp.bfloat16
            )
            values[s, :, value_a.shape[1] :] = dot(packed[:, :rank], value_b[...]).astype(
                jnp.bfloat16
            )

    first = at + 1 + upper
    loop(1, first, g_arrived)
    loop(0, first, g_step)
    loop(first, me + 1, g_arrived)
    loop(first, me + 2, g_step)

    query_at, key_at = iotas((span, total))
    allowed = key_at <= query_at + query_first

    def weigh(queries, lanes, size):
        scores = dot_over(queries, keys[:, :, lanes].reshape(total, -1), 1, 1)
        scores = jnp.where(allowed, scores, masked_score)
        top = jnp.max(scores, axis=1, keepdims=True)
        weights = jnp.exp((scores - top) * size ** (-0.5))
        return weights.astype(jnp.bfloat16), jnp.sum(weights, axis=1, keepdims=True)

    def attend(parts, lanes, each):
        group = values[:, :, lanes].reshape(total, -1)
        results = [dot(weights, group) / sums for weights, sums in parts]
        result = results[0]
        place = lax.broadcasted_iota(jnp.int32, result.shape, 1)
        for h in range(1, len(parts)):
            result = jnp.where(place < h * each, result, results[h])
        return result.astype(jnp.bfloat16)

    for load in loads[13:17]:
        load.wait()
    mixed_a = attend(
        [
            weigh(
                query_a[:, starts_a[h] : starts_a[h] + wide_a],
                slice(h * wide_a, (h + 1) * wide_a),
                nope_a + rotary,
            )
            for h in range(heads_a)
        ],
        slice(0, value_a.shape[1]),
        value_a.shape[1] // heads_a,
    )
    mixed_b = attend(
        [
            weigh(
                query_b[:, h * wide_b : (h + 1) * wide_b],
                slice(base_b + h * wide_b, base_b + (h + 1) * wide_b),
                wide_b,
            )
            for h in range(heads_b)
        ],
        slice(value_a.shape[1], value_a.shape[1] + value_b.shape[1]),
        value_b.shape[1] // heads_b,
    )

    chunks = head_part.shape[0]
    chunk_width = head_part.shape[3]

    def s_partner(c, slot):
        return send(
            head_part.at[c, (partner, diagonal)[slot]],
            head_from_partner.at[c, slot],
            sum_send.at[slot, c],
            sum_recv.at[slot, c],
            (me, partner),
        )

    def s_across(c):
        return send(
            head_pair.at[c], head_from_across.at[c], sum_send.at[2, c], sum_recv.at[2, c], (me, across)
        )

    for c in range(chunks):
        lanes = slice(c * chunk_width, (c + 1) * chunk_width)
        product = dot(mixed_a, out_a[:, lanes]) + dot(mixed_b, out_b[:, lanes])
        head_part[c] = product.astype(jnp.bfloat16).reshape(head_part.shape[1:])
        s_partner(c, 1).start()
        s_partner(c, 0).start()
    for c in range(chunks):
        s_partner(c, 1).wait_recv()
        both = head_part[c, across].astype(jnp.float32) + head_from_partner[c, 1].astype(jnp.float32)
        head_pair[c] = both.astype(jnp.bfloat16)
        s_across(c).start()

    for c in range(chunks):
        lanes = slice(c * chunk_width, (c + 1) * chunk_width)
        s_partner(c, 0).wait_recv()
        summed_rows = (
            residual[:, lanes].astype(jnp.float32)
            + head_part[c, column].astype(jnp.float32)
            + head_from_partner[c, 0].astype(jnp.float32)
        )
        s_across(c).wait_recv()
        summed_rows = summed_rows + head_from_across[c].astype(jnp.float32)
        hidden[:, lanes] = summed_rows.astype(jnp.bfloat16)
    normed = rms_scale(hidden[...], ffn_gain[...])
    outgoing[...] = dot(selection[...], normed).astype(jnp.bfloat16).reshape(outgoing.shape)

    def peer(k):
        result = 0
        bit = 1
        while bit < count:
            mine = lax.rem(me // bit, 2)
            other = lax.rem(k // bit, 2)
            result = result + bit * lax.rem(mine + other, 2)
            bit *= 2
        return result

    def over_sp(k):
        p = peer(k)
        return send(
            outgoing.at[p], rows.at[k, column], send_sem.at[0, k], recv_sem.at[0, k], (p, column)
        )

    def pass_on(k, source):
        target = rows.at[k, column]
        return (
            send(source, target, send_sem.at[1, k], recv_sem.at[1, k], (me, across)),
            send(source, target, send_sem.at[2, k], recv_sem.at[2, k], (me, partner)),
        )

    def arrival(kind, k, t):
        block = rows.at[k, t]
        return send(block, block, send_sem.at[kind, k], recv_sem.at[kind, k], (me, partner))

    def cross_on(k):
        block = rows.at[k, across]
        return send(block, block, send_sem.at[3, k], recv_sem.at[3, k], (me, partner))

    def to_partner(k, slot):
        wanted = (partner, diagonal)[slot]
        return send(
            part.at[k, wanted],
            from_partner.at[slot, k],
            send_sem.at[4 + slot, k],
            recv_sem.at[4 + slot, k],
            (me, partner),
        )

    def over_x(k):
        return send(
            pair.at[k], from_across.at[k], send_sem.at[6, k], recv_sem.at[6, k], (me, across)
        )

    def back(k):
        p = peer(k)
        return send(
            done.at[k], returned.at[me], send_sem.at[7, k], recv_sem.at[7, k], (p, column)
        )

    for copy in pass_on(0, outgoing.at[me]):
        copy.start()
    for k in (1, 4, 2, 5, 3, 6, 7):
        over_sp(k).start()
    rows[0, column] = outgoing[me]

    def arrived(k):
        arrival(0, k, column).wait_recv()
        for copy in pass_on(k, rows.at[k, column]):
            copy.start()

    def crossed(k):
        arrival(1, k, across).wait_recv()
        cross_on(k).start()

    def whole(k):
        arrival(2, k, partner).wait_recv()
        arrival(3, k, diagonal).wait_recv()

    def both_of(k, slot):
        kept = part[k, (column, across)[slot]].astype(jnp.float32)
        return kept + from_partner[slot, k].astype(jnp.float32)

    def paired(k):
        to_partner(k, 1).wait_recv()
        pair[k] = both_of(k, 1).astype(jnp.bfloat16)
        over_x(k).start()

    def summed(k):
        to_partner(k, 0).wait_recv()
        over_x(k).wait_recv()
        result = (both_of(k, 0) + from_across[k].astype(jnp.float32)).astype(jnp.bfloat16)

        @pl.when(k == 0)
        def _():
            returned[me] = result

        @pl.when(k > 0)
        def _():
            done[k] = result
            back(k).start()

    block_rows = rows.shape[1] * rows.shape[2]
    for load in loads[17:]:
        load.wait()

    def nth(i):
        return 0 if i == 0 else 1 + lax.rem(i - 1 + upper * (half - 1), count - 1)

    arrive, cross, couple, finish = arrived, crossed, paired, summed
    lower_waits = [
        [(arrive, 1), (cross, 0), (arrive, 2), (cross, 1), (arrive, 3)],
        [(cross, 2), (cross, 3), (couple, 1), (couple, 0)],
        [(arrive, 4), (arrive, 5), (couple, 2), (couple, 3), (finish, 1), (finish, 0), (arrive, 6), (cross, 4), (cross, 5)],
        [(arrive, 7), (couple, 4), (couple, 5), (finish, 2), (finish, 3), (cross, 6), (cross, 7)],
        [(couple, 6), (couple, 7), (finish, 4), (finish, 5), (finish, 6), (finish, 7)],
    ]
    upper_waits = [
        [(arrive, 1), (arrive, 2), (arrive, 3), (arrive, 4), (cross, 0), (cross, 1)],
        [(cross, 2), (arrive, 5), (cross, 3), (couple, 1)],
        [(arrive, 6), (arrive, 7), (couple, 2), (couple, 3), (finish, 1), (cross, 4), (cross, 5)],
        [(couple, 4), (couple, 5), (finish, 2), (finish, 3), (cross, 6), (cross, 7)],
        [(couple, 6), (couple, 7), (finish, 4), (finish, 5), (couple, 0), (finish, 6), (finish, 7), (finish, 0)],
    ]

    def turn(j):
        for side, waits in enumerate((lower_waits, upper_waits)):
            for step, now in enumerate(waits[:half]):

                @pl.when((upper == side) & (j == step))
                def _():
                    for event, i in now:
                        event(nth(i))

        start = (2 * j + count - 1) // count
        k_one = start * (1 + lax.rem(2 * j + count - 2 + upper * (half - 1), count - 1))
        k_two = 1 + lax.rem(2 * j + upper * (half - 1), count - 1)
        whole(k_one)
        whole(k_two)
        flat = jnp.concatenate(
            [rows[k_one].reshape(block_rows, width), rows[k_two].reshape(block_rows, width)], axis=0
        )
        gate_values = dot(flat, gate[...])
        up_values = dot(flat, up[...])
        act = (jax.nn.silu(gate_values) * up_values).astype(jnp.bfloat16)
        product = dot(act, down[...]).astype(jnp.bfloat16)
        part[k_one] = product[:block_rows].reshape(part.shape[1:])
        part[k_two] = product[block_rows:].reshape(part.shape[1:])
        for k in (k_one, k_two):
            to_partner(k, 1).start()
            to_partner(k, 0).start()

    loop(0, half, turn)
    for side, waits in enumerate((lower_waits, upper_waits)):

        @pl.when(upper == side)
        def _():
            for event, i in waits[half]:
                event(nth(i))


    def home(k):
        p = peer(k)
        send(
            done.at[k], returned.at[p], send_sem.at[7, k], recv_sem.at[7, k], (p, column)
        ).wait_recv()

    loop(1, count, home)
    flat_returned = returned[...].reshape(slots, width)
    mixed = dot_over(mixing[0], flat_returned, 0, 0) + dot_over(mixing[1], flat_returned, 0, 0)
    out_ref[...] = (hidden[...].astype(jnp.float32) + mixed).astype(jnp.bfloat16)

    def g_settle(k):
        s = origin(k)
        for copy in g_pass_on(s, gathered.at[s, column]):
            copy.wait_send()
        g_to_partner(s).wait_send()

    loop(0, me + 1, g_settle)
    loop(1, last, lambda k: g_over_sp(k).wait_send())

    @pl.when(upper == 0)
    def _():
        g_over_sp(half).wait_send()

    @pl.when(upper > 0)
    def _():
        loop(1, half, lambda i: g_hand_on(i).wait_send())

    for c in range(chunks):
        s_partner(c, 0).wait_send()
        s_partner(c, 1).wait_send()
        s_across(c).wait_send()

    def settle(k):
        for copy in pass_on(k, rows.at[k, column]):
            copy.wait_send()
        cross_on(k).wait_send()
        to_partner(k, 0).wait_send()
        to_partner(k, 1).wait_send()
        over_x(k).wait_send()

    loop(0, count, settle)

    def settle_far(k):
        over_sp(k).wait_send()
        back(k).wait_send()

    loop(1, count, settle_far)


def whole_layer(
    query_a,
    query_b,
    latent,
    rope_key,
    latent_gain,
    key_a_weight,
    value_a_weight,
    key_b_weight,
    value_b_weight,
    out_a_weight,
    out_b_weight,
    residual,
    ffn_gain,
    routes,
    route_weight,
    expert_gate,
    expert_up,
    expert_down,
    capacity,
):
    count, columns = lax.axis_size("sp"), lax.axis_size("tp")
    row_count, rank = latent.shape
    rotary = rope_key.shape[1]
    span = query_a.shape[0]
    width = residual.shape[1]
    heads_a = key_a_weight.shape[1] // NOPE_A
    heads_b = key_b_weight.shape[1] // NOPE_B
    table = jnp.asarray(turn_tables(np.arange(count * span), rotary))
    packed = rank + rotary + (-(rank + rotary) % 128)
    key_width = heads_a * 256 + heads_b * (NOPE_B + rotary)
    value_width = value_a_weight.shape[1] + value_b_weight.shape[1]
    chunks = 4
    chunk_width = width // chunks
    block = (count, capacity, width)
    every = (count, columns, capacity, width)
    operands = (
        query_a,
        query_b,
        latent,
        rope_key,
        latent_gain.reshape(1, rank),
        key_a_weight,
        value_a_weight,
        key_b_weight,
        value_b_weight,
        out_a_weight,
        out_b_weight,
        residual,
        ffn_gain.reshape(1, width),
        routes.T,
        route_weight.T,
        table,
        expert_gate,
        expert_up,
        expert_down,
    )
    bf16 = jnp.bfloat16

    def room(shape, dtype=bf16):
        return pltpu.VMEM(shape, dtype)

    loaded = [room(operand.shape, operand.dtype) for operand in operands[:15]]
    loaded += [room((row_count, 2 * rotary), jnp.float32), room((span, 2 * rotary), jnp.float32)]
    loaded += [room(operand.shape[1:], operand.dtype) for operand in operands[16:]]
    dma = pltpu.SemaphoreType.DMA
    return pl.pallas_call(
        functools.partial(layer_kernel, count, columns, heads_a, heads_b),
        out_shape=jax.ShapeDtypeStruct(residual.shape, bf16),
        in_specs=[pl.BlockSpec(memory_space=pl.ANY)] * len(operands),
        out_specs=pl.BlockSpec(memory_space=pltpu.VMEM),
        scratch_shapes=loaded
        + [
            room((row_count, packed)),
            room((count, columns, row_count, packed)),
            room((packed, key_width)),
            room((count, span, key_width)),
            room((count, span, value_width)),
            room((chunks, columns, row_count, chunk_width)),
            room((chunks, row_count, chunk_width)),
            room((chunks, 2, row_count, chunk_width)),
            room((chunks, row_count, chunk_width)),
            room(residual.shape),
            room((count * capacity, row_count)),
            room((2, count * capacity, row_count)),
            room(block),
            room(every),
            room(every),
            room((2,) + block),
            room(block),
            room(block),
            room(block),
            room(block),
            dma((len(operands) + 1,)),
            dma((5, count)),
            dma((4, count)),
            dma((3, chunks)),
            dma((3, chunks)),
            dma((8, count)),
            dma((8, count)),
        ],
        compiler_params=pltpu.CompilerParams(
            collective_id=5, has_side_effects=True, vmem_limit_bytes=60000 * 1024
        ),
    )(*operands)


def body(
    query_a,
    query_b,
    latent,
    rope_key,
    latent_gain,
    key_a_weight,
    value_a_weight,
    key_b_weight,
    value_b_weight,
    out_a_weight,
    out_b_weight,
    residual,
    ffn_gain,
    routes,
    route_weight,
    expert_gate,
    expert_up,
    expert_down,
):
    column_count = lax.axis_size("tp")
    row_count = latent.shape[0]
    experts = lax.axis_size("sp")
    capacity = max(2, 2 * TOP * row_count // experts)
    paired_up = experts & (experts - 1) == 0 and experts > 1 and column_count == 4
    if capacity % 16 == 0 and paired_up:
        return whole_layer(
            query_a,
            query_b,
            latent,
            rope_key,
            latent_gain,
            key_a_weight,
            value_a_weight,
            key_b_weight,
            value_b_weight,
            out_a_weight,
            out_b_weight,
            residual,
            ffn_gain,
            routes,
            route_weight,
            expert_gate,
            expert_up,
            expert_down,
            capacity,
        )
    span_size = query_a.shape[0]
    rotary_width = rope_key.shape[1]
    own_first = (lax.axis_index("sp") * column_count + lax.axis_index("tp")) * row_count
    query_first = lax.axis_index("sp") * span_size
    own_cosine, own_sine = angle_tables(
        own_first + jnp.arange(row_count, dtype=jnp.int32), rotary_width
    )
    normed_latent = rms_scale(latent, latent_gain)
    turned_key = rotate(rope_key, own_cosine, own_sine)
    query_cosine, query_sine = angle_tables(
        query_first + jnp.arange(span_size, dtype=jnp.int32), rotary_width
    )
    heads_a = key_a_weight.shape[1] // NOPE_A
    heads_b = key_b_weight.shape[1] // NOPE_B
    ready_a = prepare_queries(query_a, heads_a, NOPE_A, query_cosine, query_sine)
    ready_b = prepare_queries(query_b, heads_b, NOPE_B, query_cosine, query_sine)

    def start_state(head_count, value_width):
        return (
            jnp.full((head_count, span_size), masked_score, jnp.float32),
            jnp.zeros((head_count, span_size), jnp.float32),
            jnp.zeros((span_size, head_count, value_width), jnp.float32),
        )

    initial = (start_state(heads_a, VAL_A), start_state(heads_b, VAL_B))

    def attend_block(carried, keys_a, values_a, keys_b, values_b, key_turned):
        return (
            fold_group(carried[0], ready_a, keys_a, key_turned, values_a, query_first),
            fold_group(carried[1], ready_b, keys_b, key_turned, values_b, query_first),
        )

    rank = normed_latent.shape[1]
    filler = jnp.zeros((row_count, -(rank + rotary_width) % 128), jnp.bfloat16)
    packed = jnp.concatenate([normed_latent, turned_key, filler], axis=1)
    gathered = gather(packed[None], lax.axis_size("sp"), column_count, True, 0)
    gathered = gathered.reshape(-1, packed.shape[1])
    portion_latent = gathered[:, :rank]
    portion_turned = gathered[:, rank : rank + rotary_width]

    def compute(current):
        return attend_block(
            current,
            expand(portion_latent, key_a_weight, heads_a),
            expand(portion_latent, value_a_weight, heads_a),
            expand(portion_latent, key_b_weight, heads_b),
            expand(portion_latent, value_b_weight, heads_b),
            portion_turned,
        )

    folded = compute(initial)

    def finish(carried):
        top_score, weight_total, weighted = carried
        scaled = weighted / jnp.transpose(weight_total)[:, :, None]
        return scaled.astype(jnp.bfloat16).reshape(span_size, -1)

    out_a = finish(folded[0])
    out_b = finish(folded[1])
    projected = (
        jnp.dot(out_a, out_a_weight, preferred_element_type=jnp.float32)
        + jnp.dot(out_b, out_b_weight, preferred_element_type=jnp.float32)
    ).astype(jnp.bfloat16)
    model_width = residual.shape[1]
    chosen = routes.reshape(-1)
    expert_ids = jnp.arange(experts, dtype=jnp.int32)
    matches = (chosen[:, None] == expert_ids[None, :]).astype(jnp.int32)
    order_rank = jnp.sum((jnp.cumsum(matches, axis=0) - 1) * matches, axis=1)
    slot_index = (chosen * capacity + order_rank).reshape(row_count, TOP)
    slot_ids = jnp.arange(experts * capacity, dtype=jnp.int32)
    selection = jnp.sum(
        (slot_ids[:, None, None] == slot_index[None, :, :]).astype(jnp.bfloat16), axis=2
    )
    hidden_state, outgoing = hidden_sum(
        projected.reshape(column_count, row_count, -1), residual, ffn_gain, selection, 1
    )
    outgoing = outgoing.reshape(experts, capacity, model_width)
    if capacity % 16 == 0:
        places_of = slot_index.T.reshape(-1)
        selector = (places_of[:, None] == slot_ids[None, :]).astype(jnp.bfloat16)
        return through_experts(
            outgoing,
            selector,
            route_weight,
            hidden_state,
            expert_gate,
            expert_up,
            expert_down,
            column_count,
            4,
        )
    portion = gather(outgoing, experts, column_count, False, 2)
    portion_shape = portion.shape
    flat_rows = portion.reshape(-1, model_width)
    gate_values = jnp.dot(flat_rows, expert_gate[0], preferred_element_type=jnp.float32)
    up_values = jnp.dot(flat_rows, expert_up[0], preferred_element_type=jnp.float32)
    hidden = (jax.nn.silu(gate_values) * up_values).astype(jnp.bfloat16)
    partial_value = jnp.dot(hidden, expert_down[0], preferred_element_type=jnp.float32).astype(
        jnp.bfloat16
    )
    returned = give_back(partial_value.reshape(portion_shape), 3)
    flat_returned = returned.reshape(experts * capacity, model_width)
    expert_mix = jnp.zeros((row_count, model_width), jnp.float32)
    for route_index in range(TOP):
        selector = (slot_index[:, route_index][:, None] == slot_ids[None, :]).astype(jnp.bfloat16)
        picked = jnp.dot(selector, flat_returned, preferred_element_type=jnp.float32)
        expert_mix = expert_mix + route_weight[:, route_index][:, None] * picked
    return (hidden_state.astype(jnp.float32) + expert_mix).astype(jnp.bfloat16)


def solution(mesh):
    placed = (
        P("sp", "tp"),
        P("sp", "tp"),
        P(("sp", "tp"), None),
        P(("sp", "tp"), None),
        P(),
        P(None, "tp"),
        P(None, "tp"),
        P(None, "tp"),
        P(None, "tp"),
        P("tp", None),
        P("tp", None),
        P(("sp", "tp"), None),
        P(),
        P(("sp", "tp"), None),
        P(("sp", "tp"), None),
        P("sp", None, "tp"),
        P("sp", None, "tp"),
        P("sp", "tp", None),
    )
    return jax.shard_map(
        body, mesh=mesh, in_specs=placed, out_specs=P(("sp", "tp"), None), check_vma=False
    )
```

```python
import functools

import jax
import jax.numpy as jnp
import numpy as np
from jax import lax
from jax.experimental import pallas as pl
from jax.experimental.pallas import tpu as pltpu
from jax.sharding import PartitionSpec as P

NOPE_A = 128
VAL_A = 128
NOPE_B = 64
VAL_B = 64
TOP = 2


epsilon = 1e-06
base_theta = 500000.0
masked_score = -1e30


def rms_scale(values, scales):
    floats = values.astype(jnp.float32)
    scaled = floats * lax.rsqrt(jnp.mean(floats * floats, axis=-1, keepdims=True) + epsilon)
    return (scaled * scales).astype(jnp.bfloat16)


def angle_tables(positions, rotary_width):
    inverse = jnp.power(
        jnp.float32(base_theta), -jnp.arange(0, rotary_width, 2, dtype=jnp.float32) / rotary_width
    )
    angles = positions.astype(jnp.float32)[:, None] * inverse[None, :]
    return (jnp.cos(angles), jnp.sin(angles))


def rotate(values, cosine, sine_table):
    middle = cosine.shape[-1]
    first_half = values[..., :middle].astype(jnp.float32)
    second_half = values[..., middle:].astype(jnp.float32)
    turned = jnp.concatenate(
        [
            first_half * cosine - second_half * sine_table,
            second_half * cosine + first_half * sine_table,
        ],
        axis=-1,
    )
    return turned.astype(jnp.bfloat16)


def prepare_queries(queries, head_count, nope_width, cosine, sine_table):
    shaped = queries.reshape(queries.shape[0], head_count, queries.shape[1] // head_count)
    turned = rotate(shaped[:, :, nope_width:], cosine[:, None, :], sine_table[:, None, :])
    return jnp.concatenate([shaped[:, :, :nope_width], turned], axis=-1)


def fold_group(carried, queries, key_nope, key_turned, values, query_first):
    top_score, weight_total, weighted = carried
    nope_width = key_nope.shape[2]
    scale = (nope_width + key_turned.shape[1]) ** (-0.5)
    scores = jnp.einsum(
        "thd,shd->hts", queries[:, :, :nope_width], key_nope, preferred_element_type=jnp.float32
    )
    scores = scores + jnp.einsum(
        "thd,sd->hts", queries[:, :, nope_width:], key_turned, preferred_element_type=jnp.float32
    )
    scores = scores * scale
    query_places = query_first + jnp.arange(queries.shape[0], dtype=jnp.int32)
    key_places = jnp.arange(key_nope.shape[0], dtype=jnp.int32)
    allowed = (key_places[None, :] <= query_places[:, None])[None]
    scores = jnp.where(allowed, scores, masked_score)
    new_top = jnp.maximum(top_score, jnp.max(scores, axis=-1))
    weights = jnp.where(allowed, jnp.exp(scores - new_top[:, :, None]), 0.0)
    new_total = jnp.sum(weights, axis=-1)
    product = jnp.einsum(
        "hts,shd->thd", weights.astype(jnp.bfloat16), values, preferred_element_type=jnp.float32
    )
    return (new_top, new_total, product)


def expand(source, weight, head_count):
    product = jnp.dot(source, weight, preferred_element_type=jnp.float32).astype(jnp.bfloat16)
    return product.reshape(source.shape[0], head_count, weight.shape[1] // head_count)


MESH = pl.DeviceIdType.MESH


def places():
    me, column = lax.axis_index("sp"), lax.axis_index("tp")
    half = lax.axis_size("tp") // 2
    across = lax.rem(column + half, 2 * half)
    partner = column + 1 - 2 * lax.rem(column, 2)
    return me, column, across, partner


def send(source, target, send_sem, recv_sem, place):
    return pltpu.make_async_remote_copy(
        src_ref=source,
        dst_ref=target,
        send_sem=send_sem,
        recv_sem=recv_sem,
        device_id={"sp": place[0], "tp": place[1]},
        device_id_type=MESH,
    )


def greet(count, me, column, others):
    barrier = pltpu.get_barrier_semaphore()

    def step(k, carry):
        pl.semaphore_signal(
            barrier,
            inc=1,
            device_id={"sp": lax.rem(me + k, count), "tp": column},
            device_id_type=MESH,
        )
        return carry

    lax.fori_loop(1, count, step, 0)
    for other in others:
        pl.semaphore_signal(
            barrier, inc=1, device_id={"sp": me, "tp": other}, device_id_type=MESH
        )
    pl.semaphore_wait(barrier, max(count, 1) - 1 + len(others))


def loop(low, high, step):
    lax.fori_loop(low, high, lambda k, carry: (step(k), carry)[1], 0)


def gather_kernel(count, causal, in_ref, out_ref, send_sem, recv_sem):
    me, column, across, partner = places()
    diagonal = lax.rem(partner + lax.axis_size("tp") // 2, lax.axis_size("tp"))
    greet(count, me, column, (across, partner))

    def own(p):
        return in_ref.at[0] if causal else in_ref.at[p]

    def over_sp(k):
        p = lax.rem(me + k, count)
        return send(
            own(p), out_ref.at[me, column], send_sem.at[0, k], recv_sem.at[0, me], (p, column)
        )

    def arrival(kind, s, t):
        block = out_ref.at[s, t]
        return send(block, block, send_sem.at[kind, s], recv_sem.at[kind, s], (me, partner))

    def pass_on(s, source):
        target = out_ref.at[s, column]
        return (
            send(source, target, send_sem.at[1, s], recv_sem.at[1, s], (me, across)),
            send(source, target, send_sem.at[2, s], recv_sem.at[2, s], (me, partner)),
        )

    def to_partner(s):
        block = out_ref.at[s, across]
        return send(block, block, send_sem.at[3, s], recv_sem.at[3, s], (me, partner))

    last = count - me if causal else count
    arrivals = me + 1 if causal else count

    loop(1, last, lambda k: over_sp(last - k).start())
    for copy in pass_on(me, own(me)):
        copy.start()
    out_ref[me, column] = in_ref[0] if causal else in_ref[me]
    if causal:

        def clear(s):
            out_ref[s] = jnp.zeros(out_ref.shape[1:], out_ref.dtype)

        loop(me + 1, count, clear)

    def origin(k):
        return lax.rem(me + count - k, count)

    def arrived(k):
        s = origin(k)
        arrival(0, s, column).wait_recv()
        for copy in pass_on(s, out_ref.at[s, column]):
            copy.start()

    loop(1, arrivals, arrived)

    def crossed(k):
        s = origin(k)
        arrival(1, s, across).wait_recv()
        to_partner(s).start()

    loop(0, arrivals, crossed)

    def settle(k):
        s = origin(k)
        arrival(2, s, partner).wait_recv()
        arrival(3, s, diagonal).wait_recv()
        for copy in pass_on(s, out_ref.at[s, column]):
            copy.wait_send()
        to_partner(s).wait_send()

    loop(0, arrivals, settle)
    loop(1, last, lambda k: over_sp(k).wait_send())


def gather(blocks, count, columns, causal, collective_id):
    return pl.pallas_call(
        functools.partial(gather_kernel, count, causal),
        out_shape=jax.ShapeDtypeStruct((count, columns) + blocks.shape[1:], blocks.dtype),
        in_specs=[pl.BlockSpec(memory_space=pltpu.VMEM)],
        out_specs=pl.BlockSpec(memory_space=pltpu.VMEM),
        scratch_shapes=[
            pltpu.SemaphoreType.DMA((4, count)),
            pltpu.SemaphoreType.DMA((4, count)),
        ],
        compiler_params=pltpu.CompilerParams(
            collective_id=collective_id, has_side_effects=True, vmem_limit_bytes=60000 * 1024
        ),
    )(blocks)


def hidden_kernel(
    columns, part_ref, residual_ref, gain_ref, pick_ref, hidden_ref, outgoing_ref, held, send_sem, recv_sem
):
    me, column, _, _ = places()
    others = [lax.rem(column + k, columns) for k in range(1, columns)]
    greet(1, me, column, others)
    copies = []
    for k, other in enumerate(others):
        copies.append(
            send(part_ref.at[other], held.at[k], send_sem.at[k], recv_sem.at[k], (me, other))
        )
    for copy in copies:
        copy.start()
    total = residual_ref[...].astype(jnp.float32) + part_ref[column].astype(jnp.float32)
    for k, copy in enumerate(copies):
        copy.wait_recv()
        total = total + held[k].astype(jnp.float32)
    hidden = total.astype(jnp.bfloat16)
    hidden_ref[...] = hidden
    normed = rms_scale(hidden, gain_ref[...])
    outgoing = jnp.dot(pick_ref[...], normed, preferred_element_type=jnp.float32)
    outgoing_ref[...] = outgoing.astype(jnp.bfloat16)
    for copy in copies:
        copy.wait_send()


def hidden_sum(parts, residual, gain, selection, collective_id):
    columns, rows, width = parts.shape
    return pl.pallas_call(
        functools.partial(hidden_kernel, columns),
        out_shape=[
            jax.ShapeDtypeStruct((rows, width), jnp.bfloat16),
            jax.ShapeDtypeStruct((selection.shape[0], width), jnp.bfloat16),
        ],
        in_specs=[pl.BlockSpec(memory_space=pltpu.VMEM)] * 4,
        out_specs=[pl.BlockSpec(memory_space=pltpu.VMEM)] * 2,
        scratch_shapes=[
            pltpu.VMEM((columns - 1, rows, width), jnp.bfloat16),
            pltpu.SemaphoreType.DMA((columns - 1,)),
            pltpu.SemaphoreType.DMA((columns - 1,)),
        ],
        compiler_params=pltpu.CompilerParams(
            collective_id=collective_id, has_side_effects=True, vmem_limit_bytes=60000 * 1024
        ),
    )(parts, residual, gain.reshape(1, width), selection)


def return_kernel(
    count, in_ref, out_ref, from_partner, pair, mine, from_across, done, send_sem, recv_sem
):
    me, column, across, partner = places()
    diagonal = lax.rem(partner + lax.axis_size("tp") // 2, lax.axis_size("tp"))
    greet(count, me, column, (across, partner))

    def place(k):
        return lax.rem(me + 1 + k, count)

    def to_partner(s, slot):
        wanted = (partner, diagonal)[slot]
        return send(
            in_ref.at[s, wanted],
            from_partner.at[slot, s],
            send_sem.at[slot, s],
            recv_sem.at[slot, s],
            (me, partner),
        )

    def over_x(s):
        return send(
            pair.at[s], from_across.at[s], send_sem.at[2, s], recv_sem.at[2, s], (me, across)
        )

    def back(s):
        return send(
            done.at[s], out_ref.at[me], send_sem.at[3, s], recv_sem.at[3, me], (s, column)
        )

    def start(k):
        s = place(k)
        to_partner(s, 1).start()
        to_partner(s, 0).start()

    loop(0, count, start)

    def both(s, slot):
        kept = in_ref[s, (column, across)[slot]].astype(jnp.float32)
        return kept + from_partner[slot, s].astype(jnp.float32)

    def paired(k):
        s = place(k)
        to_partner(s, 1).wait_recv()
        pair[s] = both(s, 1).astype(jnp.bfloat16)
        over_x(s).start()

    loop(0, count, paired)

    def total(s):
        to_partner(s, 0).wait_recv()
        mine[...] = both(s, 0)
        over_x(s).wait_recv()
        return (mine[...] + from_across[s].astype(jnp.float32)).astype(jnp.bfloat16)

    def summed(k):
        s = place(k)
        done[s] = total(s)
        back(s).start()

    loop(0, count - 1, summed)
    out_ref[me] = total(me)

    def arrived(k):
        s = place(k)
        send(
            done.at[s], out_ref.at[s], send_sem.at[3, s], recv_sem.at[3, s], (s, column)
        ).wait_recv()
        back(s).wait_send()

    loop(0, count - 1, arrived)

    def settle(s):
        to_partner(s, 0).wait_send()
        to_partner(s, 1).wait_send()
        over_x(s).wait_send()

    loop(0, count, settle)


def give_back(partials, collective_id):
    count, _, rows, width = partials.shape
    block = (count, rows, width)
    return pl.pallas_call(
        functools.partial(return_kernel, count),
        out_shape=jax.ShapeDtypeStruct(block, jnp.bfloat16),
        in_specs=[pl.BlockSpec(memory_space=pltpu.VMEM)],
        out_specs=pl.BlockSpec(memory_space=pltpu.VMEM),
        scratch_shapes=[
            pltpu.VMEM((2,) + block, jnp.bfloat16),
            pltpu.VMEM(block, jnp.bfloat16),
            pltpu.VMEM(block[1:], jnp.float32),
            pltpu.VMEM(block, jnp.bfloat16),
            pltpu.VMEM(block, jnp.bfloat16),
            pltpu.SemaphoreType.DMA((4, count)),
            pltpu.SemaphoreType.DMA((4, count)),
        ],
        compiler_params=pltpu.CompilerParams(
            collective_id=collective_id, has_side_effects=True, vmem_limit_bytes=60000 * 1024
        ),
    )(partials)


def experts_kernel(
    count,
    group,
    in_ref,
    selector_ref,
    share_ref,
    hidden_ref,
    gate_hbm,
    up_hbm,
    down_hbm,
    out_ref,
    rows,
    part,
    from_partner,
    pair,
    from_across,
    done,
    returned,
    gate,
    up,
    down,
    weight_sem,
    send_sem,
    recv_sem,
):
    me, column, across, partner = places()
    diagonal = lax.rem(partner + lax.axis_size("tp") // 2, lax.axis_size("tp"))
    loads = [
        pltpu.make_async_copy(source.at[0], target, weight_sem.at[index])
        for index, (source, target) in enumerate(((gate_hbm, gate), (up_hbm, up), (down_hbm, down)))
    ]
    for load in loads:
        load.start()
    greet(count, me, column, (across, partner))

    def origin(k):
        return lax.rem(me + count - k, count)

    def over_sp(k):
        p = lax.rem(me + k, count)
        return send(
            in_ref.at[p], rows.at[me, column], send_sem.at[0, k], recv_sem.at[0, me], (p, column)
        )

    def arrival(kind, s, t):
        block = rows.at[s, t]
        return send(block, block, send_sem.at[kind, s], recv_sem.at[kind, s], (me, partner))

    def pass_on(s, source):
        target = rows.at[s, column]
        return (
            send(source, target, send_sem.at[1, s], recv_sem.at[1, s], (me, across)),
            send(source, target, send_sem.at[2, s], recv_sem.at[2, s], (me, partner)),
        )

    def cross_on(s):
        block = rows.at[s, across]
        return send(block, block, send_sem.at[3, s], recv_sem.at[3, s], (me, partner))

    def to_partner(s, slot):
        wanted = (partner, diagonal)[slot]
        return send(
            part.at[s, wanted],
            from_partner.at[slot, s],
            send_sem.at[4 + slot, s],
            recv_sem.at[4 + slot, s],
            (me, partner),
        )

    def over_x(s):
        return send(
            pair.at[s], from_across.at[s], send_sem.at[6, s], recv_sem.at[6, s], (me, across)
        )

    def back(s):
        return send(
            done.at[s], returned.at[me], send_sem.at[7, s], recv_sem.at[7, me], (s, column)
        )

    loop(1, count, lambda k: over_sp(k).start())
    for copy in pass_on(me, in_ref.at[me]):
        copy.start()
    rows[me, column] = in_ref[me]

    def arrived(k):
        s = origin(k)
        arrival(0, s, column).wait_recv()
        for copy in pass_on(s, rows.at[s, column]):
            copy.start()

    def both(s, slot):
        kept = part[s, (column, across)[slot]].astype(jnp.float32)
        return kept + from_partner[slot, s].astype(jnp.float32)

    def paired(k):
        s = origin(k)
        to_partner(s, 1).wait_recv()
        pair[s] = both(s, 1).astype(jnp.bfloat16)
        over_x(s).start()

    def summed(k):
        s = origin(k)
        to_partner(s, 0).wait_recv()
        over_x(s).wait_recv()
        total = (both(s, 0) + from_across[s].astype(jnp.float32)).astype(jnp.bfloat16)

        @pl.when(k == 0)
        def _():
            returned[me] = total

        @pl.when(k > 0)
        def _():
            done[s] = total
            back(s).start()

    loop(1, group, arrived)
    block_rows = rows.shape[1] * rows.shape[2]
    width = rows.shape[3]

    def turn(j):
        first = j * group

        @pl.when(first + group < count)
        def _():
            loop(first + group, first + 2 * group, arrived)

        def crossed(k):
            s = origin(k)
            arrival(1, s, across).wait_recv()
            cross_on(s).start()

        loop(first, first + group, crossed)

        def whole(k):
            s = origin(k)
            arrival(2, s, partner).wait_recv()
            arrival(3, s, diagonal).wait_recv()

        loop(first, first + group, whole)

        @pl.when(j == 0)
        def _():
            for load in loads:
                load.wait()

        sources = [origin(first + i) for i in range(group)]
        flat = jnp.concatenate([rows[s].reshape(block_rows, width) for s in sources], axis=0)
        gate_values = jnp.dot(flat, gate[...], preferred_element_type=jnp.float32)
        up_values = jnp.dot(flat, up[...], preferred_element_type=jnp.float32)
        hidden = (jax.nn.silu(gate_values) * up_values).astype(jnp.bfloat16)
        product = jnp.dot(hidden, down[...], preferred_element_type=jnp.float32)
        product = product.astype(jnp.bfloat16)
        for i, s in enumerate(sources):
            part[s] = product[i * block_rows : (i + 1) * block_rows].reshape(rows.shape[1:])

        def leave(k):
            s = origin(k)
            to_partner(s, 1).start()
            to_partner(s, 0).start()

        loop(first, first + group, leave)

        @pl.when(j > 0)
        def _():
            loop(first - group, first, paired)

        @pl.when(j > 1)
        def _():
            loop(first - 2 * group, first - group, summed)

    turns = count // group
    loop(0, turns, turn)
    loop(count - group, count, paired)
    loop(max(turns - 2, 0) * group, count, summed)

    def home(k):
        s = origin(k)
        send(
            done.at[s], returned.at[s], send_sem.at[7, s], recv_sem.at[7, s], (s, column)
        ).wait_recv()
        back(s).wait_send()

    loop(1, count, home)
    picked = jnp.dot(
        selector_ref[...], returned[...].reshape(-1, width), preferred_element_type=jnp.float32
    )
    own_rows = hidden_ref.shape[0]
    mixed = jnp.zeros(hidden_ref.shape, jnp.float32)
    for route_index in range(TOP):
        mixed = mixed + (
            share_ref[:, route_index : route_index + 1]
            * picked[route_index * own_rows : (route_index + 1) * own_rows]
        )
    out_ref[...] = (hidden_ref[...].astype(jnp.float32) + mixed).astype(jnp.bfloat16)

    def settle(s):
        for copy in pass_on(s, rows.at[s, column]):
            copy.wait_send()
        cross_on(s).wait_send()
        to_partner(s, 0).wait_send()
        to_partner(s, 1).wait_send()
        over_x(s).wait_send()

    loop(0, count, settle)
    loop(1, count, lambda k: over_sp(k).wait_send())


def through_experts(outgoing, selector, share, hidden, gate, up, down, columns, collective_id):
    count, rows, width = outgoing.shape
    group = 2 if count % 2 == 0 else 1
    block = (count, rows, width)
    every = (count, columns, rows, width)
    return pl.pallas_call(
        functools.partial(experts_kernel, count, group),
        out_shape=jax.ShapeDtypeStruct(hidden.shape, jnp.bfloat16),
        in_specs=[pl.BlockSpec(memory_space=pltpu.VMEM)] * 4
        + [pl.BlockSpec(memory_space=pl.ANY)] * 3,
        out_specs=pl.BlockSpec(memory_space=pltpu.VMEM),
        scratch_shapes=[
            pltpu.VMEM(every, jnp.bfloat16),
            pltpu.VMEM(every, jnp.bfloat16),
            pltpu.VMEM((2,) + block, jnp.bfloat16),
            pltpu.VMEM(block, jnp.bfloat16),
            pltpu.VMEM(block, jnp.bfloat16),
            pltpu.VMEM(block, jnp.bfloat16),
            pltpu.VMEM(block, jnp.bfloat16),
            pltpu.VMEM(gate.shape[1:], jnp.bfloat16),
            pltpu.VMEM(up.shape[1:], jnp.bfloat16),
            pltpu.VMEM(down.shape[1:], jnp.bfloat16),
            pltpu.SemaphoreType.DMA((3,)),
            pltpu.SemaphoreType.DMA((8, count)),
            pltpu.SemaphoreType.DMA((8, count)),
        ],
        compiler_params=pltpu.CompilerParams(
            collective_id=collective_id, has_side_effects=True, vmem_limit_bytes=60000 * 1024
        ),
    )(outgoing, selector, share, hidden, gate, up, down)


def turn_tables(positions, rotary_width):
    inverse = np.power(
        np.float32(base_theta), -np.arange(0, rotary_width, 2, dtype=np.float32) / rotary_width
    ).astype(np.float32)
    angles = positions.astype(np.float32)[:, None] * inverse[None, :]
    cosine, sine = np.cos(angles), np.sin(angles)
    return np.concatenate([cosine, cosine, -sine, sine], axis=1).astype(np.float32)


def iotas(shape):
    return (
        lax.broadcasted_iota(jnp.int32, shape, 0),
        lax.broadcasted_iota(jnp.int32, shape, 1),
    )


def dot(left, right):
    return jnp.dot(left, right, preferred_element_type=jnp.float32)


def dot_over(left, right, left_dim, right_dim):
    return lax.dot_general(
        left, right, (((left_dim,), (right_dim,)), ((), ())), preferred_element_type=jnp.float32
    )


def layer_kernel(
    count,
    columns,
    heads_a,
    heads_b,
    query_a_hbm,
    query_b_hbm,
    latent_hbm,
    rope_hbm,
    latent_gain_hbm,
    key_a_hbm,
    value_a_hbm,
    key_b_hbm,
    value_b_hbm,
    out_a_hbm,
    out_b_hbm,
    residual_hbm,
    ffn_gain_hbm,
    routes_hbm,
    share_hbm,
    table_hbm,
    gate_hbm,
    up_hbm,
    down_hbm,
    out_ref,
    query_a,
    query_b,
    latent,
    rope,
    latent_gain,
    key_a,
    value_a,
    key_b,
    value_b,
    out_a,
    out_b,
    residual,
    ffn_gain,
    routes,
    share,
    own_table,
    query_table,
    gate,
    up,
    down,
    own,
    gathered,
    key_weight,
    keys,
    values,
    head_part,
    head_pair,
    head_from_partner,
    head_from_across,
    hidden,
    selection,
    mixing,
    outgoing,
    rows,
    part,
    from_partner,
    pair,
    from_across,
    done,
    returned,
    load_sem,
    gather_send,
    gather_recv,
    sum_send,
    sum_recv,
    send_sem,
    recv_sem,
):
    me, column, across, partner = places()
    diagonal = lax.rem(partner + columns // 2, columns)
    row_count = latent.shape[0]
    span = query_a.shape[0]
    rank = latent.shape[1]
    rotary = rope.shape[1]
    width = residual.shape[1]
    total = count * span

    own_first = pl.multiple_of((me * columns + column) * row_count, row_count)
    query_first = pl.multiple_of(me * span, span)
    plan = [
        (latent_hbm, latent),
        (rope_hbm, rope),
        (latent_gain_hbm, latent_gain),
        (table_hbm.at[pl.ds(own_first, row_count)], own_table),
        (key_a_hbm, key_a),
        (key_b_hbm, key_b),
        (query_a_hbm, query_a),
        (query_b_hbm, query_b),
        (table_hbm.at[pl.ds(query_first, span)], query_table),
        (value_a_hbm, value_a),
        (value_b_hbm, value_b),
        (routes_hbm, routes),
        (share_hbm, share),
        (out_a_hbm, out_a),
        (out_b_hbm, out_b),
        (residual_hbm, residual),
        (ffn_gain_hbm, ffn_gain),
        (gate_hbm.at[0], gate),
        (up_hbm.at[0], up),
        (down_hbm.at[0], down),
    ]
    loads = [
        pltpu.make_async_copy(source, target, load_sem.at[index])
        for index, (source, target) in enumerate(plan)
    ]
    for load in loads[:17]:
        load.start()

    barrier = pltpu.get_barrier_semaphore()

    def hello(k, carry):
        pl.semaphore_signal(
            barrier,
            inc=1,
            device_id={"sp": lax.rem(me + k, count), "tp": column},
            device_id_type=MESH,
        )
        return carry

    lax.fori_loop(1, count, hello, 0)
    for other in (across, partner):
        pl.semaphore_signal(
            barrier, inc=1, device_id={"sp": me, "tp": other}, device_id_type=MESH
        )

    for load in loads[:4]:
        load.wait()
    row, col = iotas((128, 128))
    swap = (row == jnp.where(jnp.bitwise_and(col, rotary - 1) < rotary // 2, col + rotary // 2, col - rotary // 2))
    swap = swap.astype(jnp.bfloat16)
    own[:, :rank] = rms_scale(latent[...], latent_gain[...])
    key = rope[...]
    turned = key.astype(jnp.float32) * own_table[:, :rotary] + (
        dot(key, swap[:rotary, :rotary]) * own_table[:, rotary:]
    )
    own[:, rank : rank + rotary] = turned.astype(jnp.bfloat16)
    own[:, rank + rotary :] = jnp.zeros(
        (row_count, own.shape[1] - rank - rotary), jnp.bfloat16
    )
    for load in loads[4:13]:
        load.wait()
    nope_a = key_a.shape[1] // heads_a
    nope_b = key_b.shape[1] // heads_b
    wide_a = 256
    wide_b = nope_b + rotary
    starts_a = []
    for h in range(heads_a):
        start = h * (nope_a + rotary)
        starts_a.append(start // 128 * 128)
        pad = start - starts_a[h]
        r, c = iotas((key_a.shape[1], wide_a))
        inside = (c >= pad) & (c < pad + nope_a)
        piece = ((r - c == h * nope_a - pad) & inside).astype(jnp.bfloat16)
        lanes = slice(h * wide_a, (h + 1) * wide_a)
        key_weight[:rank, lanes] = dot(key_a[...], piece).astype(jnp.bfloat16)
        r, c = iotas((own.shape[1] - rank, wide_a))
        key_weight[rank:, lanes] = ((c - r == pad + nope_a) & (r < rotary)).astype(jnp.bfloat16)
    base_b = heads_a * wide_a
    for h in range(heads_b):
        r, c = iotas((key_b.shape[1], wide_b))
        piece = ((r - c == h * nope_b) & (c < nope_b)).astype(jnp.bfloat16)
        lanes = slice(base_b + h * wide_b, base_b + (h + 1) * wide_b)
        key_weight[:rank, lanes] = dot(key_b[...], piece).astype(jnp.bfloat16)
        r, c = iotas((own.shape[1] - rank, wide_b))
        key_weight[rank:, lanes] = ((c - r == nope_b) & (r < rotary)).astype(jnp.bfloat16)

    lane = lax.broadcasted_iota(jnp.int32, (span, 128), 1)
    table = query_table[...]
    rolled = jnp.concatenate([table[:, rotary:], table[:, :rotary]], axis=1)
    low = lane < rotary
    one = jnp.ones((span, 128), jnp.float32)
    zero = jnp.zeros((span, 128), jnp.float32)
    turn_low = (jnp.where(low, table, one), jnp.where(low, rolled, zero))
    turn_high = (jnp.where(low, one, rolled), jnp.where(low, zero, table))

    def turn_tile(ref, start, factors):
        tile = ref[:, start : start + 128]
        turned_tile = tile.astype(jnp.float32) * factors[0] + dot(tile, swap) * factors[1]
        ref[:, start : start + 128] = turned_tile.astype(jnp.bfloat16)

    for h in range(heads_a):
        start = h * (nope_a + rotary) + nope_a
        turn_tile(query_a, start // 128 * 128, turn_low if start % 128 == 0 else turn_high)
    for h in range(heads_b):
        turn_tile(query_b, h * wide_b, turn_high)

    capacity = outgoing.shape[1]
    slots = count * capacity
    expert_at = lax.broadcasted_iota(jnp.int32, (count, row_count), 0)
    before = iotas((row_count, row_count))
    before = (before[0] < before[1]).astype(jnp.bfloat16)
    slot_at = lax.broadcasted_iota(jnp.int32, (slots, row_count), 0)
    earlier = jnp.zeros((count, 1), jnp.float32)
    picks = []
    for k in range(TOP):
        expert = routes[k : k + 1, :]
        named = (expert_at == expert).astype(jnp.float32)
        place = dot(named.astype(jnp.bfloat16), before) + earlier
        place = jnp.sum(place * named, axis=0, keepdims=True).astype(jnp.int32)
        picks.append((slot_at == expert * capacity + place).astype(jnp.float32))
        earlier = earlier + jnp.sum(named, axis=1, keepdims=True)
    selection[...] = functools.reduce(lambda a, b: a + b, picks).astype(jnp.bfloat16)
    mix = functools.reduce(
        lambda a, b: a + b, [pick * share[k : k + 1, :] for k, pick in enumerate(picks)]
    )
    mix_high = mix.astype(jnp.bfloat16)
    mixing[0] = mix_high
    mixing[1] = (mix - mix_high.astype(jnp.float32)).astype(jnp.bfloat16)

    pl.semaphore_wait(barrier, count + 1)

    half = count // 2
    upper = me // half
    at = lax.rem(me, half)

    def g_over_sp(k):
        p = lax.rem(me + k, count)
        return send(
            own, gathered.at[me, column], gather_send.at[0, k], gather_recv.at[0, me], (p, column)
        )

    def g_hand_on(k):
        p = upper * half + lax.rem(at + k, half)
        block = gathered.at[at, column]
        return send(block, block, gather_send.at[4, k], gather_recv.at[0, at], (p, column))

    def g_arrival(kind, s, t):
        block = gathered.at[s, t]
        return send(
            block, block, gather_send.at[kind, s], gather_recv.at[kind, s], (me, partner)
        )

    def g_pass_on(s, source):
        target = gathered.at[s, column]
        return (
            send(source, target, gather_send.at[1, s], gather_recv.at[1, s], (me, across)),
            send(source, target, gather_send.at[2, s], gather_recv.at[2, s], (me, partner)),
        )

    def g_to_partner(s):
        block = gathered.at[s, across]
        return send(
            block, block, gather_send.at[3, s], gather_recv.at[3, s], (me, partner)
        )

    last = half - at

    @pl.when(upper == 0)
    def _():
        g_over_sp(half).start()

    for copy in g_pass_on(me, own):
        copy.start()
    loop(1, last, lambda k: g_over_sp(last - k).start())
    gathered[me, column] = own[...]

    def clear(s):
        values[s] = jnp.zeros(values.shape[1:], values.dtype)
        keys[s] = jnp.zeros(keys.shape[1:], keys.dtype)

    loop(me + 1, count, clear)

    def origin(k):
        later = (k + count - at - 1) // count
        return (1 - later) * (me - k) + later * lax.rem(k - 1 + half, half)

    def g_arrived(k):
        s = origin(k)
        g_arrival(0, s, column).wait_recv()

        @pl.when(k == at + 1)
        def _():
            loop(1, half, lambda i: g_hand_on(i).start())

        for copy in g_pass_on(s, gathered.at[s, column]):
            copy.start()


    def g_step(k):
        @pl.when(k <= me)
        def _():
            s = origin(k)
            g_arrival(1, s, across).wait_recv()
            g_to_partner(s).start()

        @pl.when(k >= 1)
        def _():
            s = origin(k - 1)
            g_arrival(2, s, partner).wait_recv()
            g_arrival(3, s, diagonal).wait_recv()
            packed = gathered[s].reshape(span, own.shape[1])
            keys[s] = dot(packed, key_weight[...]).astype(jnp.bfloat16)
            values[s, :, : value_a.shape[1]] = dot(packed[:, :rank], value_a[...]).astype(
                jnp.bfloat16
            )
            values[s, :, value_a.shape[1] :] = dot(packed[:, :rank], value_b[...]).astype(
                jnp.bfloat16
            )

    first = at + 1 + upper
    loop(1, first, g_arrived)
    loop(0, first, g_step)
    loop(first, me + 1, g_arrived)
    for load in loads[17:]:
        load.start()
    loop(first, me + 2, g_step)

    query_at, key_at = iotas((span, total))
    allowed = key_at <= query_at + query_first

    def weigh(queries, lanes, size):
        scores = dot_over(queries, keys[:, :, lanes].reshape(total, -1), 1, 1)
        scores = jnp.where(allowed, scores, masked_score)
        top = jnp.max(scores, axis=1, keepdims=True)
        weights = jnp.exp((scores - top) * size ** (-0.5))
        return weights.astype(jnp.bfloat16), jnp.sum(weights, axis=1, keepdims=True)

    def attend(parts, lanes, each):
        group = values[:, :, lanes].reshape(total, -1)
        results = [dot(weights, group) / sums for weights, sums in parts]
        result = results[0]
        place = lax.broadcasted_iota(jnp.int32, result.shape, 1)
        for h in range(1, len(parts)):
            result = jnp.where(place < h * each, result, results[h])
        return result.astype(jnp.bfloat16)

    for load in loads[13:17]:
        load.wait()
    mixed_a = attend(
        [
            weigh(
                query_a[:, starts_a[h] : starts_a[h] + wide_a],
                slice(h * wide_a, (h + 1) * wide_a),
                nope_a + rotary,
            )
            for h in range(heads_a)
        ],
        slice(0, value_a.shape[1]),
        value_a.shape[1] // heads_a,
    )
    mixed_b = attend(
        [
            weigh(
                query_b[:, h * wide_b : (h + 1) * wide_b],
                slice(base_b + h * wide_b, base_b + (h + 1) * wide_b),
                wide_b,
            )
            for h in range(heads_b)
        ],
        slice(value_a.shape[1], value_a.shape[1] + value_b.shape[1]),
        value_b.shape[1] // heads_b,
    )

    chunks = head_part.shape[0]
    chunk_width = head_part.shape[3]

    def s_partner(c, slot):
        return send(
            head_part.at[c, (partner, diagonal)[slot]],
            head_from_partner.at[c, slot],
            sum_send.at[slot, c],
            sum_recv.at[slot, c],
            (me, partner),
        )

    def s_across(c):
        return send(
            head_pair.at[c], head_from_across.at[c], sum_send.at[2, c], sum_recv.at[2, c], (me, across)
        )

    for c in range(chunks):
        lanes = slice(c * chunk_width, (c + 1) * chunk_width)
        product = dot(mixed_a, out_a[:, lanes]) + dot(mixed_b, out_b[:, lanes])
        head_part[c] = product.astype(jnp.bfloat16).reshape(head_part.shape[1:])
        s_partner(c, 1).start()
        s_partner(c, 0).start()
    for c in range(chunks):
        s_partner(c, 1).wait_recv()
        both = head_part[c, across].astype(jnp.float32) + head_from_partner[c, 1].astype(jnp.float32)
        head_pair[c] = both.astype(jnp.bfloat16)
        s_across(c).start()

    for c in range(chunks):
        lanes = slice(c * chunk_width, (c + 1) * chunk_width)
        s_partner(c, 0).wait_recv()
        summed_rows = (
            residual[:, lanes].astype(jnp.float32)
            + head_part[c, column].astype(jnp.float32)
            + head_from_partner[c, 0].astype(jnp.float32)
        )
        s_across(c).wait_recv()
        summed_rows = summed_rows + head_from_across[c].astype(jnp.float32)
        hidden[:, lanes] = summed_rows.astype(jnp.bfloat16)
    normed = rms_scale(hidden[...], ffn_gain[...])
    outgoing[...] = dot(selection[...], normed).astype(jnp.bfloat16).reshape(outgoing.shape)

    def peer(k):
        result = 0
        bit = 1
        while bit < count:
            mine = lax.rem(me // bit, 2)
            other = lax.rem(k // bit, 2)
            result = result + bit * lax.rem(mine + other, 2)
            bit *= 2
        return result

    def over_sp(k):
        p = peer(k)
        return send(
            outgoing.at[p], rows.at[k, column], send_sem.at[0, k], recv_sem.at[0, k], (p, column)
        )

    def pass_on(k, source):
        target = rows.at[k, column]
        return (
            send(source, target, send_sem.at[1, k], recv_sem.at[1, k], (me, across)),
            send(source, target, send_sem.at[2, k], recv_sem.at[2, k], (me, partner)),
        )

    def arrival(kind, k, t):
        block = rows.at[k, t]
        return send(block, block, send_sem.at[kind, k], recv_sem.at[kind, k], (me, partner))

    def cross_on(k):
        block = rows.at[k, across]
        return send(block, block, send_sem.at[3, k], recv_sem.at[3, k], (me, partner))

    def to_partner(k, slot):
        wanted = (partner, diagonal)[slot]
        return send(
            part.at[k, wanted],
            from_partner.at[slot, k],
            send_sem.at[4 + slot, k],
            recv_sem.at[4 + slot, k],
            (me, partner),
        )

    def over_x(k):
        return send(
            pair.at[k], from_across.at[k], send_sem.at[6, k], recv_sem.at[6, k], (me, across)
        )

    def back(k):
        p = peer(k)
        return send(
            done.at[k], returned.at[me], send_sem.at[7, k], recv_sem.at[7, k], (p, column)
        )

    for copy in pass_on(0, outgoing.at[me]):
        copy.start()
    for k in (1, 4, 2, 5, 3, 6, 7):
        over_sp(k).start()
    rows[0, column] = outgoing[me]

    def arrived(k):
        arrival(0, k, column).wait_recv()
        for copy in pass_on(k, rows.at[k, column]):
            copy.start()

    def crossed(k):
        arrival(1, k, across).wait_recv()
        cross_on(k).start()

    def whole(k):
        arrival(2, k, partner).wait_recv()
        arrival(3, k, diagonal).wait_recv()

    def both_of(k, slot):
        kept = part[k, (column, across)[slot]].astype(jnp.float32)
        return kept + from_partner[slot, k].astype(jnp.float32)

    def paired(k):
        to_partner(k, 1).wait_recv()
        pair[k] = both_of(k, 1).astype(jnp.bfloat16)
        over_x(k).start()

    def summed(k):
        to_partner(k, 0).wait_recv()
        over_x(k).wait_recv()
        result = (both_of(k, 0) + from_across[k].astype(jnp.float32)).astype(jnp.bfloat16)

        @pl.when(k == 0)
        def _():
            returned[me] = result

        @pl.when(k > 0)
        def _():
            done[k] = result
            back(k).start()

    block_rows = rows.shape[1] * rows.shape[2]
    for load in loads[17:]:
        load.wait()

    def nth(i):
        return 0 if i == 0 else 1 + lax.rem(i - 1 + upper * (half - 1), count - 1)

    arrive, cross, couple, finish = arrived, crossed, paired, summed
    lower_waits = [
        [(arrive, 1), (cross, 0), (arrive, 2), (cross, 1), (arrive, 3)],
        [(cross, 2), (cross, 3), (couple, 1), (couple, 0)],
        [(arrive, 4), (arrive, 5), (couple, 2), (couple, 3), (finish, 1), (finish, 0), (arrive, 6), (cross, 4), (cross, 5), (arrive, 7)],
        [(couple, 4), (couple, 5), (finish, 2), (finish, 3), (cross, 6), (cross, 7)],
        [(couple, 6), (couple, 7), (finish, 4), (finish, 5), (finish, 6), (finish, 7)],
    ]
    upper_waits = [
        [(arrive, 1), (arrive, 2), (arrive, 3), (arrive, 4), (cross, 0), (cross, 1)],
        [(arrive, 5), (arrive, 6), (cross, 2), (cross, 3), (couple, 1)],
        [(arrive, 7), (couple, 2), (couple, 3), (finish, 1), (cross, 4), (cross, 5)],
        [(couple, 4), (couple, 5), (finish, 2), (finish, 3), (cross, 6), (cross, 7)],
        [(couple, 6), (couple, 7), (finish, 4), (finish, 5), (couple, 0), (finish, 6), (finish, 7), (finish, 0)],
    ]

    def turn(j):
        for side, waits in enumerate((lower_waits, upper_waits)):
            for step, now in enumerate(waits[:half]):

                @pl.when((upper == side) & (j == step))
                def _():
                    for event, i in now:
                        event(nth(i))

        start = (2 * j + count - 1) // count
        k_one = start * (1 + lax.rem(2 * j + count - 2 + upper * (half - 1), count - 1))
        k_two = 1 + lax.rem(2 * j + upper * (half - 1), count - 1)
        whole(k_one)
        whole(k_two)
        flat = jnp.concatenate(
            [rows[k_one].reshape(block_rows, width), rows[k_two].reshape(block_rows, width)], axis=0
        )
        gate_values = dot(flat, gate[...])
        up_values = dot(flat, up[...])
        act = (jax.nn.silu(gate_values) * up_values).astype(jnp.bfloat16)
        product = dot(act, down[...]).astype(jnp.bfloat16)
        part[k_one] = product[:block_rows].reshape(part.shape[1:])
        part[k_two] = product[block_rows:].reshape(part.shape[1:])
        for k in (k_one, k_two):
            to_partner(k, 1).start()
            to_partner(k, 0).start()

    loop(0, half, turn)
    for side, waits in enumerate((lower_waits, upper_waits)):

        @pl.when(upper == side)
        def _():
            for event, i in waits[half]:
                event(nth(i))


    def g_settle(k):
        s = origin(k)
        for copy in g_pass_on(s, gathered.at[s, column]):
            copy.wait_send()
        g_to_partner(s).wait_send()

    loop(0, me + 1, g_settle)
    loop(1, last, lambda k: g_over_sp(k).wait_send())

    @pl.when(upper == 0)
    def _():
        g_over_sp(half).wait_send()

    @pl.when(upper > 0)
    def _():
        loop(1, half, lambda i: g_hand_on(i).wait_send())

    for c in range(chunks):
        s_partner(c, 0).wait_send()
        s_partner(c, 1).wait_send()
        s_across(c).wait_send()

    def settle(k):
        for copy in pass_on(k, rows.at[k, column]):
            copy.wait_send()
        cross_on(k).wait_send()
        to_partner(k, 0).wait_send()
        to_partner(k, 1).wait_send()
        over_x(k).wait_send()

    loop(0, count, settle)

    def home(k):
        p = peer(k)
        send(
            done.at[k], returned.at[p], send_sem.at[7, k], recv_sem.at[7, k], (p, column)
        ).wait_recv()

    loop(1, count, home)
    flat_returned = returned[...].reshape(slots, width)
    mixed = dot_over(mixing[0], flat_returned, 0, 0) + dot_over(mixing[1], flat_returned, 0, 0)
    out_ref[...] = (hidden[...].astype(jnp.float32) + mixed).astype(jnp.bfloat16)

    def settle_far(k):
        over_sp(k).wait_send()
        back(k).wait_send()

    loop(1, count, settle_far)


def whole_layer(
    query_a,
    query_b,
    latent,
    rope_key,
    latent_gain,
    key_a_weight,
    value_a_weight,
    key_b_weight,
    value_b_weight,
    out_a_weight,
    out_b_weight,
    residual,
    ffn_gain,
    routes,
    route_weight,
    expert_gate,
    expert_up,
    expert_down,
    capacity,
):
    count, columns = lax.axis_size("sp"), lax.axis_size("tp")
    row_count, rank = latent.shape
    rotary = rope_key.shape[1]
    span = query_a.shape[0]
    width = residual.shape[1]
    heads_a = key_a_weight.shape[1] // NOPE_A
    heads_b = key_b_weight.shape[1] // NOPE_B
    table = jnp.asarray(turn_tables(np.arange(count * span), rotary))
    packed = rank + rotary + (-(rank + rotary) % 128)
    key_width = heads_a * 256 + heads_b * (NOPE_B + rotary)
    value_width = value_a_weight.shape[1] + value_b_weight.shape[1]
    chunks = 2
    chunk_width = width // chunks
    block = (count, capacity, width)
    every = (count, columns, capacity, width)
    operands = (
        query_a,
        query_b,
        latent,
        rope_key,
        latent_gain.reshape(1, rank),
        key_a_weight,
        value_a_weight,
        key_b_weight,
        value_b_weight,
        out_a_weight,
        out_b_weight,
        residual,
        ffn_gain.reshape(1, width),
        routes.T,
        route_weight.T,
        table,
        expert_gate,
        expert_up,
        expert_down,
    )
    bf16 = jnp.bfloat16

    def room(shape, dtype=bf16):
        return pltpu.VMEM(shape, dtype)

    loaded = [room(operand.shape, operand.dtype) for operand in operands[:15]]
    loaded += [room((row_count, 2 * rotary), jnp.float32), room((span, 2 * rotary), jnp.float32)]
    loaded += [room(operand.shape[1:], operand.dtype) for operand in operands[16:]]
    dma = pltpu.SemaphoreType.DMA
    return pl.pallas_call(
        functools.partial(layer_kernel, count, columns, heads_a, heads_b),
        out_shape=jax.ShapeDtypeStruct(residual.shape, bf16),
        in_specs=[pl.BlockSpec(memory_space=pl.ANY)] * len(operands),
        out_specs=pl.BlockSpec(memory_space=pltpu.VMEM),
        scratch_shapes=loaded
        + [
            room((row_count, packed)),
            room((count, columns, row_count, packed)),
            room((packed, key_width)),
            room((count, span, key_width)),
            room((count, span, value_width)),
            room((chunks, columns, row_count, chunk_width)),
            room((chunks, row_count, chunk_width)),
            room((chunks, 2, row_count, chunk_width)),
            room((chunks, row_count, chunk_width)),
            room(residual.shape),
            room((count * capacity, row_count)),
            room((2, count * capacity, row_count)),
            room(block),
            room(every),
            room(every),
            room((2,) + block),
            room(block),
            room(block),
            room(block),
            room(block),
            dma((len(operands) + 1,)),
            dma((5, count)),
            dma((4, count)),
            dma((3, chunks)),
            dma((3, chunks)),
            dma((8, count)),
            dma((8, count)),
        ],
        compiler_params=pltpu.CompilerParams(
            collective_id=5, has_side_effects=True, vmem_limit_bytes=60000 * 1024
        ),
    )(*operands)


def body(
    query_a,
    query_b,
    latent,
    rope_key,
    latent_gain,
    key_a_weight,
    value_a_weight,
    key_b_weight,
    value_b_weight,
    out_a_weight,
    out_b_weight,
    residual,
    ffn_gain,
    routes,
    route_weight,
    expert_gate,
    expert_up,
    expert_down,
):
    column_count = lax.axis_size("tp")
    row_count = latent.shape[0]
    experts = lax.axis_size("sp")
    capacity = max(2, 2 * TOP * row_count // experts)
    paired_up = experts & (experts - 1) == 0 and experts > 1 and column_count == 4
    if capacity % 16 == 0 and paired_up:
        return whole_layer(
            query_a,
            query_b,
            latent,
            rope_key,
            latent_gain,
            key_a_weight,
            value_a_weight,
            key_b_weight,
            value_b_weight,
            out_a_weight,
            out_b_weight,
            residual,
            ffn_gain,
            routes,
            route_weight,
            expert_gate,
            expert_up,
            expert_down,
            capacity,
        )
    span_size = query_a.shape[0]
    rotary_width = rope_key.shape[1]
    own_first = (lax.axis_index("sp") * column_count + lax.axis_index("tp")) * row_count
    query_first = lax.axis_index("sp") * span_size
    own_cosine, own_sine = angle_tables(
        own_first + jnp.arange(row_count, dtype=jnp.int32), rotary_width
    )
    normed_latent = rms_scale(latent, latent_gain)
    turned_key = rotate(rope_key, own_cosine, own_sine)
    query_cosine, query_sine = angle_tables(
        query_first + jnp.arange(span_size, dtype=jnp.int32), rotary_width
    )
    heads_a = key_a_weight.shape[1] // NOPE_A
    heads_b = key_b_weight.shape[1] // NOPE_B
    ready_a = prepare_queries(query_a, heads_a, NOPE_A, query_cosine, query_sine)
    ready_b = prepare_queries(query_b, heads_b, NOPE_B, query_cosine, query_sine)

    def start_state(head_count, value_width):
        return (
            jnp.full((head_count, span_size), masked_score, jnp.float32),
            jnp.zeros((head_count, span_size), jnp.float32),
            jnp.zeros((span_size, head_count, value_width), jnp.float32),
        )

    initial = (start_state(heads_a, VAL_A), start_state(heads_b, VAL_B))

    def attend_block(carried, keys_a, values_a, keys_b, values_b, key_turned):
        return (
            fold_group(carried[0], ready_a, keys_a, key_turned, values_a, query_first),
            fold_group(carried[1], ready_b, keys_b, key_turned, values_b, query_first),
        )

    rank = normed_latent.shape[1]
    filler = jnp.zeros((row_count, -(rank + rotary_width) % 128), jnp.bfloat16)
    packed = jnp.concatenate([normed_latent, turned_key, filler], axis=1)
    gathered = gather(packed[None], lax.axis_size("sp"), column_count, True, 0)
    gathered = gathered.reshape(-1, packed.shape[1])
    portion_latent = gathered[:, :rank]
    portion_turned = gathered[:, rank : rank + rotary_width]

    def compute(current):
        return attend_block(
            current,
            expand(portion_latent, key_a_weight, heads_a),
            expand(portion_latent, value_a_weight, heads_a),
            expand(portion_latent, key_b_weight, heads_b),
            expand(portion_latent, value_b_weight, heads_b),
            portion_turned,
        )

    folded = compute(initial)

    def finish(carried):
        top_score, weight_total, weighted = carried
        scaled = weighted / jnp.transpose(weight_total)[:, :, None]
        return scaled.astype(jnp.bfloat16).reshape(span_size, -1)

    out_a = finish(folded[0])
    out_b = finish(folded[1])
    projected = (
        jnp.dot(out_a, out_a_weight, preferred_element_type=jnp.float32)
        + jnp.dot(out_b, out_b_weight, preferred_element_type=jnp.float32)
    ).astype(jnp.bfloat16)
    model_width = residual.shape[1]
    chosen = routes.reshape(-1)
    expert_ids = jnp.arange(experts, dtype=jnp.int32)
    matches = (chosen[:, None] == expert_ids[None, :]).astype(jnp.int32)
    order_rank = jnp.sum((jnp.cumsum(matches, axis=0) - 1) * matches, axis=1)
    slot_index = (chosen * capacity + order_rank).reshape(row_count, TOP)
    slot_ids = jnp.arange(experts * capacity, dtype=jnp.int32)
    selection = jnp.sum(
        (slot_ids[:, None, None] == slot_index[None, :, :]).astype(jnp.bfloat16), axis=2
    )
    hidden_state, outgoing = hidden_sum(
        projected.reshape(column_count, row_count, -1), residual, ffn_gain, selection, 1
    )
    outgoing = outgoing.reshape(experts, capacity, model_width)
    if capacity % 16 == 0:
        places_of = slot_index.T.reshape(-1)
        selector = (places_of[:, None] == slot_ids[None, :]).astype(jnp.bfloat16)
        return through_experts(
            outgoing,
            selector,
            route_weight,
            hidden_state,
            expert_gate,
            expert_up,
            expert_down,
            column_count,
            4,
        )
    portion = gather(outgoing, experts, column_count, False, 2)
    portion_shape = portion.shape
    flat_rows = portion.reshape(-1, model_width)
    gate_values = jnp.dot(flat_rows, expert_gate[0], preferred_element_type=jnp.float32)
    up_values = jnp.dot(flat_rows, expert_up[0], preferred_element_type=jnp.float32)
    hidden = (jax.nn.silu(gate_values) * up_values).astype(jnp.bfloat16)
    partial_value = jnp.dot(hidden, expert_down[0], preferred_element_type=jnp.float32).astype(
        jnp.bfloat16
    )
    returned = give_back(partial_value.reshape(portion_shape), 3)
    flat_returned = returned.reshape(experts * capacity, model_width)
    expert_mix = jnp.zeros((row_count, model_width), jnp.float32)
    for route_index in range(TOP):
        selector = (slot_index[:, route_index][:, None] == slot_ids[None, :]).astype(jnp.bfloat16)
        picked = jnp.dot(selector, flat_returned, preferred_element_type=jnp.float32)
        expert_mix = expert_mix + route_weight[:, route_index][:, None] * picked
    return (hidden_state.astype(jnp.float32) + expert_mix).astype(jnp.bfloat16)


def solution(mesh):
    placed = (
        P("sp", "tp"),
        P("sp", "tp"),
        P(("sp", "tp"), None),
        P(("sp", "tp"), None),
        P(),
        P(None, "tp"),
        P(None, "tp"),
        P(None, "tp"),
        P(None, "tp"),
        P("tp", None),
        P("tp", None),
        P(("sp", "tp"), None),
        P(),
        P(("sp", "tp"), None),
        P(("sp", "tp"), None),
        P("sp", None, "tp"),
        P("sp", None, "tp"),
        P("sp", "tp", None),
    )
    return jax.shard_map(
        body, mesh=mesh, in_specs=placed, out_specs=P(("sp", "tp"), None), check_vma=False
    )
```

```python
import functools

import jax
import jax.numpy as jnp
import numpy as np
from jax import lax
from jax.experimental import pallas as pl
from jax.experimental.pallas import tpu as pltpu
from jax.sharding import PartitionSpec as P

NOPE_A = 128
VAL_A = 128
NOPE_B = 64
VAL_B = 64
TOP = 2


epsilon = 1e-06
base_theta = 500000.0
masked_score = -1e30


def rms_scale(values, scales):
    floats = values.astype(jnp.float32)
    scaled = floats * lax.rsqrt(jnp.mean(floats * floats, axis=-1, keepdims=True) + epsilon)
    return (scaled * scales).astype(jnp.bfloat16)


def angle_tables(positions, rotary_width):
    inverse = jnp.power(
        jnp.float32(base_theta), -jnp.arange(0, rotary_width, 2, dtype=jnp.float32) / rotary_width
    )
    angles = positions.astype(jnp.float32)[:, None] * inverse[None, :]
    return (jnp.cos(angles), jnp.sin(angles))


def rotate(values, cosine, sine_table):
    middle = cosine.shape[-1]
    first_half = values[..., :middle].astype(jnp.float32)
    second_half = values[..., middle:].astype(jnp.float32)
    turned = jnp.concatenate(
        [
            first_half * cosine - second_half * sine_table,
            second_half * cosine + first_half * sine_table,
        ],
        axis=-1,
    )
    return turned.astype(jnp.bfloat16)


def prepare_queries(queries, head_count, nope_width, cosine, sine_table):
    shaped = queries.reshape(queries.shape[0], head_count, queries.shape[1] // head_count)
    turned = rotate(shaped[:, :, nope_width:], cosine[:, None, :], sine_table[:, None, :])
    return jnp.concatenate([shaped[:, :, :nope_width], turned], axis=-1)


def fold_group(carried, queries, key_nope, key_turned, values, query_first):
    top_score, weight_total, weighted = carried
    nope_width = key_nope.shape[2]
    scale = (nope_width + key_turned.shape[1]) ** (-0.5)
    scores = jnp.einsum(
        "thd,shd->hts", queries[:, :, :nope_width], key_nope, preferred_element_type=jnp.float32
    )
    scores = scores + jnp.einsum(
        "thd,sd->hts", queries[:, :, nope_width:], key_turned, preferred_element_type=jnp.float32
    )
    scores = scores * scale
    query_places = query_first + jnp.arange(queries.shape[0], dtype=jnp.int32)
    key_places = jnp.arange(key_nope.shape[0], dtype=jnp.int32)
    allowed = (key_places[None, :] <= query_places[:, None])[None]
    scores = jnp.where(allowed, scores, masked_score)
    new_top = jnp.maximum(top_score, jnp.max(scores, axis=-1))
    weights = jnp.where(allowed, jnp.exp(scores - new_top[:, :, None]), 0.0)
    new_total = jnp.sum(weights, axis=-1)
    product = jnp.einsum(
        "hts,shd->thd", weights.astype(jnp.bfloat16), values, preferred_element_type=jnp.float32
    )
    return (new_top, new_total, product)


def expand(source, weight, head_count):
    product = jnp.dot(source, weight, preferred_element_type=jnp.float32).astype(jnp.bfloat16)
    return product.reshape(source.shape[0], head_count, weight.shape[1] // head_count)


MESH = pl.DeviceIdType.MESH


def places():
    me, column = lax.axis_index("sp"), lax.axis_index("tp")
    half = lax.axis_size("tp") // 2
    across = lax.rem(column + half, 2 * half)
    partner = column + 1 - 2 * lax.rem(column, 2)
    return me, column, across, partner


def send(source, target, send_sem, recv_sem, place):
    return pltpu.make_async_remote_copy(
        src_ref=source,
        dst_ref=target,
        send_sem=send_sem,
        recv_sem=recv_sem,
        device_id={"sp": place[0], "tp": place[1]},
        device_id_type=MESH,
    )


def greet(count, me, column, others):
    barrier = pltpu.get_barrier_semaphore()

    def step(k, carry):
        pl.semaphore_signal(
            barrier,
            inc=1,
            device_id={"sp": lax.rem(me + k, count), "tp": column},
            device_id_type=MESH,
        )
        return carry

    lax.fori_loop(1, count, step, 0)
    for other in others:
        pl.semaphore_signal(
            barrier, inc=1, device_id={"sp": me, "tp": other}, device_id_type=MESH
        )
    pl.semaphore_wait(barrier, max(count, 1) - 1 + len(others))


def loop(low, high, step):
    lax.fori_loop(low, high, lambda k, carry: (step(k), carry)[1], 0)


def gather_kernel(count, causal, in_ref, out_ref, send_sem, recv_sem):
    me, column, across, partner = places()
    diagonal = lax.rem(partner + lax.axis_size("tp") // 2, lax.axis_size("tp"))
    greet(count, me, column, (across, partner))

    def own(p):
        return in_ref.at[0] if causal else in_ref.at[p]

    def over_sp(k):
        p = lax.rem(me + k, count)
        return send(
            own(p), out_ref.at[me, column], send_sem.at[0, k], recv_sem.at[0, me], (p, column)
        )

    def arrival(kind, s, t):
        block = out_ref.at[s, t]
        return send(block, block, send_sem.at[kind, s], recv_sem.at[kind, s], (me, partner))

    def pass_on(s, source):
        target = out_ref.at[s, column]
        return (
            send(source, target, send_sem.at[1, s], recv_sem.at[1, s], (me, across)),
            send(source, target, send_sem.at[2, s], recv_sem.at[2, s], (me, partner)),
        )

    def to_partner(s):
        block = out_ref.at[s, across]
        return send(block, block, send_sem.at[3, s], recv_sem.at[3, s], (me, partner))

    last = count - me if causal else count
    arrivals = me + 1 if causal else count

    loop(1, last, lambda k: over_sp(last - k).start())
    for copy in pass_on(me, own(me)):
        copy.start()
    out_ref[me, column] = in_ref[0] if causal else in_ref[me]
    if causal:

        def clear(s):
            out_ref[s] = jnp.zeros(out_ref.shape[1:], out_ref.dtype)

        loop(me + 1, count, clear)

    def origin(k):
        return lax.rem(me + count - k, count)

    def arrived(k):
        s = origin(k)
        arrival(0, s, column).wait_recv()
        for copy in pass_on(s, out_ref.at[s, column]):
            copy.start()

    loop(1, arrivals, arrived)

    def crossed(k):
        s = origin(k)
        arrival(1, s, across).wait_recv()
        to_partner(s).start()

    loop(0, arrivals, crossed)

    def settle(k):
        s = origin(k)
        arrival(2, s, partner).wait_recv()
        arrival(3, s, diagonal).wait_recv()
        for copy in pass_on(s, out_ref.at[s, column]):
            copy.wait_send()
        to_partner(s).wait_send()

    loop(0, arrivals, settle)
    loop(1, last, lambda k: over_sp(k).wait_send())


def gather(blocks, count, columns, causal, collective_id):
    return pl.pallas_call(
        functools.partial(gather_kernel, count, causal),
        out_shape=jax.ShapeDtypeStruct((count, columns) + blocks.shape[1:], blocks.dtype),
        in_specs=[pl.BlockSpec(memory_space=pltpu.VMEM)],
        out_specs=pl.BlockSpec(memory_space=pltpu.VMEM),
        scratch_shapes=[
            pltpu.SemaphoreType.DMA((4, count)),
            pltpu.SemaphoreType.DMA((4, count)),
        ],
        compiler_params=pltpu.CompilerParams(
            collective_id=collective_id, has_side_effects=True, vmem_limit_bytes=60000 * 1024
        ),
    )(blocks)


def hidden_kernel(
    columns, part_ref, residual_ref, gain_ref, pick_ref, hidden_ref, outgoing_ref, held, send_sem, recv_sem
):
    me, column, _, _ = places()
    others = [lax.rem(column + k, columns) for k in range(1, columns)]
    greet(1, me, column, others)
    copies = []
    for k, other in enumerate(others):
        copies.append(
            send(part_ref.at[other], held.at[k], send_sem.at[k], recv_sem.at[k], (me, other))
        )
    for copy in copies:
        copy.start()
    total = residual_ref[...].astype(jnp.float32) + part_ref[column].astype(jnp.float32)
    for k, copy in enumerate(copies):
        copy.wait_recv()
        total = total + held[k].astype(jnp.float32)
    hidden = total.astype(jnp.bfloat16)
    hidden_ref[...] = hidden
    normed = rms_scale(hidden, gain_ref[...])
    outgoing = jnp.dot(pick_ref[...], normed, preferred_element_type=jnp.float32)
    outgoing_ref[...] = outgoing.astype(jnp.bfloat16)
    for copy in copies:
        copy.wait_send()


def hidden_sum(parts, residual, gain, selection, collective_id):
    columns, rows, width = parts.shape
    return pl.pallas_call(
        functools.partial(hidden_kernel, columns),
        out_shape=[
            jax.ShapeDtypeStruct((rows, width), jnp.bfloat16),
            jax.ShapeDtypeStruct((selection.shape[0], width), jnp.bfloat16),
        ],
        in_specs=[pl.BlockSpec(memory_space=pltpu.VMEM)] * 4,
        out_specs=[pl.BlockSpec(memory_space=pltpu.VMEM)] * 2,
        scratch_shapes=[
            pltpu.VMEM((columns - 1, rows, width), jnp.bfloat16),
            pltpu.SemaphoreType.DMA((columns - 1,)),
            pltpu.SemaphoreType.DMA((columns - 1,)),
        ],
        compiler_params=pltpu.CompilerParams(
            collective_id=collective_id, has_side_effects=True, vmem_limit_bytes=60000 * 1024
        ),
    )(parts, residual, gain.reshape(1, width), selection)


def return_kernel(
    count, in_ref, out_ref, from_partner, pair, mine, from_across, done, send_sem, recv_sem
):
    me, column, across, partner = places()
    diagonal = lax.rem(partner + lax.axis_size("tp") // 2, lax.axis_size("tp"))
    greet(count, me, column, (across, partner))

    def place(k):
        return lax.rem(me + 1 + k, count)

    def to_partner(s, slot):
        wanted = (partner, diagonal)[slot]
        return send(
            in_ref.at[s, wanted],
            from_partner.at[slot, s],
            send_sem.at[slot, s],
            recv_sem.at[slot, s],
            (me, partner),
        )

    def over_x(s):
        return send(
            pair.at[s], from_across.at[s], send_sem.at[2, s], recv_sem.at[2, s], (me, across)
        )

    def back(s):
        return send(
            done.at[s], out_ref.at[me], send_sem.at[3, s], recv_sem.at[3, me], (s, column)
        )

    def start(k):
        s = place(k)
        to_partner(s, 1).start()
        to_partner(s, 0).start()

    loop(0, count, start)

    def both(s, slot):
        kept = in_ref[s, (column, across)[slot]].astype(jnp.float32)
        return kept + from_partner[slot, s].astype(jnp.float32)

    def paired(k):
        s = place(k)
        to_partner(s, 1).wait_recv()
        pair[s] = both(s, 1).astype(jnp.bfloat16)
        over_x(s).start()

    loop(0, count, paired)

    def total(s):
        to_partner(s, 0).wait_recv()
        mine[...] = both(s, 0)
        over_x(s).wait_recv()
        return (mine[...] + from_across[s].astype(jnp.float32)).astype(jnp.bfloat16)

    def summed(k):
        s = place(k)
        done[s] = total(s)
        back(s).start()

    loop(0, count - 1, summed)
    out_ref[me] = total(me)

    def arrived(k):
        s = place(k)
        send(
            done.at[s], out_ref.at[s], send_sem.at[3, s], recv_sem.at[3, s], (s, column)
        ).wait_recv()
        back(s).wait_send()

    loop(0, count - 1, arrived)

    def settle(s):
        to_partner(s, 0).wait_send()
        to_partner(s, 1).wait_send()
        over_x(s).wait_send()

    loop(0, count, settle)


def give_back(partials, collective_id):
    count, _, rows, width = partials.shape
    block = (count, rows, width)
    return pl.pallas_call(
        functools.partial(return_kernel, count),
        out_shape=jax.ShapeDtypeStruct(block, jnp.bfloat16),
        in_specs=[pl.BlockSpec(memory_space=pltpu.VMEM)],
        out_specs=pl.BlockSpec(memory_space=pltpu.VMEM),
        scratch_shapes=[
            pltpu.VMEM((2,) + block, jnp.bfloat16),
            pltpu.VMEM(block, jnp.bfloat16),
            pltpu.VMEM(block[1:], jnp.float32),
            pltpu.VMEM(block, jnp.bfloat16),
            pltpu.VMEM(block, jnp.bfloat16),
            pltpu.SemaphoreType.DMA((4, count)),
            pltpu.SemaphoreType.DMA((4, count)),
        ],
        compiler_params=pltpu.CompilerParams(
            collective_id=collective_id, has_side_effects=True, vmem_limit_bytes=60000 * 1024
        ),
    )(partials)


def experts_kernel(
    count,
    group,
    in_ref,
    selector_ref,
    share_ref,
    hidden_ref,
    gate_hbm,
    up_hbm,
    down_hbm,
    out_ref,
    rows,
    part,
    from_partner,
    pair,
    from_across,
    done,
    returned,
    gate,
    up,
    down,
    weight_sem,
    send_sem,
    recv_sem,
):
    me, column, across, partner = places()
    diagonal = lax.rem(partner + lax.axis_size("tp") // 2, lax.axis_size("tp"))
    loads = [
        pltpu.make_async_copy(source.at[0], target, weight_sem.at[index])
        for index, (source, target) in enumerate(((gate_hbm, gate), (up_hbm, up), (down_hbm, down)))
    ]
    for load in loads:
        load.start()
    greet(count, me, column, (across, partner))

    def origin(k):
        return lax.rem(me + count - k, count)

    def over_sp(k):
        p = lax.rem(me + k, count)
        return send(
            in_ref.at[p], rows.at[me, column], send_sem.at[0, k], recv_sem.at[0, me], (p, column)
        )

    def arrival(kind, s, t):
        block = rows.at[s, t]
        return send(block, block, send_sem.at[kind, s], recv_sem.at[kind, s], (me, partner))

    def pass_on(s, source):
        target = rows.at[s, column]
        return (
            send(source, target, send_sem.at[1, s], recv_sem.at[1, s], (me, across)),
            send(source, target, send_sem.at[2, s], recv_sem.at[2, s], (me, partner)),
        )

    def cross_on(s):
        block = rows.at[s, across]
        return send(block, block, send_sem.at[3, s], recv_sem.at[3, s], (me, partner))

    def to_partner(s, slot):
        wanted = (partner, diagonal)[slot]
        return send(
            part.at[s, wanted],
            from_partner.at[slot, s],
            send_sem.at[4 + slot, s],
            recv_sem.at[4 + slot, s],
            (me, partner),
        )

    def over_x(s):
        return send(
            pair.at[s], from_across.at[s], send_sem.at[6, s], recv_sem.at[6, s], (me, across)
        )

    def back(s):
        return send(
            done.at[s], returned.at[me], send_sem.at[7, s], recv_sem.at[7, me], (s, column)
        )

    loop(1, count, lambda k: over_sp(k).start())
    for copy in pass_on(me, in_ref.at[me]):
        copy.start()
    rows[me, column] = in_ref[me]

    def arrived(k):
        s = origin(k)
        arrival(0, s, column).wait_recv()
        for copy in pass_on(s, rows.at[s, column]):
            copy.start()

    def both(s, slot):
        kept = part[s, (column, across)[slot]].astype(jnp.float32)
        return kept + from_partner[slot, s].astype(jnp.float32)

    def paired(k):
        s = origin(k)
        to_partner(s, 1).wait_recv()
        pair[s] = both(s, 1).astype(jnp.bfloat16)
        over_x(s).start()

    def summed(k):
        s = origin(k)
        to_partner(s, 0).wait_recv()
        over_x(s).wait_recv()
        total = (both(s, 0) + from_across[s].astype(jnp.float32)).astype(jnp.bfloat16)

        @pl.when(k == 0)
        def _():
            returned[me] = total

        @pl.when(k > 0)
        def _():
            done[s] = total
            back(s).start()

    loop(1, group, arrived)
    block_rows = rows.shape[1] * rows.shape[2]
    width = rows.shape[3]

    def turn(j):
        first = j * group

        @pl.when(first + group < count)
        def _():
            loop(first + group, first + 2 * group, arrived)

        def crossed(k):
            s = origin(k)
            arrival(1, s, across).wait_recv()
            cross_on(s).start()

        loop(first, first + group, crossed)

        def whole(k):
            s = origin(k)
            arrival(2, s, partner).wait_recv()
            arrival(3, s, diagonal).wait_recv()

        loop(first, first + group, whole)

        @pl.when(j == 0)
        def _():
            for load in loads:
                load.wait()

        sources = [origin(first + i) for i in range(group)]
        flat = jnp.concatenate([rows[s].reshape(block_rows, width) for s in sources], axis=0)
        gate_values = jnp.dot(flat, gate[...], preferred_element_type=jnp.float32)
        up_values = jnp.dot(flat, up[...], preferred_element_type=jnp.float32)
        hidden = (jax.nn.silu(gate_values) * up_values).astype(jnp.bfloat16)
        product = jnp.dot(hidden, down[...], preferred_element_type=jnp.float32)
        product = product.astype(jnp.bfloat16)
        for i, s in enumerate(sources):
            part[s] = product[i * block_rows : (i + 1) * block_rows].reshape(rows.shape[1:])

        def leave(k):
            s = origin(k)
            to_partner(s, 1).start()
            to_partner(s, 0).start()

        loop(first, first + group, leave)

        @pl.when(j > 0)
        def _():
            loop(first - group, first, paired)

        @pl.when(j > 1)
        def _():
            loop(first - 2 * group, first - group, summed)

    turns = count // group
    loop(0, turns, turn)
    loop(count - group, count, paired)
    loop(max(turns - 2, 0) * group, count, summed)

    def home(k):
        s = origin(k)
        send(
            done.at[s], returned.at[s], send_sem.at[7, s], recv_sem.at[7, s], (s, column)
        ).wait_recv()
        back(s).wait_send()

    loop(1, count, home)
    picked = jnp.dot(
        selector_ref[...], returned[...].reshape(-1, width), preferred_element_type=jnp.float32
    )
    own_rows = hidden_ref.shape[0]
    mixed = jnp.zeros(hidden_ref.shape, jnp.float32)
    for route_index in range(TOP):
        mixed = mixed + (
            share_ref[:, route_index : route_index + 1]
            * picked[route_index * own_rows : (route_index + 1) * own_rows]
        )
    out_ref[...] = (hidden_ref[...].astype(jnp.float32) + mixed).astype(jnp.bfloat16)

    def settle(s):
        for copy in pass_on(s, rows.at[s, column]):
            copy.wait_send()
        cross_on(s).wait_send()
        to_partner(s, 0).wait_send()
        to_partner(s, 1).wait_send()
        over_x(s).wait_send()

    loop(0, count, settle)
    loop(1, count, lambda k: over_sp(k).wait_send())


def through_experts(outgoing, selector, share, hidden, gate, up, down, columns, collective_id):
    count, rows, width = outgoing.shape
    group = 2 if count % 2 == 0 else 1
    block = (count, rows, width)
    every = (count, columns, rows, width)
    return pl.pallas_call(
        functools.partial(experts_kernel, count, group),
        out_shape=jax.ShapeDtypeStruct(hidden.shape, jnp.bfloat16),
        in_specs=[pl.BlockSpec(memory_space=pltpu.VMEM)] * 4
        + [pl.BlockSpec(memory_space=pl.ANY)] * 3,
        out_specs=pl.BlockSpec(memory_space=pltpu.VMEM),
        scratch_shapes=[
            pltpu.VMEM(every, jnp.bfloat16),
            pltpu.VMEM(every, jnp.bfloat16),
            pltpu.VMEM((2,) + block, jnp.bfloat16),
            pltpu.VMEM(block, jnp.bfloat16),
            pltpu.VMEM(block, jnp.bfloat16),
            pltpu.VMEM(block, jnp.bfloat16),
            pltpu.VMEM(block, jnp.bfloat16),
            pltpu.VMEM(gate.shape[1:], jnp.bfloat16),
            pltpu.VMEM(up.shape[1:], jnp.bfloat16),
            pltpu.VMEM(down.shape[1:], jnp.bfloat16),
            pltpu.SemaphoreType.DMA((3,)),
            pltpu.SemaphoreType.DMA((8, count)),
            pltpu.SemaphoreType.DMA((8, count)),
        ],
        compiler_params=pltpu.CompilerParams(
            collective_id=collective_id, has_side_effects=True, vmem_limit_bytes=60000 * 1024
        ),
    )(outgoing, selector, share, hidden, gate, up, down)


def turn_tables(positions, rotary_width):
    inverse = np.power(
        np.float32(base_theta), -np.arange(0, rotary_width, 2, dtype=np.float32) / rotary_width
    ).astype(np.float32)
    angles = positions.astype(np.float32)[:, None] * inverse[None, :]
    cosine, sine = np.cos(angles), np.sin(angles)
    return np.concatenate([cosine, cosine, -sine, sine], axis=1).astype(np.float32)


def iotas(shape):
    return (
        lax.broadcasted_iota(jnp.int32, shape, 0),
        lax.broadcasted_iota(jnp.int32, shape, 1),
    )


def dot(left, right):
    return jnp.dot(left, right, preferred_element_type=jnp.float32)


def dot_over(left, right, left_dim, right_dim):
    return lax.dot_general(
        left, right, (((left_dim,), (right_dim,)), ((), ())), preferred_element_type=jnp.float32
    )


def layer_kernel(
    count,
    columns,
    heads_a,
    heads_b,
    query_a_hbm,
    query_b_hbm,
    latent_hbm,
    rope_hbm,
    latent_gain_hbm,
    key_a_hbm,
    value_a_hbm,
    key_b_hbm,
    value_b_hbm,
    out_a_hbm,
    out_b_hbm,
    residual_hbm,
    ffn_gain_hbm,
    routes_hbm,
    share_hbm,
    table_hbm,
    gate_hbm,
    up_hbm,
    down_hbm,
    out_ref,
    query_a,
    query_b,
    latent,
    rope,
    latent_gain,
    key_a,
    value_a,
    key_b,
    value_b,
    out_a,
    out_b,
    residual,
    ffn_gain,
    routes,
    share,
    own_table,
    query_table,
    gate,
    up,
    down,
    own,
    gathered,
    key_weight,
    keys,
    values,
    head_part,
    head_pair,
    head_from_partner,
    head_from_across,
    hidden,
    selection,
    mixing,
    outgoing,
    rows,
    part,
    from_partner,
    pair,
    from_across,
    done,
    returned,
    load_sem,
    gather_send,
    gather_recv,
    sum_send,
    sum_recv,
    send_sem,
    recv_sem,
):
    me, column, across, partner = places()
    diagonal = lax.rem(partner + columns // 2, columns)
    row_count = latent.shape[0]
    span = query_a.shape[0]
    rank = latent.shape[1]
    rotary = rope.shape[1]
    width = residual.shape[1]
    total = count * span

    own_first = pl.multiple_of((me * columns + column) * row_count, row_count)
    query_first = pl.multiple_of(me * span, span)
    plan = [
        (latent_hbm, latent),
        (rope_hbm, rope),
        (latent_gain_hbm, latent_gain),
        (table_hbm.at[pl.ds(own_first, row_count)], own_table),
        (key_a_hbm, key_a),
        (key_b_hbm, key_b),
        (query_a_hbm, query_a),
        (query_b_hbm, query_b),
        (table_hbm.at[pl.ds(query_first, span)], query_table),
        (value_a_hbm, value_a),
        (value_b_hbm, value_b),
        (routes_hbm, routes),
        (share_hbm, share),
        (out_a_hbm, out_a),
        (out_b_hbm, out_b),
        (residual_hbm, residual),
        (ffn_gain_hbm, ffn_gain),
        (gate_hbm.at[0], gate),
        (up_hbm.at[0], up),
        (down_hbm.at[0], down),
    ]
    loads = [
        pltpu.make_async_copy(source, target, load_sem.at[index])
        for index, (source, target) in enumerate(plan)
    ]
    for load in loads[:17]:
        load.start()

    barrier = pltpu.get_barrier_semaphore()

    def hello(k, carry):
        pl.semaphore_signal(
            barrier,
            inc=1,
            device_id={"sp": lax.rem(me + k, count), "tp": column},
            device_id_type=MESH,
        )
        return carry

    lax.fori_loop(1, count, hello, 0)
    for other in (across, partner):
        pl.semaphore_signal(
            barrier, inc=1, device_id={"sp": me, "tp": other}, device_id_type=MESH
        )

    for load in loads[:4]:
        load.wait()
    row, col = iotas((128, 128))
    swap = (row == jnp.where(jnp.bitwise_and(col, rotary - 1) < rotary // 2, col + rotary // 2, col - rotary // 2))
    swap = swap.astype(jnp.bfloat16)
    own[:, :rank] = rms_scale(latent[...], latent_gain[...])
    key = rope[...]
    turned = key.astype(jnp.float32) * own_table[:, :rotary] + (
        dot(key, swap[:rotary, :rotary]) * own_table[:, rotary:]
    )
    own[:, rank : rank + rotary] = turned.astype(jnp.bfloat16)
    own[:, rank + rotary :] = jnp.zeros(
        (row_count, own.shape[1] - rank - rotary), jnp.bfloat16
    )
    for load in loads[4:13]:
        load.wait()
    nope_a = key_a.shape[1] // heads_a
    nope_b = key_b.shape[1] // heads_b
    wide_a = 256
    wide_b = nope_b + rotary
    starts_a = []
    for h in range(heads_a):
        start = h * (nope_a + rotary)
        starts_a.append(start // 128 * 128)
        pad = start - starts_a[h]
        r, c = iotas((key_a.shape[1], wide_a))
        inside = (c >= pad) & (c < pad + nope_a)
        piece = ((r - c == h * nope_a - pad) & inside).astype(jnp.bfloat16)
        lanes = slice(h * wide_a, (h + 1) * wide_a)
        key_weight[:rank, lanes] = dot(key_a[...], piece).astype(jnp.bfloat16)
        r, c = iotas((own.shape[1] - rank, wide_a))
        key_weight[rank:, lanes] = ((c - r == pad + nope_a) & (r < rotary)).astype(jnp.bfloat16)
    base_b = heads_a * wide_a
    for h in range(heads_b):
        r, c = iotas((key_b.shape[1], wide_b))
        piece = ((r - c == h * nope_b) & (c < nope_b)).astype(jnp.bfloat16)
        lanes = slice(base_b + h * wide_b, base_b + (h + 1) * wide_b)
        key_weight[:rank, lanes] = dot(key_b[...], piece).astype(jnp.bfloat16)
        r, c = iotas((own.shape[1] - rank, wide_b))
        key_weight[rank:, lanes] = ((c - r == nope_b) & (r < rotary)).astype(jnp.bfloat16)

    lane = lax.broadcasted_iota(jnp.int32, (span, 128), 1)
    table = query_table[...]
    rolled = jnp.concatenate([table[:, rotary:], table[:, :rotary]], axis=1)
    low = lane < rotary
    one = jnp.ones((span, 128), jnp.float32)
    zero = jnp.zeros((span, 128), jnp.float32)
    turn_low = (jnp.where(low, table, one), jnp.where(low, rolled, zero))
    turn_high = (jnp.where(low, one, rolled), jnp.where(low, zero, table))

    def turn_tile(ref, start, factors):
        tile = ref[:, start : start + 128]
        turned_tile = tile.astype(jnp.float32) * factors[0] + dot(tile, swap) * factors[1]
        ref[:, start : start + 128] = turned_tile.astype(jnp.bfloat16)

    for h in range(heads_a):
        start = h * (nope_a + rotary) + nope_a
        turn_tile(query_a, start // 128 * 128, turn_low if start % 128 == 0 else turn_high)
    for h in range(heads_b):
        turn_tile(query_b, h * wide_b, turn_high)

    capacity = outgoing.shape[1]
    slots = count * capacity
    expert_at = lax.broadcasted_iota(jnp.int32, (count, row_count), 0)
    before = iotas((row_count, row_count))
    before = (before[0] < before[1]).astype(jnp.bfloat16)
    slot_at = lax.broadcasted_iota(jnp.int32, (slots, row_count), 0)
    earlier = jnp.zeros((count, 1), jnp.float32)
    picks = []
    for k in range(TOP):
        expert = routes[k : k + 1, :]
        named = (expert_at == expert).astype(jnp.float32)
        place = dot(named.astype(jnp.bfloat16), before) + earlier
        place = jnp.sum(place * named, axis=0, keepdims=True).astype(jnp.int32)
        picks.append((slot_at == expert * capacity + place).astype(jnp.float32))
        earlier = earlier + jnp.sum(named, axis=1, keepdims=True)
    selection[...] = functools.reduce(lambda a, b: a + b, picks).astype(jnp.bfloat16)
    mix = functools.reduce(
        lambda a, b: a + b, [pick * share[k : k + 1, :] for k, pick in enumerate(picks)]
    )
    mix_high = mix.astype(jnp.bfloat16)
    mixing[0] = mix_high
    mixing[1] = (mix - mix_high.astype(jnp.float32)).astype(jnp.bfloat16)

    pl.semaphore_wait(barrier, count + 1)

    half = count // 2
    upper = me // half
    at = lax.rem(me, half)

    def g_over_sp(k):
        p = lax.rem(me + k, count)
        return send(
            own, gathered.at[me, column], gather_send.at[0, k], gather_recv.at[0, me], (p, column)
        )

    def g_hand_on(k):
        p = upper * half + lax.rem(at + k, half)
        block = gathered.at[at, column]
        return send(block, block, gather_send.at[4, k], gather_recv.at[0, at], (p, column))

    def g_arrival(kind, s, t):
        block = gathered.at[s, t]
        return send(
            block, block, gather_send.at[kind, s], gather_recv.at[kind, s], (me, partner)
        )

    def g_pass_on(s, source):
        target = gathered.at[s, column]
        return (
            send(source, target, gather_send.at[1, s], gather_recv.at[1, s], (me, across)),
            send(source, target, gather_send.at[2, s], gather_recv.at[2, s], (me, partner)),
        )

    def g_to_partner(s):
        block = gathered.at[s, across]
        return send(
            block, block, gather_send.at[3, s], gather_recv.at[3, s], (me, partner)
        )

    last = half - at

    @pl.when(upper == 0)
    def _():
        g_over_sp(half).start()

    for copy in g_pass_on(me, own):
        copy.start()
    loop(1, last, lambda k: g_over_sp(last - k).start())
    gathered[me, column] = own[...]

    def clear(s):
        values[s] = jnp.zeros(values.shape[1:], values.dtype)
        keys[s] = jnp.zeros(keys.shape[1:], keys.dtype)

    loop(me + 1, count, clear)

    def origin(k):
        later = (k + count - at - 1) // count
        return (1 - later) * (me - k) + later * lax.rem(k - 1 + half, half)

    def g_arrived(k):
        s = origin(k)
        g_arrival(0, s, column).wait_recv()

        @pl.when(k == at + 1)
        def _():
            loop(1, half, lambda i: g_hand_on(i).start())

        for copy in g_pass_on(s, gathered.at[s, column]):
            copy.start()


    def g_step(k):
        @pl.when(k <= me)
        def _():
            s = origin(k)
            g_arrival(1, s, across).wait_recv()
            g_to_partner(s).start()

        @pl.when(k >= 1)
        def _():
            s = origin(k - 1)
            g_arrival(2, s, partner).wait_recv()
            g_arrival(3, s, diagonal).wait_recv()
            packed = gathered[s].reshape(span, own.shape[1])
            keys[s] = dot(packed, key_weight[...]).astype(jnp.bfloat16)
            values[s, :, : value_a.shape[1]] = dot(packed[:, :rank], value_a[...]).astype(
                jnp.bfloat16
            )
            values[s, :, value_a.shape[1] :] = dot(packed[:, :rank], value_b[...]).astype(
                jnp.bfloat16
            )

    first = at + 1 + upper
    loop(1, first, g_arrived)
    loop(0, first, g_step)
    loop(first, me + 1, g_arrived)
    for load in loads[17:]:
        load.start()
    loop(first, me + 2, g_step)

    query_at, key_at = iotas((span, total))
    allowed = key_at <= query_at + query_first

    def weigh(queries, lanes, size):
        scores = dot_over(queries, keys[:, :, lanes].reshape(total, -1), 1, 1)
        scores = jnp.where(allowed, scores, masked_score)
        top = jnp.max(scores, axis=1, keepdims=True)
        weights = jnp.exp((scores - top) * size ** (-0.5))
        return weights.astype(jnp.bfloat16), jnp.sum(weights, axis=1, keepdims=True)

    def attend(parts, lanes, each):
        group = values[:, :, lanes].reshape(total, -1)
        results = [dot(weights, group) / sums for weights, sums in parts]
        result = results[0]
        place = lax.broadcasted_iota(jnp.int32, result.shape, 1)
        for h in range(1, len(parts)):
            result = jnp.where(place < h * each, result, results[h])
        return result.astype(jnp.bfloat16)

    for load in loads[13:17]:
        load.wait()
    mixed_a = attend(
        [
            weigh(
                query_a[:, starts_a[h] : starts_a[h] + wide_a],
                slice(h * wide_a, (h + 1) * wide_a),
                nope_a + rotary,
            )
            for h in range(heads_a)
        ],
        slice(0, value_a.shape[1]),
        value_a.shape[1] // heads_a,
    )
    mixed_b = attend(
        [
            weigh(
                query_b[:, h * wide_b : (h + 1) * wide_b],
                slice(base_b + h * wide_b, base_b + (h + 1) * wide_b),
                wide_b,
            )
            for h in range(heads_b)
        ],
        slice(value_a.shape[1], value_a.shape[1] + value_b.shape[1]),
        value_b.shape[1] // heads_b,
    )

    chunks = head_part.shape[0]
    chunk_width = head_part.shape[3]

    def s_partner(c, slot):
        return send(
            head_part.at[c, (partner, diagonal)[slot]],
            head_from_partner.at[c, slot],
            sum_send.at[slot, c],
            sum_recv.at[slot, c],
            (me, partner),
        )

    def s_across(c):
        return send(
            head_pair.at[c], head_from_across.at[c], sum_send.at[2, c], sum_recv.at[2, c], (me, across)
        )

    for c in range(chunks):
        lanes = slice(c * chunk_width, (c + 1) * chunk_width)
        product = dot(mixed_a, out_a[:, lanes]) + dot(mixed_b, out_b[:, lanes])
        head_part[c] = product.astype(jnp.bfloat16).reshape(head_part.shape[1:])
        s_partner(c, 1).start()
        s_partner(c, 0).start()
    for c in range(chunks):
        s_partner(c, 1).wait_recv()
        both = head_part[c, across].astype(jnp.float32) + head_from_partner[c, 1].astype(jnp.float32)
        head_pair[c] = both.astype(jnp.bfloat16)
        s_across(c).start()

    for c in range(chunks):
        lanes = slice(c * chunk_width, (c + 1) * chunk_width)
        s_partner(c, 0).wait_recv()
        summed_rows = (
            residual[:, lanes].astype(jnp.float32)
            + head_part[c, column].astype(jnp.float32)
            + head_from_partner[c, 0].astype(jnp.float32)
        )
        s_across(c).wait_recv()
        summed_rows = summed_rows + head_from_across[c].astype(jnp.float32)
        hidden[:, lanes] = summed_rows.astype(jnp.bfloat16)
    normed = rms_scale(hidden[...], ffn_gain[...])
    outgoing[...] = dot(selection[...], normed).astype(jnp.bfloat16).reshape(outgoing.shape)

    def peer(k):
        result = 0
        bit = 1
        while bit < count:
            mine = lax.rem(me // bit, 2)
            other = lax.rem(k // bit, 2)
            result = result + bit * lax.rem(mine + other, 2)
            bit *= 2
        return result

    def over_sp(k):
        p = peer(k)
        return send(
            outgoing.at[p], rows.at[k, column], send_sem.at[0, k], recv_sem.at[0, k], (p, column)
        )

    def pass_on(k, source):
        target = rows.at[k, column]
        return (
            send(source, target, send_sem.at[1, k], recv_sem.at[1, k], (me, across)),
            send(source, target, send_sem.at[2, k], recv_sem.at[2, k], (me, partner)),
        )

    def arrival(kind, k, t):
        block = rows.at[k, t]
        return send(block, block, send_sem.at[kind, k], recv_sem.at[kind, k], (me, partner))

    def cross_on(k):
        block = rows.at[k, across]
        return send(block, block, send_sem.at[3, k], recv_sem.at[3, k], (me, partner))

    def to_partner(k, slot):
        wanted = (partner, diagonal)[slot]
        return send(
            part.at[k, wanted],
            from_partner.at[slot, k],
            send_sem.at[4 + slot, k],
            recv_sem.at[4 + slot, k],
            (me, partner),
        )

    def over_x(k):
        return send(
            pair.at[k], from_across.at[k], send_sem.at[6, k], recv_sem.at[6, k], (me, across)
        )

    def back(k):
        p = peer(k)
        return send(
            done.at[k], returned.at[me], send_sem.at[7, k], recv_sem.at[7, k], (p, column)
        )

    for copy in pass_on(0, outgoing.at[me]):
        copy.start()
    for k in (1, 4, 2, 5, 3, 6, 7):
        over_sp(k).start()
    rows[0, column] = outgoing[me]

    def arrived(k):
        arrival(0, k, column).wait_recv()
        for copy in pass_on(k, rows.at[k, column]):
            copy.start()

    def crossed(k):
        arrival(1, k, across).wait_recv()
        cross_on(k).start()

    def whole(k):
        arrival(2, k, partner).wait_recv()
        arrival(3, k, diagonal).wait_recv()

    def both_of(k, slot):
        kept = part[k, (column, across)[slot]].astype(jnp.float32)
        return kept + from_partner[slot, k].astype(jnp.float32)

    def paired(k):
        to_partner(k, 1).wait_recv()
        pair[k] = both_of(k, 1).astype(jnp.bfloat16)
        over_x(k).start()

    def summed(k):
        to_partner(k, 0).wait_recv()
        over_x(k).wait_recv()
        result = (both_of(k, 0) + from_across[k].astype(jnp.float32)).astype(jnp.bfloat16)

        @pl.when(k == 0)
        def _():
            returned[me] = result

        @pl.when(k > 0)
        def _():
            done[k] = result
            back(k).start()

    block_rows = rows.shape[1] * rows.shape[2]
    for load in loads[17:]:
        load.wait()

    def nth(i):
        return 0 if i == 0 else 1 + lax.rem(i - 1 + upper * (half - 1), count - 1)

    arrive, cross, couple, finish = arrived, crossed, paired, summed
    lower_waits = [
        [(arrive, 1), (cross, 0), (arrive, 2), (cross, 1), (arrive, 3)],
        [(cross, 2), (cross, 3), (couple, 1), (couple, 0)],
        [(arrive, 4), (arrive, 5), (couple, 2), (couple, 3), (finish, 1), (finish, 0), (arrive, 6), (cross, 4), (cross, 5), (arrive, 7)],
        [(couple, 4), (couple, 5), (finish, 2), (finish, 3), (cross, 6), (cross, 7)],
        [(couple, 6), (couple, 7), (finish, 4), (finish, 5), (finish, 6), (finish, 7)],
    ]
    upper_waits = [
        [(arrive, 1), (arrive, 2), (arrive, 3), (arrive, 4), (cross, 0), (cross, 1)],
        [(arrive, 5), (arrive, 6), (cross, 2), (cross, 3), (couple, 1)],
        [(arrive, 7), (couple, 2), (couple, 3), (finish, 1), (cross, 4), (cross, 5)],
        [(couple, 4), (couple, 5), (finish, 2), (finish, 3), (cross, 6), (cross, 7)],
        [(couple, 6), (couple, 7), (finish, 4), (finish, 5), (couple, 0), (finish, 6), (finish, 7), (finish, 0)],
    ]

    def turn(j):
        for side, waits in enumerate((lower_waits, upper_waits)):
            for step, now in enumerate(waits[:half]):

                @pl.when((upper == side) & (j == step))
                def _():
                    for event, i in now:
                        event(nth(i))

        start = (2 * j + count - 1) // count
        k_one = start * (1 + lax.rem(2 * j + count - 2 + upper * (half - 1), count - 1))
        k_two = 1 + lax.rem(2 * j + upper * (half - 1), count - 1)
        whole(k_one)
        whole(k_two)
        flat = jnp.concatenate(
            [rows[k_one].reshape(block_rows, width), rows[k_two].reshape(block_rows, width)], axis=0
        )
        gate_values = dot(flat, gate[...])
        up_values = dot(flat, up[...])
        act = (jax.nn.silu(gate_values) * up_values).astype(jnp.bfloat16)
        product = dot(act, down[...]).astype(jnp.bfloat16)
        part[k_one] = product[:block_rows].reshape(part.shape[1:])
        part[k_two] = product[block_rows:].reshape(part.shape[1:])
        for slot in (1, 0):
            for k in (k_one, k_two):
                to_partner(k, slot).start()

    loop(0, half, turn)
    for side, waits in enumerate((lower_waits, upper_waits)):

        @pl.when(upper == side)
        def _():
            for event, i in waits[half]:
                event(nth(i))


    def g_settle(k):
        s = origin(k)
        for copy in g_pass_on(s, gathered.at[s, column]):
            copy.wait_send()
        g_to_partner(s).wait_send()

    loop(0, me + 1, g_settle)
    loop(1, last, lambda k: g_over_sp(k).wait_send())

    @pl.when(upper == 0)
    def _():
        g_over_sp(half).wait_send()

    @pl.when(upper > 0)
    def _():
        loop(1, half, lambda i: g_hand_on(i).wait_send())

    for c in range(chunks):
        s_partner(c, 0).wait_send()
        s_partner(c, 1).wait_send()
        s_across(c).wait_send()

    def settle(k):
        for copy in pass_on(k, rows.at[k, column]):
            copy.wait_send()
        cross_on(k).wait_send()
        to_partner(k, 0).wait_send()
        to_partner(k, 1).wait_send()
        over_x(k).wait_send()

    loop(0, count, settle)

    def home(k):
        p = peer(k)
        send(
            done.at[k], returned.at[p], send_sem.at[7, k], recv_sem.at[7, k], (p, column)
        ).wait_recv()

    loop(1, count, home)
    flat_returned = returned[...].reshape(slots, width)
    mixed = dot_over(mixing[0], flat_returned, 0, 0) + dot_over(mixing[1], flat_returned, 0, 0)
    out_ref[...] = (hidden[...].astype(jnp.float32) + mixed).astype(jnp.bfloat16)

    def settle_far(k):
        over_sp(k).wait_send()
        back(k).wait_send()

    loop(1, count, settle_far)


def whole_layer(
    query_a,
    query_b,
    latent,
    rope_key,
    latent_gain,
    key_a_weight,
    value_a_weight,
    key_b_weight,
    value_b_weight,
    out_a_weight,
    out_b_weight,
    residual,
    ffn_gain,
    routes,
    route_weight,
    expert_gate,
    expert_up,
    expert_down,
    capacity,
):
    count, columns = lax.axis_size("sp"), lax.axis_size("tp")
    row_count, rank = latent.shape
    rotary = rope_key.shape[1]
    span = query_a.shape[0]
    width = residual.shape[1]
    heads_a = key_a_weight.shape[1] // NOPE_A
    heads_b = key_b_weight.shape[1] // NOPE_B
    table = jnp.asarray(turn_tables(np.arange(count * span), rotary))
    packed = rank + rotary + (-(rank + rotary) % 128)
    key_width = heads_a * 256 + heads_b * (NOPE_B + rotary)
    value_width = value_a_weight.shape[1] + value_b_weight.shape[1]
    chunks = 2
    chunk_width = width // chunks
    block = (count, capacity, width)
    every = (count, columns, capacity, width)
    operands = (
        query_a,
        query_b,
        latent,
        rope_key,
        latent_gain.reshape(1, rank),
        key_a_weight,
        value_a_weight,
        key_b_weight,
        value_b_weight,
        out_a_weight,
        out_b_weight,
        residual,
        ffn_gain.reshape(1, width),
        routes.T,
        route_weight.T,
        table,
        expert_gate,
        expert_up,
        expert_down,
    )
    bf16 = jnp.bfloat16

    def room(shape, dtype=bf16):
        return pltpu.VMEM(shape, dtype)

    loaded = [room(operand.shape, operand.dtype) for operand in operands[:15]]
    loaded += [room((row_count, 2 * rotary), jnp.float32), room((span, 2 * rotary), jnp.float32)]
    loaded += [room(operand.shape[1:], operand.dtype) for operand in operands[16:]]
    dma = pltpu.SemaphoreType.DMA
    return pl.pallas_call(
        functools.partial(layer_kernel, count, columns, heads_a, heads_b),
        out_shape=jax.ShapeDtypeStruct(residual.shape, bf16),
        in_specs=[pl.BlockSpec(memory_space=pl.ANY)] * len(operands),
        out_specs=pl.BlockSpec(memory_space=pltpu.VMEM),
        scratch_shapes=loaded
        + [
            room((row_count, packed)),
            room((count, columns, row_count, packed)),
            room((packed, key_width)),
            room((count, span, key_width)),
            room((count, span, value_width)),
            room((chunks, columns, row_count, chunk_width)),
            room((chunks, row_count, chunk_width)),
            room((chunks, 2, row_count, chunk_width)),
            room((chunks, row_count, chunk_width)),
            room(residual.shape),
            room((count * capacity, row_count)),
            room((2, count * capacity, row_count)),
            room(block),
            room(every),
            room(every),
            room((2,) + block),
            room(block),
            room(block),
            room(block),
            room(block),
            dma((len(operands) + 1,)),
            dma((5, count)),
            dma((4, count)),
            dma((3, chunks)),
            dma((3, chunks)),
            dma((8, count)),
            dma((8, count)),
        ],
        compiler_params=pltpu.CompilerParams(
            collective_id=5, has_side_effects=True, vmem_limit_bytes=60000 * 1024
        ),
    )(*operands)


def body(
    query_a,
    query_b,
    latent,
    rope_key,
    latent_gain,
    key_a_weight,
    value_a_weight,
    key_b_weight,
    value_b_weight,
    out_a_weight,
    out_b_weight,
    residual,
    ffn_gain,
    routes,
    route_weight,
    expert_gate,
    expert_up,
    expert_down,
):
    column_count = lax.axis_size("tp")
    row_count = latent.shape[0]
    experts = lax.axis_size("sp")
    capacity = max(2, 2 * TOP * row_count // experts)
    paired_up = experts & (experts - 1) == 0 and experts > 1 and column_count == 4
    if capacity % 16 == 0 and paired_up:
        return whole_layer(
            query_a,
            query_b,
            latent,
            rope_key,
            latent_gain,
            key_a_weight,
            value_a_weight,
            key_b_weight,
            value_b_weight,
            out_a_weight,
            out_b_weight,
            residual,
            ffn_gain,
            routes,
            route_weight,
            expert_gate,
            expert_up,
            expert_down,
            capacity,
        )
    span_size = query_a.shape[0]
    rotary_width = rope_key.shape[1]
    own_first = (lax.axis_index("sp") * column_count + lax.axis_index("tp")) * row_count
    query_first = lax.axis_index("sp") * span_size
    own_cosine, own_sine = angle_tables(
        own_first + jnp.arange(row_count, dtype=jnp.int32), rotary_width
    )
    normed_latent = rms_scale(latent, latent_gain)
    turned_key = rotate(rope_key, own_cosine, own_sine)
    query_cosine, query_sine = angle_tables(
        query_first + jnp.arange(span_size, dtype=jnp.int32), rotary_width
    )
    heads_a = key_a_weight.shape[1] // NOPE_A
    heads_b = key_b_weight.shape[1] // NOPE_B
    ready_a = prepare_queries(query_a, heads_a, NOPE_A, query_cosine, query_sine)
    ready_b = prepare_queries(query_b, heads_b, NOPE_B, query_cosine, query_sine)

    def start_state(head_count, value_width):
        return (
            jnp.full((head_count, span_size), masked_score, jnp.float32),
            jnp.zeros((head_count, span_size), jnp.float32),
            jnp.zeros((span_size, head_count, value_width), jnp.float32),
        )

    initial = (start_state(heads_a, VAL_A), start_state(heads_b, VAL_B))

    def attend_block(carried, keys_a, values_a, keys_b, values_b, key_turned):
        return (
            fold_group(carried[0], ready_a, keys_a, key_turned, values_a, query_first),
            fold_group(carried[1], ready_b, keys_b, key_turned, values_b, query_first),
        )

    rank = normed_latent.shape[1]
    filler = jnp.zeros((row_count, -(rank + rotary_width) % 128), jnp.bfloat16)
    packed = jnp.concatenate([normed_latent, turned_key, filler], axis=1)
    gathered = gather(packed[None], lax.axis_size("sp"), column_count, True, 0)
    gathered = gathered.reshape(-1, packed.shape[1])
    portion_latent = gathered[:, :rank]
    portion_turned = gathered[:, rank : rank + rotary_width]

    def compute(current):
        return attend_block(
            current,
            expand(portion_latent, key_a_weight, heads_a),
            expand(portion_latent, value_a_weight, heads_a),
            expand(portion_latent, key_b_weight, heads_b),
            expand(portion_latent, value_b_weight, heads_b),
            portion_turned,
        )

    folded = compute(initial)

    def finish(carried):
        top_score, weight_total, weighted = carried
        scaled = weighted / jnp.transpose(weight_total)[:, :, None]
        return scaled.astype(jnp.bfloat16).reshape(span_size, -1)

    out_a = finish(folded[0])
    out_b = finish(folded[1])
    projected = (
        jnp.dot(out_a, out_a_weight, preferred_element_type=jnp.float32)
        + jnp.dot(out_b, out_b_weight, preferred_element_type=jnp.float32)
    ).astype(jnp.bfloat16)
    model_width = residual.shape[1]
    chosen = routes.reshape(-1)
    expert_ids = jnp.arange(experts, dtype=jnp.int32)
    matches = (chosen[:, None] == expert_ids[None, :]).astype(jnp.int32)
    order_rank = jnp.sum((jnp.cumsum(matches, axis=0) - 1) * matches, axis=1)
    slot_index = (chosen * capacity + order_rank).reshape(row_count, TOP)
    slot_ids = jnp.arange(experts * capacity, dtype=jnp.int32)
    selection = jnp.sum(
        (slot_ids[:, None, None] == slot_index[None, :, :]).astype(jnp.bfloat16), axis=2
    )
    hidden_state, outgoing = hidden_sum(
        projected.reshape(column_count, row_count, -1), residual, ffn_gain, selection, 1
    )
    outgoing = outgoing.reshape(experts, capacity, model_width)
    if capacity % 16 == 0:
        places_of = slot_index.T.reshape(-1)
        selector = (places_of[:, None] == slot_ids[None, :]).astype(jnp.bfloat16)
        return through_experts(
            outgoing,
            selector,
            route_weight,
            hidden_state,
            expert_gate,
            expert_up,
            expert_down,
            column_count,
            4,
        )
    portion = gather(outgoing, experts, column_count, False, 2)
    portion_shape = portion.shape
    flat_rows = portion.reshape(-1, model_width)
    gate_values = jnp.dot(flat_rows, expert_gate[0], preferred_element_type=jnp.float32)
    up_values = jnp.dot(flat_rows, expert_up[0], preferred_element_type=jnp.float32)
    hidden = (jax.nn.silu(gate_values) * up_values).astype(jnp.bfloat16)
    partial_value = jnp.dot(hidden, expert_down[0], preferred_element_type=jnp.float32).astype(
        jnp.bfloat16
    )
    returned = give_back(partial_value.reshape(portion_shape), 3)
    flat_returned = returned.reshape(experts * capacity, model_width)
    expert_mix = jnp.zeros((row_count, model_width), jnp.float32)
    for route_index in range(TOP):
        selector = (slot_index[:, route_index][:, None] == slot_ids[None, :]).astype(jnp.bfloat16)
        picked = jnp.dot(selector, flat_returned, preferred_element_type=jnp.float32)
        expert_mix = expert_mix + route_weight[:, route_index][:, None] * picked
    return (hidden_state.astype(jnp.float32) + expert_mix).astype(jnp.bfloat16)


def solution(mesh):
    placed = (
        P("sp", "tp"),
        P("sp", "tp"),
        P(("sp", "tp"), None),
        P(("sp", "tp"), None),
        P(),
        P(None, "tp"),
        P(None, "tp"),
        P(None, "tp"),
        P(None, "tp"),
        P("tp", None),
        P("tp", None),
        P(("sp", "tp"), None),
        P(),
        P(("sp", "tp"), None),
        P(("sp", "tp"), None),
        P("sp", None, "tp"),
        P("sp", None, "tp"),
        P("sp", "tp", None),
    )
    return jax.shard_map(
        body, mesh=mesh, in_specs=placed, out_specs=P(("sp", "tp"), None), check_vma=False
    )
```
